32 devices in a mesh: sp: 16 (over z, y, x), tp: 2 (over core).
Axes of the slice: x: 2, y: 2, z: 4, core: 2. Of those that a mesh axis runs over, the one named last changes fastest.
Arguments:
- tokens: bfloat16 [4096, 2048], P('sp'), may hold values from -6 to 6
- input_norm_gain: float32 [2048], replicated, may hold values from 0.1 to 1.9
- mq_weight: bfloat16 [2048, 1024], P('sp', 'tp'), may hold values from -0.125 to 0.125
- mk_weight: bfloat16 [2048, 1024], P('sp', 'tp'), may hold values from -0.125 to 0.125
- mv_weight: bfloat16 [2048, 1024], P('sp', 'tp'), may hold values from -0.125 to 0.125
- mo_weight: bfloat16 [2048, 1024], P('sp', 'tp'), may hold values from -0.125 to 0.125
- gate_weight: bfloat16 [2048, 4, 8], P('sp', None, 'tp'), may hold values from -0.125 to 0.125
- gate_bias: float32 [4, 8], P(None, 'tp'), may hold values from -3 to 100
- decay_extra: float32 [2, 8, 4096], P(None, 'tp', 'sp'), may hold values from -1 to 0
- m_gain: float32 [1024], P('tp'), may hold values from 0.1 to 1.9
- aq_weight: bfloat16 [2048, 1024], P('sp', 'tp'), may hold values from -0.125 to 0.125
- ak_weight: bfloat16 [2048, 512], P('sp', 'tp'), may hold values from -8.838835 to 8.838835
- av_weight: bfloat16 [2048, 512], P('sp', 'tp'), may hold values from -0.125 to 0.125
- sink_logit: float32 [16], P('tp'), may hold values from 3 to 6
- out_m_weight: bfloat16 [1024, 2048], P('sp', 'tp'), may hold values from -0.1875 to 0.1875
- out_a_weight: bfloat16 [1024, 2048], P('sp', 'tp'), may hold values from -1.5 to 1.5
Outputs:
- mixed: bfloat16 [4096, 2048], P('sp', 'tp')
- log_total: float32 [16, 4096], P('tp', 'sp')
The draws below stay inside these ranges and needn't reach their ends.
All inputs are finite; a program needn't handle non-finite values.
Results may differ from the reference program's by a relative error of at most 0.015.
The reference program's roundings to bfloat16 on the way count: a program that leaves them out, or rounds other values in their place, can miss the bound.
Values may be sent and summed in bfloat16 or wider, within the bound.
No kernel may reach another device: no remote copies, remote signals or barrier semaphores. Data moves between devices by JAX's collectives and lax.ppermute only.
A program may use at most 64 MiB of HBM per device.

```python
import math
import jax
import jax.numpy as jnp
from jax import lax

D = 2048
M_HEADS = 8
M_DIM = 128
W_HEADS = 16
KEY_VALUE_HEADS = 8
W_DIM = 64
WINDOW = 128
M_BLOCK = 64
TOK_DEV = 256
SEQUENCE_STEPS = 4096
M_WIDTH = 1024
W_WIDTH = 1024
KV_WIDTH = 512


def draw_gate_bias(key, part):
    keys_all = jax.random.split(jax.random.fold_in(key, 11), 4)
    inputs_gate = jax.random.truncated_normal(keys_all[0], -3.0, 3.0, (2, M_HEADS), jnp.float32)
    fast_share = 0.5
    fast_heads = jax.random.uniform(keys_all[1], (2, M_HEADS), jnp.float32) < fast_share
    fast_value = jax.random.uniform(keys_all[2], (2, M_HEADS), jnp.float32, 2.5, 3.5)
    slow_value = math.log(SEQUENCE_STEPS) + jax.random.uniform(keys_all[3], (2, M_HEADS), jnp.float32, 1.0, 2.0)
    forget_bias = jnp.where(fast_heads, fast_value, slow_value)
    return jnp.stack([inputs_gate[0], forget_bias[0], inputs_gate[1], forget_bias[1]])


def draw_decay_extra(key, part):
    keys_all = jax.random.split(jax.random.fold_in(key, 23), 3)
    block_total = SEQUENCE_STEPS // TOK_DEV
    rates = jnp.exp(jax.random.uniform(keys_all[0], (2, M_HEADS, block_total), jnp.float32, math.log(0.2), math.log(2.0))) / SEQUENCE_STEPS
    reference_speed = -jnp.repeat(rates, TOK_DEV, axis=2)
    spots = jax.random.randint(keys_all[1], (2, M_HEADS, 2), 0, SEQUENCE_STEPS)
    stacked_level = jnp.log(jax.random.uniform(keys_all[2], (2, M_HEADS, 2), jnp.float32, 0.5, 0.8))
    places = jnp.arange(SEQUENCE_STEPS, dtype=jnp.int32)
    equality_detected = places[None, None, :, None] == spots[:, :, None, :]
    clustered_spikes = jnp.sum(jnp.where(equality_detected, stacked_level[:, :, None, :], 0.0), axis=-1)
    return reference_speed + clustered_spikes


def draw_ak_weight(key, part):
    base_draw = jax.random.truncated_normal(jax.random.fold_in(key, 5), -4.0, 4.0, (D, KV_WIDTH), jnp.float32) * D ** (-0.5)
    return base_draw.astype(jnp.bfloat16)


def block_levels(key, extent, shards, smallest, high):
    gain = 1.0
    for dim, parts in shards:
        steps = jax.random.uniform(jax.random.fold_in(jax.random.fold_in(key, 6), dim), (parts,), jnp.float32, smallest / len(shards), high / len(shards))
        gain = gain * jnp.repeat(jnp.exp(steps), extent[dim] // parts).reshape((-1,) + (1,) * (len(extent) - 1 - dim))
    return gain


def centred(own_key, extent, deviation, bound, pieces=(), kind=jnp.bfloat16):
    loudness = block_levels(own_key, extent, pieces, -0.22, 0.18) if pieces else 1.0
    drawn = jax.random.normal(own_key, extent, jnp.float32) * deviation * loudness
    return jnp.minimum(jnp.maximum(drawn, -bound), bound).astype(kind)


def setup_inputs(seed: int = 0) -> dict:
    key_list = jax.random.split(jax.random.key(seed), 17)
    return {
        "tokens": centred(key_list[0], (SEQUENCE_STEPS, D), 1.0, 6.0, ((0, 16),)),
        "input_norm_gain": jnp.clip(1.0 + 0.18 * jax.random.normal(key_list[1], (D,), jnp.float32), 0.1, 1.9),
        "mq_weight": centred(key_list[2], (D, M_WIDTH), D ** -0.5, 0.125, ((0, 16), (1, 2))),
        "mk_weight": centred(key_list[3], (D, M_WIDTH), D ** -0.5, 0.125, ((0, 16), (1, 2))),
        "mv_weight": centred(key_list[4], (D, M_WIDTH), D ** -0.5, 0.125, ((0, 16), (1, 2))),
        "mo_weight": centred(key_list[5], (D, M_WIDTH), D ** -0.5, 0.125, ((0, 16), (1, 2))),
        "gate_weight": centred(key_list[6], (D, 4, M_HEADS), D ** -0.5, 0.125, ((0, 16), (2, 2))),
        "gate_bias": draw_gate_bias(jax.random.fold_in(key_list[16], 71), 0),
        "decay_extra": draw_decay_extra(jax.random.fold_in(key_list[16], 71), 0),
        "m_gain": jnp.clip(1.0 + 0.18 * jax.random.normal(key_list[9], (M_WIDTH,), jnp.float32), 0.1, 1.9),
        "aq_weight": centred(key_list[10], (D, W_WIDTH), D ** -0.5, 0.125, ((0, 16), (1, 2))),
        "ak_weight": draw_ak_weight(jax.random.fold_in(key_list[16], 71), 0),
        "av_weight": centred(key_list[12], (D, KV_WIDTH), D ** -0.5, 0.125, ((0, 16), (1, 2))),
        "sink_logit": jnp.clip(3.0 + 3.0 * jax.random.uniform(key_list[13], (W_HEADS,), jnp.float32) ** block_levels(key_list[13], (W_HEADS,), ((0, 2),), -0.2, 0.2), 3.0, 6.0),
        "out_m_weight": centred(key_list[14], (M_WIDTH, D), M_WIDTH ** -0.5, 0.1875, ((0, 16), (1, 2))),
        "out_a_weight": centred(key_list[15], (W_WIDTH, D), (W_WIDTH // 64) ** -0.5, 1.5, ((0, 16), (1, 2))),
    }


EPS = 1e-06
HIGHEST = lax.Precision.HIGHEST

def rms_rows(inputs, gain_vec):
    return inputs * lax.rsqrt(lax.optimization_barrier(jnp.mean(inputs * inputs, axis=-1, keepdims=True)) + EPS) * gain_vec

def stored(result):
    return lax.optimization_barrier(result.astype(jnp.bfloat16))

def block_pass(queries, key_vecs, value_vecs, in_gate, log_forget, start_state):
    head_count, length, head_width = queries.shape
    block_count = length // M_BLOCK

    def blocks(array_in):
        return jnp.moveaxis(array_in.reshape((head_count, block_count, M_BLOCK) + array_in.shape[2:]), 1, 0)
    lower_mask = jnp.tril(jnp.ones((M_BLOCK, M_BLOCK), dtype=bool))

    def advance(state_in, block_in):
        cell_mat, norm_vec, stab_max = state_in
        q_blk, k_blk, v_blk, i_blk, f_blk = block_in
        cum_log = jnp.cumsum(f_blk, axis=-1)
        seg_total = cum_log[:, -1]
        log_end = seg_total[:, None] - cum_log + i_blk
        max_next = jnp.maximum(seg_total + stab_max, lax.optimization_barrier(jnp.max(log_end, axis=-1)))
        w_end = jnp.exp(log_end - max_next[:, None])
        fade_old = jnp.exp(seg_total + stab_max - max_next)
        cell_next = fade_old[:, None, None] * cell_mat + jnp.einsum('hsv,hsk->hvk', w_end[:, :, None] * v_blk, k_blk, precision=HIGHEST)
        norm_next = fade_old[:, None] * norm_vec + jnp.einsum('hs,hsk->hk', w_end, k_blk, precision=HIGHEST)
        log_w = jnp.where(lower_mask, cum_log[:, :, None] - cum_log[:, None, :] + i_blk[:, None, :], -jnp.inf)
        log_inter = cum_log + stab_max[:, None]
        row_max = jnp.maximum(log_inter, lax.optimization_barrier(jnp.max(log_w, axis=-1)))
        w_intra = jnp.exp(log_w - row_max[:, :, None])
        w_inter = jnp.exp(log_inter - row_max)
        scores = jnp.einsum('htk,hsk->hts', q_blk, k_blk, precision=HIGHEST) * w_intra
        numerator = jnp.einsum('hts,hsv->htv', scores, v_blk, precision=HIGHEST) + w_inter[..., None] * jnp.einsum('hvk,htk->htv', cell_mat, q_blk, precision=HIGHEST)
        denominator = lax.optimization_barrier(jnp.sum(scores, axis=-1)) + w_inter * jnp.einsum('hk,htk->ht', norm_vec, q_blk, precision=HIGHEST)
        result_rows = numerator / jnp.maximum(jnp.abs(denominator), jnp.exp(-row_max))[..., None]
        return ((cell_next, norm_next, max_next), result_rows)
    final_state, outputs = lax.scan(advance, start_state, tuple((blocks(array_in) for array_in in (queries, key_vecs, value_vecs, in_gate, log_forget))))
    return (jnp.moveaxis(outputs, 0, 1).reshape(head_count, length, head_width), final_state)

def flip_tokens(array_in):
    return jnp.flip(array_in, axis=1)

def window_attention(a_query, a_key, a_value, sink_logit):
    length = a_query.shape[0]
    block_count = length // WINDOW
    groups = W_HEADS // KEY_VALUE_HEADS
    query_blocks = a_query.reshape(block_count, WINDOW, KEY_VALUE_HEADS, groups, W_DIM)
    border = ((WINDOW, WINDOW), (0, 0))
    key_pad = jnp.pad(a_key, border).reshape(length + 2 * WINDOW, KEY_VALUE_HEADS, W_DIM)
    value_pad = jnp.pad(a_value, border).reshape(length + 2 * WINDOW, KEY_VALUE_HEADS, W_DIM)
    query_off = jnp.arange(WINDOW, dtype=jnp.int32)
    key_off = jnp.arange(3 * WINDOW, dtype=jnp.int32) - WINDOW
    in_window = jnp.abs(query_off[:, None] - key_off[None, :]) <= WINDOW
    sink_col = sink_logit.reshape(KEY_VALUE_HEADS, groups, 1)

    def one_block(block_in):
        index, query_rows = block_in
        first = (index * WINDOW).astype(jnp.int32)
        key_rows = lax.dynamic_slice_in_dim(key_pad, first, 3 * WINDOW, 0).astype(jnp.float32)
        value_rows = lax.dynamic_slice_in_dim(value_pad, first, 3 * WINDOW, 0).astype(jnp.float32)
        key_place = first + key_off
        usable = in_window & ((key_place >= 0) & (key_place < length))[None, :]
        scores = jnp.einsum('qgrd,kgd->grqk', query_rows.astype(jnp.float32), key_rows) * W_DIM ** (-0.5)
        scores = jnp.where(usable, scores, -jnp.inf)
        peak_log = jnp.maximum(sink_col, lax.optimization_barrier(jnp.max(scores, axis=-1)))
        weights_exp = jnp.exp(scores - peak_log[..., None])
        weight_total_sum = jnp.exp(sink_col - peak_log) + lax.optimization_barrier(jnp.sum(weights_exp, axis=-1))
        rounded = weights_exp.astype(jnp.bfloat16).astype(jnp.float32)
        weighted = jnp.einsum('grqk,kgd->qgrd', rounded, value_rows)
        mixed_rows = (weighted / jnp.transpose(weight_total_sum, (2, 0, 1))[..., None]).astype(jnp.bfloat16)
        return (mixed_rows.reshape(WINDOW, W_HEADS * W_DIM), (peak_log + jnp.log(weight_total_sum)).reshape(W_HEADS, WINDOW))
    mixed_blocks, log_blocks = lax.map(one_block, (jnp.arange(block_count, dtype=jnp.int32), query_blocks))
    return (mixed_blocks.reshape(length, W_HEADS * W_DIM), jnp.transpose(log_blocks, (1, 0, 2)).reshape(W_HEADS, length))

def reference(tokens, input_norm_gain, mq_weight, mk_weight, mv_weight, mo_weight, gate_weight, gate_bias, decay_extra, m_gain, aq_weight, ak_weight, av_weight, sink_logit, out_m_weight, out_a_weight):
    length = tokens.shape[0]
    normed = rms_rows(tokens.astype(jnp.float32), input_norm_gain).astype(jnp.bfloat16)

    def project(weight_mat):
        return jnp.dot(normed, weight_mat, preferred_element_type=jnp.float32)
    m_query = stored(project(mq_weight))
    m_key = stored(project(mk_weight))
    m_value = stored(project(mv_weight))
    m_out = stored(project(mo_weight))
    gates = project(gate_weight.reshape(D, 4 * M_HEADS)).reshape(length, 4, M_HEADS) + gate_bias[None]

    def heads_first(matrix):
        return jnp.transpose(matrix.astype(jnp.float32).reshape(length, M_HEADS, M_DIM), (1, 0, 2))
    queries = heads_first(m_query)
    key_vecs = heads_first(m_key) * M_DIM ** (-0.5)
    value_vecs = heads_first(m_value)
    in_fwd = gates[:, 0, :].T
    forget_fwd = jax.nn.log_sigmoid(gates[:, 1, :].T) + decay_extra[0]
    in_bwd = gates[:, 2, :].T
    forget_bwd = jax.nn.log_sigmoid(gates[:, 3, :].T) + decay_extra[1]
    zero_state = (jnp.zeros((M_HEADS, M_DIM, M_DIM), jnp.float32), jnp.zeros((M_HEADS, M_DIM), jnp.float32), jnp.zeros((M_HEADS,), jnp.float32))
    hidden_fwd, forward_unused = block_pass(queries, key_vecs, value_vecs, in_fwd, forget_fwd, zero_state)
    hidden_bwd, unused_bwd = block_pass(flip_tokens(queries), flip_tokens(key_vecs), flip_tokens(value_vecs), flip_tokens(in_bwd), flip_tokens(forget_bwd), zero_state)
    cell_out = hidden_fwd + flip_tokens(hidden_bwd)
    gate_open = jax.nn.sigmoid(m_out.astype(jnp.float32)).reshape(length, M_HEADS, M_DIM)
    cell_rows = jnp.transpose(cell_out, (1, 0, 2)) * gate_open
    mixed_m = rms_rows(cell_rows, m_gain.reshape(M_HEADS, M_DIM)).astype(jnp.bfloat16).reshape(length, M_WIDTH)
    a_query = stored(project(aq_weight))
    a_key = stored(project(ak_weight))
    a_value = stored(project(av_weight))
    mixed_a, log_total = window_attention(a_query, a_key, a_value, sink_logit)
    mixed = jnp.dot(mixed_m, out_m_weight, preferred_element_type=jnp.float32) + jnp.dot(mixed_a, out_a_weight, preferred_element_type=jnp.float32)
    return (mixed.astype(jnp.bfloat16), log_total)
```

```python
import jax
import jax.numpy as jnp
from jax import lax
from jax.experimental import pallas as pl
from jax.experimental.pallas import tpu as pltpu
from jax.sharding import PartitionSpec as P

M_DIM = 128
W_DIM = 64
WINDOW = 128
M_BLOCK = 64


EPS = 1e-06
FLOOR_LOG = -1e30
HIGHEST = lax.Precision.HIGHEST


def with_halo(x, sides, width):
    for axis, dim in sides:
        peers, length = (lax.axis_size(axis), x.shape[dim])
        up = [(i, (i + 1) % peers) for i in range(peers - 1)]
        down = [(j, i) for i, j in up]
        last = lax.slice_in_dim(x, length - width, length, axis=dim)
        first = lax.slice_in_dim(x, 0, width, axis=dim)
        before = lax.ppermute(last, axis, up)
        after = lax.ppermute(first, axis, down)
        x = jnp.concatenate([before, x, after], axis=dim)
    return x


def rms_rows(inputs, gain_vec):
    return inputs * lax.rsqrt(jnp.mean(inputs * inputs, axis=-1, keepdims=True) + EPS) * gain_vec


def stored(result):
    return lax.optimization_barrier(result.astype(jnp.bfloat16))


def flip_tokens(array_in):
    return jnp.flip(array_in, axis=1)


def block_pass(queries, key_vecs, value_vecs, in_gate, log_forget, start_state):
    head_count, length, head_width = queries.shape
    block_count = length // M_BLOCK

    def blocks(array_in):
        return jnp.moveaxis(
            array_in.reshape((head_count, block_count, M_BLOCK) + array_in.shape[2:]), 1, 0
        )

    lower_mask = jnp.tril(jnp.ones((M_BLOCK, M_BLOCK), dtype=bool))

    def advance(state_in, block_in):
        cell_mat, norm_vec, stab_max = state_in
        q_blk, k_blk, v_blk, i_blk, f_blk = block_in
        cum_log = jnp.cumsum(f_blk, axis=-1)
        seg_total = cum_log[:, -1]
        log_end = seg_total[:, None] - cum_log + i_blk
        max_next = jnp.maximum(seg_total + stab_max, jnp.max(log_end, axis=-1))
        w_end = jnp.exp(log_end - max_next[:, None])
        fade_old = jnp.exp(seg_total + stab_max - max_next)
        cell_next = fade_old[:, None, None] * cell_mat + jnp.einsum(
            "hsv,hsk->hvk", w_end[:, :, None] * v_blk, k_blk, precision=HIGHEST
        )
        norm_next = fade_old[:, None] * norm_vec + jnp.einsum(
            "hs,hsk->hk", w_end, k_blk, precision=HIGHEST
        )
        log_w = jnp.where(
            lower_mask, cum_log[:, :, None] - cum_log[:, None, :] + i_blk[:, None, :], -jnp.inf
        )
        log_inter = cum_log + stab_max[:, None]
        row_max = jnp.maximum(log_inter, jnp.max(log_w, axis=-1))
        w_intra = jnp.exp(log_w - row_max[:, :, None])
        w_inter = jnp.exp(log_inter - row_max)
        scores = jnp.einsum("htk,hsk->hts", q_blk, k_blk, precision=HIGHEST) * w_intra
        numerator = jnp.einsum("hts,hsv->htv", scores, v_blk, precision=HIGHEST) + w_inter[
            ..., None
        ] * jnp.einsum("hvk,htk->htv", cell_mat, q_blk, precision=HIGHEST)
        denominator = jnp.sum(scores, axis=-1) + w_inter * jnp.einsum(
            "hk,htk->ht", norm_vec, q_blk, precision=HIGHEST
        )
        result_rows = numerator / jnp.maximum(jnp.abs(denominator), jnp.exp(-row_max))[..., None]
        return ((cell_next, norm_next, max_next), result_rows)

    final_state, outputs = lax.scan(
        advance,
        start_state,
        tuple(
            (blocks(array_in) for array_in in (queries, key_vecs, value_vecs, in_gate, log_forget))
        ),
    )
    return (jnp.moveaxis(outputs, 0, 1).reshape(head_count, length, head_width), final_state)


def summarize(key_vecs, value_vecs, in_gate, log_forget):
    cum_log = jnp.cumsum(log_forget, axis=-1)
    seg_total = cum_log[:, -1]
    log_end = seg_total[:, None] - cum_log + in_gate
    peak_log = jnp.max(log_end, axis=-1)
    weights_end = jnp.exp(log_end - peak_log[:, None])
    cell_mat = jnp.einsum(
        "hsv,hsk->hvk", weights_end[:, :, None] * value_vecs, key_vecs, precision=HIGHEST
    )
    norm_vec = jnp.einsum("hs,hsk->hk", weights_end, key_vecs, precision=HIGHEST)
    return (seg_total, cell_mat, norm_vec, peak_log)


def merge_side(state_in, cell_mats, norm_vecs, logs, usable):
    cell_mat, norm_vec, peak_log = state_in
    masked = jnp.where(usable, logs, FLOOR_LOG)
    new_peak = jnp.maximum(peak_log, jnp.max(masked, axis=0))
    scales = jnp.where(usable, jnp.exp(masked - new_peak[None]), 0.0)
    cell_mat = jnp.einsum("jh,jhvk->hvk", scales, cell_mats, precision=HIGHEST)
    norm_vec = jnp.einsum("jh,jhk->hk", scales, norm_vecs, precision=HIGHEST)
    return (cell_mat, norm_vec, new_peak)


def gather_states(forward_sum, backward_sum):
    decay_all = (
        lax.all_gather(forward_sum[0][None], "sp", axis=0, tiled=True),
        lax.all_gather(backward_sum[0][None], "sp", axis=0, tiled=True),
    )
    own_index = lax.axis_index("sp")
    acc_fwd = jnp.cumsum(decay_all[0], axis=0)
    acc_bwd = jnp.cumsum(decay_all[1], axis=0)
    before_own = lax.dynamic_index_in_dim(acc_fwd - decay_all[0], own_index, 0, keepdims=False)
    after_own = lax.dynamic_index_in_dim(acc_bwd, own_index, 0, keepdims=False)
    lead_bwd = acc_bwd - decay_all[1]
    empty_side = (
        jnp.zeros_like(forward_sum[1]),
        jnp.zeros_like(forward_sum[2]),
        jnp.full_like(forward_sum[3], FLOOR_LOG),
    )
    state_in = empty_side + empty_side
    pieces = (
        lax.all_gather(forward_sum[1][None], "sp", axis=0, tiled=True),
        lax.all_gather(forward_sum[2][None], "sp", axis=0, tiled=True),
        lax.all_gather(forward_sum[3][None], "sp", axis=0, tiled=True),
        lax.all_gather(backward_sum[1][None], "sp", axis=0, tiled=True),
        lax.all_gather(backward_sum[2][None], "sp", axis=0, tiled=True),
        lax.all_gather(backward_sum[3][None], "sp", axis=0, tiled=True),
    )
    piece_count = pieces[0].shape[0]
    device_ids = jnp.arange(piece_count, dtype=jnp.int32)
    log_fwd = before_own[None] - acc_fwd + pieces[2]
    log_bwd = lead_bwd - after_own[None] + pieces[5]
    left_side = merge_side(
        state_in[:3], pieces[0], pieces[1], log_fwd, (device_ids < own_index)[:, None]
    )
    right_side = merge_side(
        state_in[3:], pieces[3], pieces[4], log_bwd, (device_ids > own_index)[:, None]
    )
    states = left_side + right_side
    return (states[:3], states[3:])


def window_attend(a_query, kv_pairs, sink_logit, first_row, total_rows):
    tok_rows = a_query.shape[0]
    block_len = WINDOW
    block_count = tok_rows // block_len
    kv_width = kv_pairs.shape[1] // 2
    kv_heads = kv_width // W_DIM
    q_heads = a_query.shape[1] // W_DIM
    groups = q_heads // kv_heads
    filled_margin = with_halo(kv_pairs, (("sp", 0),), WINDOW)
    windows = jnp.concatenate(
        [
            filled_margin[place_idx * block_len : place_idx * block_len + tok_rows].reshape(
                block_count, block_len, 2 * kv_width
            )
            for place_idx in range(3)
        ],
        axis=1,
    )
    key_block = windows[:, :, :kv_width].reshape(block_count, 3 * block_len, kv_heads, W_DIM)
    content_tile = windows[:, :, kv_width:].reshape(block_count, 3 * block_len, kv_heads, W_DIM)
    query_block = a_query.reshape(block_count, block_len, kv_heads, groups, W_DIM)
    scores = jnp.einsum(
        "nqgrd,nkgd->ngrqk", query_block, key_block, preferred_element_type=jnp.float32
    ) * W_DIM ** (-0.5)
    query_off = jnp.arange(block_len, dtype=jnp.int32)
    key_off = jnp.arange(3 * block_len, dtype=jnp.int32) - block_len
    in_window = jnp.abs(query_off[:, None] - key_off[None, :]) <= WINDOW
    key_place = (
        first_row + jnp.arange(block_count, dtype=jnp.int32)[:, None] * block_len + key_off[None, :]
    )
    inside = (key_place >= 0) & (key_place < total_rows)
    usable = in_window[None] & inside[:, None, :]
    scores = jnp.where(usable[:, None, None], scores, -jnp.inf)
    sink_col = sink_logit.reshape(kv_heads, groups)[None, :, :, None]
    peak_log = jnp.maximum(sink_col, jnp.max(scores, axis=-1))
    weights_exp = jnp.exp(scores - peak_log[..., None])
    weight_total_sum = jnp.exp(sink_col - peak_log) + jnp.sum(weights_exp, axis=-1)
    weighted = jnp.einsum(
        "ngrqk,nkgd->nqgrd",
        weights_exp.astype(jnp.bfloat16),
        content_tile,
        preferred_element_type=jnp.float32,
    )
    scale_back = jnp.transpose(weight_total_sum, (0, 3, 1, 2))[..., None]
    mixed_rows = (weighted / scale_back).astype(jnp.bfloat16).reshape(tok_rows, q_heads * W_DIM)
    log_total = jnp.transpose(peak_log + jnp.log(weight_total_sum), (1, 2, 0, 3)).reshape(
        q_heads, tok_rows
    )
    return (mixed_rows, log_total)


def on_device(
    tokens,
    input_norm_gain,
    mq_weight,
    mk_weight,
    mv_weight,
    mo_weight,
    gate_weight,
    gate_bias,
    decay_extra,
    m_gain,
    aq_weight,
    ak_weight,
    av_weight,
    sink_logit,
    out_m_weight,
    out_a_weight,
):
    tok_rows = tokens.shape[0]
    normed = rms_rows(tokens.astype(jnp.float32), input_norm_gain).astype(jnp.bfloat16)
    local_heads = gate_weight.shape[2]
    gate_cols = 4 * local_heads
    pieces = (
        lax.all_gather(mq_weight, "sp", axis=0, tiled=True),
        lax.all_gather(mk_weight, "sp", axis=0, tiled=True),
        lax.all_gather(mv_weight, "sp", axis=0, tiled=True),
        lax.all_gather(mo_weight, "sp", axis=0, tiled=True),
        lax.all_gather(gate_weight, "sp", axis=0, tiled=True),
        lax.all_gather(aq_weight, "sp", axis=0, tiled=True),
        lax.all_gather(ak_weight, "sp", axis=0, tiled=True),
        lax.all_gather(av_weight, "sp", axis=0, tiled=True),
    )
    piece_rows = pieces[0].shape[0]
    flat_gate = pieces[4].reshape(piece_rows, gate_cols)
    segments = (
        pieces[0],
        pieces[1],
        pieces[2],
        pieces[3],
        flat_gate,
        pieces[5],
        pieces[6],
        pieces[7],
    )
    projected = tuple(
        (jnp.dot(normed, segment, preferred_element_type=jnp.float32) for segment in segments)
    )
    m_query = stored(projected[0])
    m_key = stored(projected[1])
    m_value = stored(projected[2])
    m_out = stored(projected[3])
    gates = projected[4].reshape(tok_rows, 4, local_heads) + gate_bias[None]

    def heads_first(matrix):
        return jnp.transpose(
            matrix.astype(jnp.float32).reshape(tok_rows, local_heads, M_DIM), (1, 0, 2)
        )

    queries = heads_first(m_query)
    key_vecs = heads_first(m_key) * M_DIM ** (-0.5)
    value_vecs = heads_first(m_value)
    in_fwd = gates[:, 0, :].T
    forget_fwd = jax.nn.log_sigmoid(gates[:, 1, :].T) + decay_extra[0]
    in_bwd = flip_tokens(gates[:, 2, :].T)
    forget_bwd = flip_tokens(jax.nn.log_sigmoid(gates[:, 3, :].T) + decay_extra[1])
    queries_bwd = flip_tokens(queries)
    keys_bwd = flip_tokens(key_vecs)
    values_bwd = flip_tokens(value_vecs)
    forward_sum = summarize(key_vecs, value_vecs, in_fwd, forget_fwd)
    backward_sum = summarize(keys_bwd, values_bwd, in_bwd, forget_bwd)
    state_fwd, state_bwd = gather_states(forward_sum, backward_sum)
    hidden_fwd, forward_unused = block_pass(
        queries, key_vecs, value_vecs, in_fwd, forget_fwd, state_fwd
    )
    hidden_bwd, unused_bwd = block_pass(
        queries_bwd, keys_bwd, values_bwd, in_bwd, forget_bwd, state_bwd
    )
    cell_out = hidden_fwd + flip_tokens(hidden_bwd)
    gate_open = jax.nn.sigmoid(m_out.astype(jnp.float32)).reshape(tok_rows, local_heads, M_DIM)
    cell_rows = jnp.transpose(cell_out, (1, 0, 2)) * gate_open
    mixed_m = (
        rms_rows(cell_rows, m_gain.reshape(local_heads, M_DIM))
        .astype(jnp.bfloat16)
        .reshape(tok_rows, local_heads * M_DIM)
    )
    a_query = stored(projected[5])
    kv_pairs = jnp.concatenate([stored(projected[6]), stored(projected[7])], axis=1)
    first_row = lax.axis_index("sp") * tok_rows
    total_rows = tok_rows * lax.axis_size("sp")
    mixed_a, log_total = window_attend(a_query, kv_pairs, sink_logit, first_row, total_rows)
    full_m, full_a = (
        lax.all_gather(mixed_m, "tp", axis=1, tiled=True),
        lax.all_gather(mixed_a, "tp", axis=1, tiled=True),
    )
    pieces = (
        lax.all_gather(out_m_weight, "sp", axis=0, tiled=True),
        lax.all_gather(out_a_weight, "sp", axis=0, tiled=True),
    )
    running = jnp.dot(full_m, pieces[0], preferred_element_type=jnp.float32)
    mixed = running + jnp.dot(full_a, pieces[1], preferred_element_type=jnp.float32)
    return (mixed.astype(jnp.bfloat16), log_total)


CHUNK = 256
LANES = 128
EMPTY = -1e30


def split_plan(mesh, args):
    sp, tp = mesh.shape["sp"], mesh.shape["tp"]
    tok_rows, width = args[0].shape
    rows = args[2].shape[0]
    local_heads = args[6].shape[2]
    group = local_heads * tp
    if tp != 2 or sp != 2 * group or group % 4 or (group // 2) & (group // 2 - 1):
        return None
    plane = group // 2
    ok = (
        args[2].shape[1] == local_heads * M_DIM
        and args[10].shape[1] == local_heads * LANES
        and args[11].shape[1] == local_heads * W_DIM
        and args[12].shape[1] == local_heads * W_DIM
        and 2 * W_DIM == LANES
        and M_DIM == LANES
        and WINDOW == LANES
        and tok_rows == CHUNK
        and rows == LANES
        and args[14].shape[0] * sp == group * M_DIM
        and args[15].shape[0] * sp == group * LANES
    )
    if not ok:
        return None
    return dict(
        sp=sp, tp=tp, tok=tok_rows, width=width, rows=rows, lh=local_heads, group=group, plane=plane
    )


def mm(a, b, ca=1, cb=0, precision=None):
    return lax.dot_general(
        a, b, (((ca,), (cb,)), ((), ())), precision=precision, preferred_element_type=jnp.float32
    )


def vmem_call(kernel, outs, scratch=(), smem=0, n_in=0, flops=0):
    return pl.pallas_call(
        kernel,
        out_shape=outs,
        in_specs=[pl.BlockSpec(memory_space=pltpu.SMEM)] * smem
        + [pl.BlockSpec(memory_space=pltpu.VMEM)] * n_in,
        out_specs=jax.tree.map(lambda _: pl.BlockSpec(memory_space=pltpu.VMEM), outs),
        scratch_shapes=scratch,
        cost_estimate=pl.CostEstimate(flops=flops, bytes_accessed=0, transcendentals=0),
        compiler_params=pltpu.CompilerParams(vmem_limit_bytes=56 * 1024 * 1024),
    )


def pack_kernel(mq, mk, mv, mo, aq, ak, av, small, out):
    halves, heads = out.shape[0], out.shape[1]
    rows = mq.shape[0] // halves
    for u in range(halves):
        for h in range(heads):
            for c, ref in enumerate((mq, mk, mv, mo, aq)):
                out[u, h, c * rows : (c + 1) * rows, :] = ref[
                    u * rows : (u + 1) * rows, h * LANES : (h + 1) * LANES
                ]
            pair = jnp.concatenate(
                [
                    ref[u * rows : (u + 1) * rows, h * W_DIM : (h + 1) * W_DIM]
                    for ref in (ak, av)
                ],
                axis=1,
            )
            out[u, h, 5 * rows : 6 * rows, :] = pair
            out[u, h, 6 * rows :, :] = small[u, h]


def chunk_vecs(rows):
    n = rows.shape[1]
    r = lax.broadcasted_iota(jnp.int32, (n, n), 0)
    c = lax.broadcasted_iota(jnp.int32, (n, n), 1)
    lower = jnp.where(r >= c, 1.0, 0.0).astype(jnp.float32)
    eye = jnp.where(r == c, 1.0, 0.0).astype(jnp.float32)
    cum_col = mm(lower, rows, 1, 1, HIGHEST)
    raw_col = mm(eye, rows, 1, 1, HIGHEST)
    cum_row = mm(rows, lower, 1, 1, HIGHEST)
    f_col, f_row = cum_col[:, 1:2], cum_row[1:2]
    e_col = cum_col[:, 3:4] - raw_col[:, 3:4]
    e_row = cum_row[3:4] - rows[3:4]
    fwd = (f_col, rows[0:1] - f_row, raw_col[:, 0:1] - f_col, cum_row[1:2, n - 1 : n])
    bwd = (-e_col, rows[2:3] + e_row, raw_col[:, 2:3] + e_col, cum_row[3:4, n - 1 : n])
    return fwd, bwd


def advance_state(state, key, value, end_col, end_row, total):
    cell, norm, peak = state
    new_peak = jnp.maximum(total + peak, jnp.max(end_row, axis=1, keepdims=True))
    weighted = key * jnp.exp(end_col - new_peak)
    fade = jnp.exp(total + peak - new_peak)
    cell = fade * cell + mm(weighted, value, 0, 0, HIGHEST)
    norm = fade * norm + jnp.sum(weighted, axis=0, keepdims=True)
    return cell, norm, new_peak


def forward_state(state, key, value, vecs):
    return advance_state(state, key, value, vecs[2] + vecs[3], vecs[1] + vecs[3], vecs[3])


def backward_state(state, key, value, vecs):
    return advance_state(state, key, value, vecs[2], vecs[1], vecs[3])


def empty_state():
    return (
        jnp.zeros((M_DIM, M_DIM), jnp.float32),
        jnp.zeros((1, M_DIM), jnp.float32),
        jnp.full((1, 1), EMPTY, jnp.float32),
    )


def project_kernel(meta, bias, *refs):
    plan_plane = 4
    xs = refs[:plan_plane]
    own, partner, gate_t, decay, proj, gates, summary, halo, weight = refs[plan_plane:]
    t, k, sel, jl = meta[0], meta[1], meta[2], meta[3]
    sources = own.shape[0]
    rows = weight.shape[0] // sources // 2
    cols = weight.shape[1] // LANES

    def place(i, carry):
        for c in range(cols):
            lanes = slice(c * LANES, (c + 1) * LANES)
            span = slice(c * rows, (c + 1) * rows)
            first = pl.multiple_of((2 * i + t) * rows, rows)
            second = pl.multiple_of((2 * i + 1 - t) * rows, rows)
            weight[pl.ds(first, rows), lanes] = own[i, span, :]
            weight[pl.ds(second, rows), lanes] = partner[i, span, :]
        return carry

    lax.fori_loop(0, sources, place, 0)
    tok = xs[0].shape[0]
    for r, x in enumerate(xs):
        at = pl.ds(pl.multiple_of((k ^ r) * tok, tok), tok)
        proj[at, :] = mm(x[...], weight[...]).astype(jnp.bfloat16)
        gates[k ^ r] = mm(gate_t[...], x[...], 1, 1)[:8]
    heads = bias.shape[1] // 4
    b = [bias[sel, g * heads + jl] for g in range(4)]
    lead = jnp.concatenate([jnp.full((1, tok), b[g], jnp.float32) for g in range(4)], axis=0)
    forget = lax.broadcasted_iota(jnp.int32, (4, tok), 0) % 2 == 1
    fwd, bwd = empty_state(), empty_state()
    total_f = jnp.zeros((1, 1), jnp.float32)
    total_b = jnp.zeros((1, 1), jnp.float32)
    chunks = []
    for c in range(plan_plane):
        g = gates[c][:4] + lead
        d = decay[c]
        extra = jnp.concatenate([d[0:1], d[0:1], d[1:2], d[1:2]], axis=0)
        logs = jnp.minimum(g, 0.0) - jnp.log1p(jnp.exp(-jnp.abs(g))) + extra
        g = jnp.where(forget, logs, g)
        gates[c] = jnp.concatenate([g, jnp.zeros((4, tok), jnp.float32)], axis=0)
        vecs = chunk_vecs(gates[c])
        span = slice(c * tok, (c + 1) * tok)
        key = proj[span, LANES : 2 * LANES].astype(jnp.float32)
        value = proj[span, 2 * LANES : 3 * LANES].astype(jnp.float32)
        chunks.append((key, value, vecs))
    for key, value, vecs in chunks:
        fwd = forward_state(fwd, key, value, vecs[0])
        total_f = total_f + vecs[0][3]
    for key, value, vecs in chunks[::-1]:
        bwd = backward_state(bwd, key, value, vecs[1])
        total_b = total_b + vecs[1][3]
    for i, ((cell, norm, peak), total) in enumerate(((fwd, total_f), (bwd, total_b))):
        summary[i, :M_DIM, :] = cell
        summary[i, M_DIM:, :] = jnp.concatenate(
            [
                norm,
                jnp.broadcast_to(peak, (1, LANES)),
                jnp.broadcast_to(total, (1, LANES)),
                jnp.zeros((5, LANES), jnp.float32),
            ],
            axis=0,
        )
    last = proj.shape[0]
    halo[0] = proj[:WINDOW, 5 * LANES :].astype(jnp.float32)
    halo[1] = proj[last - WINDOW :, 5 * LANES :].astype(jnp.float32)


def read_state(ref, i):
    return (
        ref[i, :M_DIM, :],
        ref[i, M_DIM : M_DIM + 1, :],
        ref[i, M_DIM + 1 : M_DIM + 2, 0:1],
        ref[i, M_DIM + 2 : M_DIM + 3, 0:1],
    )


def merge_states(earlier, later, later_total):
    peak = jnp.maximum(later_total + earlier[2], later[2])
    old = jnp.exp(later_total + earlier[2] - peak)
    new = jnp.exp(later[2] - peak)
    return old * earlier[0] + new * later[0], old * earlier[1] + new * later[1], peak


def combine_kernel(meta, own, partner, halo_partner, out):
    t, hi = meta[0], meta[4]
    forward = hi == 0
    i = jnp.where(forward, 0, 1)
    mine, other = read_state(own, i), read_state(partner, i)
    mine_later = (t == 1) == forward
    a = tuple(jnp.where(mine_later, y, x) for x, y in zip(mine, other))
    b = tuple(jnp.where(mine_later, x, y) for x, y in zip(mine, other))
    cell, norm, peak = merge_states(a[:3], b[:3], b[3])
    out[:M_DIM, :] = cell
    out[M_DIM : M_DIM + 8, :] = jnp.concatenate(
        [norm, jnp.broadcast_to(peak, (1, LANES)), jnp.zeros((6, LANES), jnp.float32)], axis=0
    )
    out[M_DIM + 8 :, :] = halo_partner[jnp.where(forward, 1, 0)]


def mixer_kernel(meta, sink, proj, gates, partner, halo_partner, across, gain, out_m, out_a, kv, logs):
    t, sel, jl, hi = meta[0], meta[2], meta[3], meta[4]
    chunks = gates.shape[0]
    tok = gates.shape[2]
    far = (
        across[:M_DIM, :],
        across[M_DIM : M_DIM + 1, :],
        across[M_DIM + 1 : M_DIM + 2, 0:1],
    )

    def incoming(i, use_far, use_near):
        near = read_state(partner, i)
        far_peak = jnp.where(use_far, far[2], EMPTY)
        near_peak = jnp.where(use_near, near[2], EMPTY)
        near_total = jnp.where(use_near, near[3], 0.0)
        return merge_states((far[0], far[1], far_peak), (near[0], near[1], near_peak), near_total)

    scale = M_DIM ** (-0.5)
    fwd = incoming(0, hi == 1, t == 1)
    bwd = incoming(1, hi == 0, t == 0)
    vecs = [chunk_vecs(gates[c]) for c in range(chunks)]

    def kv_of(c):
        span = slice(c * tok, (c + 1) * tok)
        return (
            proj[span, LANES : 2 * LANES].astype(jnp.float32),
            proj[span, 2 * LANES : 3 * LANES].astype(jnp.float32),
        )

    back_states = [None] * chunks
    for c in range(chunks - 1, -1, -1):
        back_states[c] = bwd
        if c:
            bwd = backward_state(bwd, *kv_of(c), vecs[c][1])
    r = lax.broadcasted_iota(jnp.int32, (tok, tok), 0)
    col = lax.broadcasted_iota(jnp.int32, (tok, tok), 1)
    gain_row = gain[sel, pl.ds(jl, 1), :]
    for c in range(chunks):
        span = slice(c * tok, (c + 1) * tok)
        q = proj[span, :LANES]
        qf = q.astype(jnp.float32)
        scores = mm(q, proj[span, LANES : 2 * LANES], 1, 1) * scale
        total_w = None
        inter = None
        for state, vec, mask in ((fwd, vecs[c][0], r >= col), (back_states[c], vecs[c][1], r <= col)):
            cell, norm, peak = state
            lead_col, src_row = vec[0], vec[1]
            if mask is not None and vec is vecs[c][1]:
                reach = peak + vec[3]
            else:
                reach = peak
            masked = jnp.where(mask, src_row, EMPTY)
            top = jnp.maximum(jnp.max(masked, axis=1, keepdims=True), reach)
            w = jnp.exp(masked - top)
            w_in = jnp.exp(reach - top)
            denom = jnp.sum(scores * w, axis=1, keepdims=True) + w_in * scale * jnp.sum(
                qf * norm, axis=1, keepdims=True
            )
            inv = 1.0 / jnp.maximum(jnp.abs(denom), jnp.exp(-(lead_col + top)))
            part = w * inv
            add = mm(qf, cell, 1, 0, HIGHEST) * (scale * w_in * inv)
            total_w = part if total_w is None else total_w + part
            inter = add if inter is None else inter + add
        key, value = kv_of(c)
        cell_out = mm(scores * total_w, value, 1, 0, HIGHEST) + inter
        fwd = forward_state(fwd, key, value, vecs[c][0])
        gate = proj[span, 3 * LANES : 4 * LANES].astype(jnp.float32)
        u = cell_out / (1.0 + jnp.exp(-gate))
        u = u * lax.rsqrt(jnp.mean(u * u, axis=1, keepdims=True) + EPS) * gain_row
        out_m[c, :tok, :] = u.astype(jnp.bfloat16)
        out_m[c, tok:, :] = jnp.zeros((out_m.shape[1] - tok, LANES), jnp.bfloat16)

    length = proj.shape[0]
    inner_edge = halo_partner[jnp.where(t == 0, 0, 1)].astype(jnp.bfloat16)
    outer_edge = across[M_DIM + 8 :, :].astype(jnp.bfloat16)
    kv[:WINDOW, :] = jnp.where(t == 0, outer_edge, inner_edge)
    kv[WINDOW : WINDOW + length, :] = proj[:, 5 * LANES :]
    kv[WINDOW + length :, :] = jnp.where(t == 0, inner_edge, outer_edge)
    at_start = (hi == 0) & (t == 0)
    at_end = (hi == 1) & (t == 1)
    qi = lax.broadcasted_iota(jnp.int32, (WINDOW, 3 * WINDOW), 0)
    ki = lax.broadcasted_iota(jnp.int32, (WINDOW, 3 * WINDOW), 1) - WINDOW
    band = jnp.abs(ki - qi) <= WINDOW
    diag = lax.broadcasted_iota(jnp.int32, (WINDOW, WINDOW), 0) == lax.broadcasted_iota(
        jnp.int32, (WINDOW, WINDOW), 1
    )
    blocks = length // WINDOW
    per = tok // WINDOW
    for b in range(blocks):
        usable = band
        if b == 0:
            usable = usable & ((ki >= 0) | jnp.logical_not(at_start))
        if b == blocks - 1:
            usable = usable & ((ki < WINDOW) | jnp.logical_not(at_end))
        keys = kv[b * WINDOW : (b + 3) * WINDOW, :W_DIM]
        values = kv[b * WINDOW : (b + 3) * WINDOW, W_DIM:]
        mixed = []
        for h in range(2):
            lanes = slice(4 * LANES + h * W_DIM, 4 * LANES + (h + 1) * W_DIM)
            q = proj[b * WINDOW : (b + 1) * WINDOW, lanes]
            s = mm(q, keys, 1, 1) * W_DIM ** (-0.5)
            s = jnp.where(usable, s, EMPTY)
            sink_h = sink[sel, 2 * jl + h]
            peak = jnp.maximum(jnp.max(s, axis=1, keepdims=True), sink_h)
            e = jnp.exp(s - peak)
            total = jnp.exp(sink_h - peak) + jnp.sum(e, axis=1, keepdims=True)
            mixed.append(mm(e.astype(jnp.bfloat16), values) / total)
            log_col = peak + jnp.log(total)
            log_row = jnp.sum(jnp.where(diag, log_col, 0.0), axis=0, keepdims=True)
            at = h * per + b % per
            logs[b // per, at : at + 1, :] = log_row
        out_a[b // per, (b % per) * WINDOW : (b % per + 1) * WINDOW, :] = jnp.concatenate(
            mixed, axis=1
        ).astype(jnp.bfloat16)
    for c in range(chunks):
        x = logs[c]
        high = x.astype(jnp.bfloat16).astype(jnp.float32)
        mid = (x - high).astype(jnp.bfloat16).astype(jnp.float32)
        low = x - high - mid
        n = x.shape[0]
        pad = jnp.zeros((out_a.shape[1] - tok - 3 * n, LANES), jnp.float32)
        out_a[c, tok:, :] = jnp.concatenate([high, mid, low, pad], axis=0).astype(jnp.bfloat16)


def output_kernel(meta, own, partner, weight, mixed, log_total, left):
    t = meta[0]
    heads, tok = own.shape[0], mixed.shape[0]
    for j in range(heads):
        left[t * heads + j] = own[j, :tok, :]
        left[(1 - t) * heads + j] = partner[j, :tok, :]
    lhs = jnp.concatenate([left[i] for i in range(2 * heads)], axis=1)
    half = weight.shape[1] // 2
    rhs = jnp.concatenate(
        [weight[s, :half, :] for s in range(weight.shape[0])]
        + [weight[s, half:, :] for s in range(weight.shape[0])],
        axis=0,
    )
    mixed[...] = mm(lhs, rhs).astype(jnp.bfloat16)
    per = tok // LANES
    n = 2 * per
    for i in range(heads // 2):
        j = t * (heads // 2) + i
        rows = jnp.where(t == 1, own[j, tok:, :], partner[j, tok:, :]).astype(jnp.float32)
        x = rows[:n] + rows[n : 2 * n] + rows[2 * n : 3 * n]
        for h in range(2):
            log_total[2 * i + h : 2 * i + h + 1, :] = jnp.concatenate(
                [x[h * per + p : h * per + p + 1] for p in range(per)], axis=1
            )


def bf16_parts(x):
    high = lax.reduce_precision(x, 8, 7)
    mid = lax.reduce_precision(x - high, 8, 7)
    return jnp.stack([high, mid, x - high - mid]).astype(jnp.bfloat16)


def on_device_split(
    plan,
    tokens,
    input_norm_gain,
    mq_weight,
    mk_weight,
    mv_weight,
    mo_weight,
    gate_weight,
    gate_bias,
    decay_extra,
    m_gain,
    aq_weight,
    ak_weight,
    av_weight,
    sink_logit,
    out_m_weight,
    out_a_weight,
):
    sp, group, plane, lh, tok = (plan[n] for n in ("sp", "group", "plane", "lh", "tok"))
    width, rows = plan["width"], plan["rows"]
    half = rows // 2
    f32, bf16 = jnp.float32, jnp.bfloat16
    s = lax.axis_index("sp").astype(jnp.int32)
    t = lax.axis_index("tp").astype(jnp.int32)
    hi, j = s // group, s % group
    near_plane = (s // plane) % 2
    meta = jnp.stack([t, s % plane, jnp.where(j // lh == t, 0, 1), j % lh, hi]).astype(jnp.int32)
    swap = [(0, 1), (1, 0)]

    def flip(x):
        return lax.ppermute(x, "tp", swap)

    normed = rms_rows(tokens.astype(f32), input_norm_gain).astype(bf16)
    out_full = lax.all_gather(
        jnp.concatenate([out_m_weight, out_a_weight], axis=0), "sp", axis=0, tiled=True
    ).reshape(sp, 2 * out_m_weight.shape[0], out_m_weight.shape[1])

    cross = [
        (2 * a + (a // plane) % 2, 2 * (a ^ plane) + (a // plane) % 2) for a in range(sp)
    ]
    other = lax.ppermute(normed, ("sp", "tp"), cross)
    base = jnp.where(t == near_plane, normed, other)
    xs = [base] + [
        lax.ppermute(base, "sp", [(a, a ^ r) for a in range(sp)]) for r in range(1, plane)
    ]

    gate_rows = jnp.transpose(gate_weight.reshape(2, half, 4, lh), (0, 3, 2, 1)).reshape(
        2, lh, 4 * half // LANES, LANES
    )
    decay_rows = jnp.transpose(bf16_parts(decay_extra), (1, 2, 0, 3)).reshape(
        2, lh, 3 * tok // LANES, LANES
    )
    small = jnp.concatenate([gate_rows, decay_rows], axis=2)
    n_gate, n_small = gate_rows.shape[2], small.shape[2]
    n_rows = 6 * half + n_small
    packed = vmem_call(
        pack_kernel, jax.ShapeDtypeStruct((2, lh, n_rows, LANES), bf16), n_in=8
    )(mq_weight, mk_weight, mv_weight, mo_weight, aq_weight, ak_weight, av_weight, small)
    keep = lax.dynamic_index_in_dim(packed, t, 0, keepdims=False)
    got = flip(lax.dynamic_index_in_dim(packed, 1 - t, 0, keepdims=False))
    by_head = jnp.concatenate(
        [jnp.where(t == 0, keep, got), jnp.where(t == 0, got, keep)], axis=0
    )
    spread = jnp.concatenate([by_head, by_head], axis=0).reshape(sp * n_rows, LANES)
    own_w = lax.all_to_all(spread, "sp", 0, 0, tiled=True)
    partner_w = flip(own_w)
    own_w = own_w.reshape(sp, n_rows, LANES)
    partner_w = partner_w.reshape(sp, n_rows, LANES)
    small_both = jnp.stack([own_w[:, 6 * half :], partner_w[:, 6 * half :]])
    small_both = jnp.where(t == 0, small_both, small_both[::-1])
    gate_t = jnp.transpose(small_both[:, :, :n_gate].reshape(2, sp, 4, half), (2, 1, 0, 3))
    gate_t = jnp.pad(gate_t.reshape(4, width), ((0, 12), (0, 0)))
    first = (2 * hi + t) * plane
    decay = lax.dynamic_slice_in_dim(small_both[:, :, n_gate:], first, plane, 1)
    decay = jnp.sum(decay.reshape(2, plane, 3, tok).astype(f32), axis=2)
    decay = jnp.transpose(decay, (1, 0, 2))
    params = jnp.concatenate(
        [m_gain, gate_bias.reshape(-1), sink_logit, jnp.zeros((LANES - 6 * lh,), f32)]
    ).reshape(-1, LANES)
    params = jnp.stack([params, flip(params)])
    gain = params[:, :lh]
    bias = params[:, lh, : 4 * lh]
    sink = params[:, lh, 4 * lh : 6 * lh]

    quarter = plane * tok
    cols = 6 * LANES
    proj, gates, summary, halo = vmem_call(
        project_kernel,
        (
            jax.ShapeDtypeStruct((quarter, cols), bf16),
            jax.ShapeDtypeStruct((plane, 8, tok), f32),
            jax.ShapeDtypeStruct((2, M_DIM + 8, LANES), f32),
            jax.ShapeDtypeStruct((2, WINDOW, LANES), f32),
        ),
        scratch=[pltpu.VMEM((width, cols), bf16)],
        smem=2,
        n_in=plane + 4,
        flops=2 * quarter * width * cols,
    )(meta, bias, *xs, own_w, partner_w, gate_t, decay)
    both = flip(jnp.concatenate([summary, halo], axis=1))
    partner_sum, partner_halo = both[:, : M_DIM + 8], both[:, M_DIM + 8 :]
    sent = vmem_call(
        combine_kernel,
        jax.ShapeDtypeStruct((M_DIM + 8 + WINDOW, LANES), f32),
        smem=1,
        n_in=3,
    )(meta, summary, partner_sum, partner_halo)
    across = lax.ppermute(sent, "sp", [(a, (a + group) % sp) for a in range(sp)])
    part = jax.ShapeDtypeStruct((plane, tok + 16, LANES), bf16)
    out_m, out_a = vmem_call(
        mixer_kernel,
        (part, part),
        scratch=[
            pltpu.VMEM((quarter + 2 * WINDOW, LANES), bf16),
            pltpu.VMEM((plane, 2 * tok // WINDOW, LANES), f32),
        ],
        smem=2,
        n_in=6,
        flops=2 * quarter * width * cols,
    )(meta, sink, proj, gates, partner_sum, partner_halo, across, gain)

    lead = jnp.where(t == 0, out_m, out_a)
    got = flip(jnp.where(t == 0, out_a, out_m))
    spread = jnp.concatenate(
        [jnp.where(t == 0, lead, got), jnp.where(t == 0, got, lead)], axis=0
    ).reshape(group * (tok + 16), LANES)
    groups = [list(range(g * group, (g + 1) * group)) for g in range(sp // group)]
    mine = lax.all_to_all(spread, "sp", 0, 0, axis_index_groups=groups, tiled=True)
    theirs = flip(mine)
    shape = (group, tok + 16, LANES)
    return vmem_call(
        output_kernel,
        (
            jax.ShapeDtypeStruct((tok, out_m_weight.shape[1]), bf16),
            jax.ShapeDtypeStruct((2 * lh, tok), f32),
        ),
        scratch=[pltpu.VMEM((2 * group, tok, LANES), bf16)],
        smem=1,
        n_in=3,
        flops=2 * tok * width * out_m_weight.shape[1],
    )(meta, mine.reshape(shape), theirs.reshape(shape), out_full)


def solution(mesh):
    in_specs = (
        P("sp", None),
        P(),
        P("sp", "tp"),
        P("sp", "tp"),
        P("sp", "tp"),
        P("sp", "tp"),
        P("sp", None, "tp"),
        P(None, "tp"),
        P(None, "tp", "sp"),
        P("tp"),
        P("sp", "tp"),
        P("sp", "tp"),
        P("sp", "tp"),
        P("tp"),
        P("sp", "tp"),
        P("sp", "tp"),
    )
    out_specs = (P("sp", "tp"), P("tp", "sp"))
    def per_device(*args):
        plan = split_plan(mesh, args)
        return on_device(*args) if plan is None else on_device_split(plan, *args)

    return jax.shard_map(
        per_device, mesh=mesh, in_specs=in_specs, out_specs=out_specs, check_vma=False
    )
```

```python
import jax
import jax.numpy as jnp
from jax import lax
from jax.experimental import pallas as pl
from jax.experimental.pallas import tpu as pltpu
from jax.sharding import PartitionSpec as P

M_DIM = 128
W_DIM = 64
WINDOW = 128
M_BLOCK = 64


EPS = 1e-06
FLOOR_LOG = -1e30
HIGHEST = lax.Precision.HIGHEST


def with_halo(x, sides, width):
    for axis, dim in sides:
        peers, length = (lax.axis_size(axis), x.shape[dim])
        up = [(i, (i + 1) % peers) for i in range(peers - 1)]
        down = [(j, i) for i, j in up]
        last = lax.slice_in_dim(x, length - width, length, axis=dim)
        first = lax.slice_in_dim(x, 0, width, axis=dim)
        before = lax.ppermute(last, axis, up)
        after = lax.ppermute(first, axis, down)
        x = jnp.concatenate([before, x, after], axis=dim)
    return x


def rms_rows(inputs, gain_vec):
    return inputs * lax.rsqrt(jnp.mean(inputs * inputs, axis=-1, keepdims=True) + EPS) * gain_vec


def stored(result):
    return lax.optimization_barrier(result.astype(jnp.bfloat16))


def flip_tokens(array_in):
    return jnp.flip(array_in, axis=1)


def block_pass(queries, key_vecs, value_vecs, in_gate, log_forget, start_state):
    head_count, length, head_width = queries.shape
    block_count = length // M_BLOCK

    def blocks(array_in):
        return jnp.moveaxis(
            array_in.reshape((head_count, block_count, M_BLOCK) + array_in.shape[2:]), 1, 0
        )

    lower_mask = jnp.tril(jnp.ones((M_BLOCK, M_BLOCK), dtype=bool))

    def advance(state_in, block_in):
        cell_mat, norm_vec, stab_max = state_in
        q_blk, k_blk, v_blk, i_blk, f_blk = block_in
        cum_log = jnp.cumsum(f_blk, axis=-1)
        seg_total = cum_log[:, -1]
        log_end = seg_total[:, None] - cum_log + i_blk
        max_next = jnp.maximum(seg_total + stab_max, jnp.max(log_end, axis=-1))
        w_end = jnp.exp(log_end - max_next[:, None])
        fade_old = jnp.exp(seg_total + stab_max - max_next)
        cell_next = fade_old[:, None, None] * cell_mat + jnp.einsum(
            "hsv,hsk->hvk", w_end[:, :, None] * v_blk, k_blk, precision=HIGHEST
        )
        norm_next = fade_old[:, None] * norm_vec + jnp.einsum(
            "hs,hsk->hk", w_end, k_blk, precision=HIGHEST
        )
        log_w = jnp.where(
            lower_mask, cum_log[:, :, None] - cum_log[:, None, :] + i_blk[:, None, :], -jnp.inf
        )
        log_inter = cum_log + stab_max[:, None]
        row_max = jnp.maximum(log_inter, jnp.max(log_w, axis=-1))
        w_intra = jnp.exp(log_w - row_max[:, :, None])
        w_inter = jnp.exp(log_inter - row_max)
        scores = jnp.einsum("htk,hsk->hts", q_blk, k_blk, precision=HIGHEST) * w_intra
        numerator = jnp.einsum("hts,hsv->htv", scores, v_blk, precision=HIGHEST) + w_inter[
            ..., None
        ] * jnp.einsum("hvk,htk->htv", cell_mat, q_blk, precision=HIGHEST)
        denominator = jnp.sum(scores, axis=-1) + w_inter * jnp.einsum(
            "hk,htk->ht", norm_vec, q_blk, precision=HIGHEST
        )
        result_rows = numerator / jnp.maximum(jnp.abs(denominator), jnp.exp(-row_max))[..., None]
        return ((cell_next, norm_next, max_next), result_rows)

    final_state, outputs = lax.scan(
        advance,
        start_state,
        tuple(
            (blocks(array_in) for array_in in (queries, key_vecs, value_vecs, in_gate, log_forget))
        ),
    )
    return (jnp.moveaxis(outputs, 0, 1).reshape(head_count, length, head_width), final_state)


def summarize(key_vecs, value_vecs, in_gate, log_forget):
    cum_log = jnp.cumsum(log_forget, axis=-1)
    seg_total = cum_log[:, -1]
    log_end = seg_total[:, None] - cum_log + in_gate
    peak_log = jnp.max(log_end, axis=-1)
    weights_end = jnp.exp(log_end - peak_log[:, None])
    cell_mat = jnp.einsum(
        "hsv,hsk->hvk", weights_end[:, :, None] * value_vecs, key_vecs, precision=HIGHEST
    )
    norm_vec = jnp.einsum("hs,hsk->hk", weights_end, key_vecs, precision=HIGHEST)
    return (seg_total, cell_mat, norm_vec, peak_log)


def merge_side(state_in, cell_mats, norm_vecs, logs, usable):
    cell_mat, norm_vec, peak_log = state_in
    masked = jnp.where(usable, logs, FLOOR_LOG)
    new_peak = jnp.maximum(peak_log, jnp.max(masked, axis=0))
    scales = jnp.where(usable, jnp.exp(masked - new_peak[None]), 0.0)
    cell_mat = jnp.einsum("jh,jhvk->hvk", scales, cell_mats, precision=HIGHEST)
    norm_vec = jnp.einsum("jh,jhk->hk", scales, norm_vecs, precision=HIGHEST)
    return (cell_mat, norm_vec, new_peak)


def gather_states(forward_sum, backward_sum):
    decay_all = (
        lax.all_gather(forward_sum[0][None], "sp", axis=0, tiled=True),
        lax.all_gather(backward_sum[0][None], "sp", axis=0, tiled=True),
    )
    own_index = lax.axis_index("sp")
    acc_fwd = jnp.cumsum(decay_all[0], axis=0)
    acc_bwd = jnp.cumsum(decay_all[1], axis=0)
    before_own = lax.dynamic_index_in_dim(acc_fwd - decay_all[0], own_index, 0, keepdims=False)
    after_own = lax.dynamic_index_in_dim(acc_bwd, own_index, 0, keepdims=False)
    lead_bwd = acc_bwd - decay_all[1]
    empty_side = (
        jnp.zeros_like(forward_sum[1]),
        jnp.zeros_like(forward_sum[2]),
        jnp.full_like(forward_sum[3], FLOOR_LOG),
    )
    state_in = empty_side + empty_side
    pieces = (
        lax.all_gather(forward_sum[1][None], "sp", axis=0, tiled=True),
        lax.all_gather(forward_sum[2][None], "sp", axis=0, tiled=True),
        lax.all_gather(forward_sum[3][None], "sp", axis=0, tiled=True),
        lax.all_gather(backward_sum[1][None], "sp", axis=0, tiled=True),
        lax.all_gather(backward_sum[2][None], "sp", axis=0, tiled=True),
        lax.all_gather(backward_sum[3][None], "sp", axis=0, tiled=True),
    )
    piece_count = pieces[0].shape[0]
    device_ids = jnp.arange(piece_count, dtype=jnp.int32)
    log_fwd = before_own[None] - acc_fwd + pieces[2]
    log_bwd = lead_bwd - after_own[None] + pieces[5]
    left_side = merge_side(
        state_in[:3], pieces[0], pieces[1], log_fwd, (device_ids < own_index)[:, None]
    )
    right_side = merge_side(
        state_in[3:], pieces[3], pieces[4], log_bwd, (device_ids > own_index)[:, None]
    )
    states = left_side + right_side
    return (states[:3], states[3:])


def window_attend(a_query, kv_pairs, sink_logit, first_row, total_rows):
    tok_rows = a_query.shape[0]
    block_len = WINDOW
    block_count = tok_rows // block_len
    kv_width = kv_pairs.shape[1] // 2
    kv_heads = kv_width // W_DIM
    q_heads = a_query.shape[1] // W_DIM
    groups = q_heads // kv_heads
    filled_margin = with_halo(kv_pairs, (("sp", 0),), WINDOW)
    windows = jnp.concatenate(
        [
            filled_margin[place_idx * block_len : place_idx * block_len + tok_rows].reshape(
                block_count, block_len, 2 * kv_width
            )
            for place_idx in range(3)
        ],
        axis=1,
    )
    key_block = windows[:, :, :kv_width].reshape(block_count, 3 * block_len, kv_heads, W_DIM)
    content_tile = windows[:, :, kv_width:].reshape(block_count, 3 * block_len, kv_heads, W_DIM)
    query_block = a_query.reshape(block_count, block_len, kv_heads, groups, W_DIM)
    scores = jnp.einsum(
        "nqgrd,nkgd->ngrqk", query_block, key_block, preferred_element_type=jnp.float32
    ) * W_DIM ** (-0.5)
    query_off = jnp.arange(block_len, dtype=jnp.int32)
    key_off = jnp.arange(3 * block_len, dtype=jnp.int32) - block_len
    in_window = jnp.abs(query_off[:, None] - key_off[None, :]) <= WINDOW
    key_place = (
        first_row + jnp.arange(block_count, dtype=jnp.int32)[:, None] * block_len + key_off[None, :]
    )
    inside = (key_place >= 0) & (key_place < total_rows)
    usable = in_window[None] & inside[:, None, :]
    scores = jnp.where(usable[:, None, None], scores, -jnp.inf)
    sink_col = sink_logit.reshape(kv_heads, groups)[None, :, :, None]
    peak_log = jnp.maximum(sink_col, jnp.max(scores, axis=-1))
    weights_exp = jnp.exp(scores - peak_log[..., None])
    weight_total_sum = jnp.exp(sink_col - peak_log) + jnp.sum(weights_exp, axis=-1)
    weighted = jnp.einsum(
        "ngrqk,nkgd->nqgrd",
        weights_exp.astype(jnp.bfloat16),
        content_tile,
        preferred_element_type=jnp.float32,
    )
    scale_back = jnp.transpose(weight_total_sum, (0, 3, 1, 2))[..., None]
    mixed_rows = (weighted / scale_back).astype(jnp.bfloat16).reshape(tok_rows, q_heads * W_DIM)
    log_total = jnp.transpose(peak_log + jnp.log(weight_total_sum), (1, 2, 0, 3)).reshape(
        q_heads, tok_rows
    )
    return (mixed_rows, log_total)


def on_device(
    tokens,
    input_norm_gain,
    mq_weight,
    mk_weight,
    mv_weight,
    mo_weight,
    gate_weight,
    gate_bias,
    decay_extra,
    m_gain,
    aq_weight,
    ak_weight,
    av_weight,
    sink_logit,
    out_m_weight,
    out_a_weight,
):
    tok_rows = tokens.shape[0]
    normed = rms_rows(tokens.astype(jnp.float32), input_norm_gain).astype(jnp.bfloat16)
    local_heads = gate_weight.shape[2]
    gate_cols = 4 * local_heads
    pieces = (
        lax.all_gather(mq_weight, "sp", axis=0, tiled=True),
        lax.all_gather(mk_weight, "sp", axis=0, tiled=True),
        lax.all_gather(mv_weight, "sp", axis=0, tiled=True),
        lax.all_gather(mo_weight, "sp", axis=0, tiled=True),
        lax.all_gather(gate_weight, "sp", axis=0, tiled=True),
        lax.all_gather(aq_weight, "sp", axis=0, tiled=True),
        lax.all_gather(ak_weight, "sp", axis=0, tiled=True),
        lax.all_gather(av_weight, "sp", axis=0, tiled=True),
    )
    piece_rows = pieces[0].shape[0]
    flat_gate = pieces[4].reshape(piece_rows, gate_cols)
    segments = (
        pieces[0],
        pieces[1],
        pieces[2],
        pieces[3],
        flat_gate,
        pieces[5],
        pieces[6],
        pieces[7],
    )
    projected = tuple(
        (jnp.dot(normed, segment, preferred_element_type=jnp.float32) for segment in segments)
    )
    m_query = stored(projected[0])
    m_key = stored(projected[1])
    m_value = stored(projected[2])
    m_out = stored(projected[3])
    gates = projected[4].reshape(tok_rows, 4, local_heads) + gate_bias[None]

    def heads_first(matrix):
        return jnp.transpose(
            matrix.astype(jnp.float32).reshape(tok_rows, local_heads, M_DIM), (1, 0, 2)
        )

    queries = heads_first(m_query)
    key_vecs = heads_first(m_key) * M_DIM ** (-0.5)
    value_vecs = heads_first(m_value)
    in_fwd = gates[:, 0, :].T
    forget_fwd = jax.nn.log_sigmoid(gates[:, 1, :].T) + decay_extra[0]
    in_bwd = flip_tokens(gates[:, 2, :].T)
    forget_bwd = flip_tokens(jax.nn.log_sigmoid(gates[:, 3, :].T) + decay_extra[1])
    queries_bwd = flip_tokens(queries)
    keys_bwd = flip_tokens(key_vecs)
    values_bwd = flip_tokens(value_vecs)
    forward_sum = summarize(key_vecs, value_vecs, in_fwd, forget_fwd)
    backward_sum = summarize(keys_bwd, values_bwd, in_bwd, forget_bwd)
    state_fwd, state_bwd = gather_states(forward_sum, backward_sum)
    hidden_fwd, _ = block_pass(queries, key_vecs, value_vecs, in_fwd, forget_fwd, state_fwd)
    hidden_bwd, _ = block_pass(queries_bwd, keys_bwd, values_bwd, in_bwd, forget_bwd, state_bwd)
    cell_out = hidden_fwd + flip_tokens(hidden_bwd)
    gate_open = jax.nn.sigmoid(m_out.astype(jnp.float32)).reshape(tok_rows, local_heads, M_DIM)
    cell_rows = jnp.transpose(cell_out, (1, 0, 2)) * gate_open
    mixed_m = (
        rms_rows(cell_rows, m_gain.reshape(local_heads, M_DIM))
        .astype(jnp.bfloat16)
        .reshape(tok_rows, local_heads * M_DIM)
    )
    a_query = stored(projected[5])
    kv_pairs = jnp.concatenate([stored(projected[6]), stored(projected[7])], axis=1)
    first_row = lax.axis_index("sp") * tok_rows
    total_rows = tok_rows * lax.axis_size("sp")
    mixed_a, log_total = window_attend(a_query, kv_pairs, sink_logit, first_row, total_rows)
    full_m, full_a = (
        lax.all_gather(mixed_m, "tp", axis=1, tiled=True),
        lax.all_gather(mixed_a, "tp", axis=1, tiled=True),
    )
    pieces = (
        lax.all_gather(out_m_weight, "sp", axis=0, tiled=True),
        lax.all_gather(out_a_weight, "sp", axis=0, tiled=True),
    )
    running = jnp.dot(full_m, pieces[0], preferred_element_type=jnp.float32)
    mixed = running + jnp.dot(full_a, pieces[1], preferred_element_type=jnp.float32)
    return (mixed.astype(jnp.bfloat16), log_total)


CHUNK = 256
LANES = 128
EMPTY = -1e30


def split_plan(mesh, args):
    sp, tp = mesh.shape["sp"], mesh.shape["tp"]
    tok_rows, width = args[0].shape
    rows = args[2].shape[0]
    local_heads = args[6].shape[2]
    group = local_heads * tp
    if tp != 2 or sp != 2 * group or group % 4 or (group // 2) & (group // 2 - 1):
        return None
    plane = group // 2
    ok = (
        args[2].shape[1] == local_heads * M_DIM
        and args[10].shape[1] == local_heads * LANES
        and args[11].shape[1] == local_heads * W_DIM
        and args[12].shape[1] == local_heads * W_DIM
        and 2 * W_DIM == LANES
        and M_DIM == LANES
        and WINDOW == LANES
        and tok_rows == CHUNK
        and rows == LANES
        and args[14].shape[0] * sp == group * M_DIM
        and args[15].shape[0] * sp == group * LANES
    )
    if not ok:
        return None
    return dict(
        sp=sp, tp=tp, tok=tok_rows, width=width, rows=rows, lh=local_heads, group=group, plane=plane
    )


def mm(a, b, ca=1, cb=0, precision=None):
    return lax.dot_general(
        a, b, (((ca,), (cb,)), ((), ())), precision=precision, preferred_element_type=jnp.float32
    )


def vmem_call(kernel, outs, scratch=(), smem=0, n_in=0, flops=0, n_any=0, n_tail=0):
    return pl.pallas_call(
        kernel,
        out_shape=outs,
        in_specs=[pl.BlockSpec(memory_space=pltpu.SMEM)] * smem
        + [pl.BlockSpec(memory_space=pltpu.VMEM)] * n_in
        + [pl.BlockSpec(memory_space=pl.ANY)] * n_any
        + [pl.BlockSpec(memory_space=pltpu.VMEM)] * n_tail,
        out_specs=jax.tree.map(lambda _: pl.BlockSpec(memory_space=pltpu.VMEM), outs),
        scratch_shapes=scratch,
        cost_estimate=pl.CostEstimate(flops=flops, bytes_accessed=0, transcendentals=0),
        compiler_params=pltpu.CompilerParams(vmem_limit_bytes=56 * 1024 * 1024),
    )


def pack_kernel(meta, mq, mk, mv, mo, aq, ak, av, small, keep, send):
    t = meta[0]
    copies, heads = keep.shape[0], keep.shape[2]
    rows = mq.shape[0] // 2
    at = pl.multiple_of(t * rows, rows)
    away = pl.multiple_of((1 - t) * rows, rows)
    for h in range(heads):
        lanes = slice(h * LANES, (h + 1) * LANES)
        narrow = slice(h * W_DIM, (h + 1) * W_DIM)
        for start, mine in ((at, True), (away, False)):
            parts = [ref[pl.ds(start, rows), lanes] for ref in (mq, mk, mv, mo, aq)]
            parts.append(
                jnp.concatenate([ref[pl.ds(start, rows), narrow] for ref in (ak, av)], axis=1)
            )
            parts.append(small[t if mine else 1 - t, h])
            row = 0
            for part in parts:
                span = slice(row, row + part.shape[0])
                row += part.shape[0]
                if mine:
                    for i in range(copies):
                        keep[i, t, h, span, :] = part
                else:
                    send[h, span, :] = part


def chunk_vecs(rows):
    n = rows.shape[1]
    r = lax.broadcasted_iota(jnp.int32, (n, n), 0)
    c = lax.broadcasted_iota(jnp.int32, (n, n), 1)
    lower = jnp.where(r >= c, 1.0, 0.0).astype(jnp.float32)
    eye = jnp.where(r == c, 1.0, 0.0).astype(jnp.float32)
    cum_col = mm(lower, rows, 1, 1, HIGHEST)
    raw_col = mm(eye, rows, 1, 1, HIGHEST)
    cum_row = mm(rows, lower, 1, 1, HIGHEST)
    f_col, f_row = cum_col[:, 1:2], cum_row[1:2]
    e_col = cum_col[:, 3:4] - raw_col[:, 3:4]
    e_row = cum_row[3:4] - rows[3:4]
    fwd = (f_col, rows[0:1] - f_row, raw_col[:, 0:1] - f_col, cum_row[1:2, n - 1 : n])
    bwd = (-e_col, rows[2:3] + e_row, raw_col[:, 2:3] + e_col, cum_row[3:4, n - 1 : n])
    return fwd, bwd


def advance_state(state, key, value, end_col, end_row, total):
    cell, norm, peak = state
    new_peak = jnp.maximum(total + peak, jnp.max(end_row, axis=1, keepdims=True))
    weighted = key * jnp.exp(end_col - new_peak)
    fade = jnp.exp(total + peak - new_peak)
    cell = fade * cell + mm(weighted.astype(jnp.bfloat16), value, 0, 0)
    norm = fade * norm + jnp.sum(weighted, axis=0, keepdims=True)
    return cell, norm, new_peak


def forward_state(state, key, value, vecs):
    return advance_state(state, key, value, vecs[2] + vecs[3], vecs[1] + vecs[3], vecs[3])


def backward_state(state, key, value, vecs):
    return advance_state(state, key, value, vecs[2], vecs[1], vecs[3])


def empty_state():
    return (
        jnp.zeros((M_DIM, M_DIM), jnp.float32),
        jnp.zeros((1, M_DIM), jnp.float32),
        jnp.full((1, 1), EMPTY, jnp.float32),
    )


def project_kernel(meta, bias, *refs):
    plane = (len(refs) - 11) // 2
    same, other = refs[:plane], refs[plane : 2 * plane]
    own, partner, gate_t, decay, proj, gates, summary, weight, xs, raw, sems = refs[2 * plane :]
    t, k, sel, jl, near = meta[0], meta[1], meta[2], meta[3], meta[5]
    copies = [
        pltpu.make_async_copy(own, raw.at[0], sems.at[plane]),
        pltpu.make_async_copy(partner, raw.at[1], sems.at[plane + 1]),
    ]
    for copy in copies:
        copy.start()

    @pl.when(t == near)
    def _():
        for r in range(plane):
            pltpu.make_async_copy(same[r], xs.at[r], sems.at[r]).start()

    @pl.when(t != near)
    def _():
        for r in range(plane):
            pltpu.make_async_copy(other[r], xs.at[r], sems.at[r]).start()

    for copy in copies:
        copy.wait()
    sources = own.shape[0]
    rows = weight.shape[0] // sources // 2
    cols = weight.shape[1] // LANES
    for i in range(sources):
        for c in range(cols):
            lanes = slice(c * LANES, (c + 1) * LANES)
            span = slice(c * rows, (c + 1) * rows)
            first = pl.multiple_of((2 * i + t) * rows, rows)
            second = pl.multiple_of((2 * i + 1 - t) * rows, rows)
            weight[pl.ds(first, rows), lanes] = raw[0, i, span, :]
            weight[pl.ds(second, rows), lanes] = raw[1, i, span, :]
    tok = xs.shape[1]
    for r in range(plane):
        pltpu.make_async_copy(same[r], xs.at[r], sems.at[r]).wait()
        at = pl.ds(pl.multiple_of((k ^ r) * tok, tok), tok)
        proj[at, :] = mm(xs[r], weight[...]).astype(jnp.bfloat16)
        gates[k ^ r] = jnp.transpose(mm(xs[r], gate_t[...], 1, 1))[:8]
    heads = bias.shape[1] // 4
    b = [bias[sel, g * heads + jl] for g in range(4)]
    lead = jnp.concatenate([jnp.full((1, tok), b[g], jnp.float32) for g in range(4)], axis=0)
    forget = lax.broadcasted_iota(jnp.int32, (4, tok), 0) % 2 == 1
    fwd, bwd = empty_state(), empty_state()
    total_f = jnp.zeros((1, 1), jnp.float32)
    total_b = jnp.zeros((1, 1), jnp.float32)
    chunks = []
    for c in range(plane):
        g = gates[c][:4] + lead
        d = decay[c]
        extra = jnp.concatenate([d[0:1], d[0:1], d[1:2], d[1:2]], axis=0)
        logs = jnp.minimum(g, 0.0) - jnp.log1p(jnp.exp(-jnp.abs(g))) + extra
        g = jnp.where(forget, logs, g)
        gates[c] = jnp.concatenate([g, jnp.zeros((4, tok), jnp.float32)], axis=0)
        vecs = chunk_vecs(gates[c])
        span = slice(c * tok, (c + 1) * tok)
        key = proj[span, LANES : 2 * LANES].astype(jnp.float32)
        value = proj[span, 2 * LANES : 3 * LANES]
        chunks.append((key, value, vecs))
    for key, value, vecs in chunks:
        fwd = forward_state(fwd, key, value, vecs[0])
        total_f = total_f + vecs[0][3]
    for key, value, vecs in chunks[::-1]:
        bwd = backward_state(bwd, key, value, vecs[1])
        total_b = total_b + vecs[1][3]
    for i, ((cell, norm, peak), total) in enumerate(((fwd, total_f), (bwd, total_b))):
        summary[i, :M_DIM, :] = cell
        summary[i, M_DIM : M_DIM + 8, :] = jnp.concatenate(
            [
                norm,
                jnp.broadcast_to(peak, (1, LANES)),
                jnp.broadcast_to(total, (1, LANES)),
                jnp.zeros((5, LANES), jnp.float32),
            ],
            axis=0,
        )
    last = proj.shape[0]
    summary[0, M_DIM + 8 :, :] = proj[:WINDOW, 5 * LANES :].astype(jnp.float32)
    summary[1, M_DIM + 8 :, :] = proj[last - WINDOW :, 5 * LANES :].astype(jnp.float32)


def read_state(ref, i):
    return (
        ref[i, :M_DIM, :],
        ref[i, M_DIM : M_DIM + 1, :],
        ref[i, M_DIM + 1 : M_DIM + 2, 0:1],
        ref[i, M_DIM + 2 : M_DIM + 3, 0:1],
    )


def merge_states(earlier, later, later_total):
    peak = jnp.maximum(later_total + earlier[2], later[2])
    old = jnp.exp(later_total + earlier[2] - peak)
    new = jnp.exp(later[2] - peak)
    return old * earlier[0] + new * later[0], old * earlier[1] + new * later[1], peak


def combine_kernel(meta, own, partner, out):
    t, hi = meta[0], meta[4]
    forward = hi == 0
    i = jnp.where(forward, 0, 1)
    mine, other = read_state(own, i), read_state(partner, i)
    mine_later = (t == 1) == forward
    a = tuple(jnp.where(mine_later, y, x) for x, y in zip(mine, other))
    b = tuple(jnp.where(mine_later, x, y) for x, y in zip(mine, other))
    cell, norm, peak = merge_states(a[:3], b[:3], b[3])
    out[:M_DIM, :] = cell
    out[M_DIM : M_DIM + 8, :] = jnp.concatenate(
        [norm, jnp.broadcast_to(peak, (1, LANES)), jnp.zeros((6, LANES), jnp.float32)], axis=0
    )
    out[M_DIM + 8 :, :] = partner[jnp.where(forward, 1, 0), M_DIM + 8 :, :]


def mixer_kernel(meta, sink, proj, gates, partner, across, gain, keep, send, kv, logs):
    t, sel, jl, hi = meta[0], meta[2], meta[3], meta[4]
    chunks = gates.shape[0]
    tok = gates.shape[2]
    far = (
        across[:M_DIM, :],
        across[M_DIM : M_DIM + 1, :],
        across[M_DIM + 1 : M_DIM + 2, 0:1],
    )

    def incoming(i, use_far, use_near):
        near = read_state(partner, i)
        far_peak = jnp.where(use_far, far[2], EMPTY)
        near_peak = jnp.where(use_near, near[2], EMPTY)
        near_total = jnp.where(use_near, near[3], 0.0)
        return merge_states((far[0], far[1], far_peak), (near[0], near[1], near_peak), near_total)

    scale = M_DIM ** (-0.5)
    fwd = incoming(0, hi == 1, t == 1)
    bwd = incoming(1, hi == 0, t == 0)
    vecs = [chunk_vecs(gates[c]) for c in range(chunks)]

    def kv_of(c):
        span = slice(c * tok, (c + 1) * tok)
        return (
            proj[span, LANES : 2 * LANES].astype(jnp.float32),
            proj[span, 2 * LANES : 3 * LANES],
        )

    def store(is_cell, c, span, value):
        @pl.when((t == 0) == is_cell)
        def _():
            keep[t, c, span, :] = value

        @pl.when((t == 0) != is_cell)
        def _():
            send[c, span, :] = value


    back_states = [None] * chunks
    for c in range(chunks - 1, -1, -1):
        back_states[c] = bwd
        if c:
            bwd = backward_state(bwd, *kv_of(c), vecs[c][1])
    r = lax.broadcasted_iota(jnp.int32, (tok, tok), 0)
    col = lax.broadcasted_iota(jnp.int32, (tok, tok), 1)
    gain_row = gain[sel, pl.ds(jl, 1), :]
    for c in range(chunks):
        span = slice(c * tok, (c + 1) * tok)
        q = proj[span, :LANES]
        qf = q.astype(jnp.float32)
        scores = mm(q, proj[span, LANES : 2 * LANES], 1, 1) * scale
        total_w = None
        inter = None
        for state, vec, mask in ((fwd, vecs[c][0], r >= col), (back_states[c], vecs[c][1], r <= col)):
            cell, norm, peak = state
            lead_col, src_row = vec[0], vec[1]
            if mask is not None and vec is vecs[c][1]:
                reach = peak + vec[3]
            else:
                reach = peak
            masked = jnp.where(mask, src_row, EMPTY)
            top = jnp.maximum(jnp.max(masked, axis=1, keepdims=True), reach)
            w = jnp.exp(masked - top)
            w_in = jnp.exp(reach - top)
            denom = jnp.sum(scores * w, axis=1, keepdims=True) + w_in * scale * jnp.sum(
                qf * norm, axis=1, keepdims=True
            )
            inv = 1.0 / jnp.maximum(jnp.abs(denom), jnp.exp(-(lead_col + top)))
            part = w * inv
            high = cell.astype(jnp.bfloat16)
            low = (cell - high.astype(jnp.float32)).astype(jnp.bfloat16)
            add = (mm(q, high) + mm(q, low)) * (scale * w_in * inv)
            total_w = part if total_w is None else total_w + part
            inter = add if inter is None else inter + add
        key, value = kv_of(c)
        cell_out = mm((scores * total_w).astype(jnp.bfloat16), value) + inter
        fwd = forward_state(fwd, key, value, vecs[c][0])
        gate = proj[span, 3 * LANES : 4 * LANES].astype(jnp.float32)
        u = cell_out / (1.0 + jnp.exp(-gate))
        u = u * lax.rsqrt(jnp.mean(u * u, axis=1, keepdims=True) + EPS) * gain_row
        store(True, c, slice(0, tok), u.astype(jnp.bfloat16))
        store(True, c, slice(tok, tok + 16), jnp.zeros((16, LANES), jnp.bfloat16))

    length = proj.shape[0]
    inner_edge = partner[jnp.where(t == 0, 0, 1), M_DIM + 8 :, :].astype(jnp.bfloat16)
    outer_edge = across[M_DIM + 8 :, :].astype(jnp.bfloat16)
    kv[:WINDOW, :] = jnp.where(t == 0, outer_edge, inner_edge)
    kv[WINDOW : WINDOW + length, :] = proj[:, 5 * LANES :]
    kv[WINDOW + length :, :] = jnp.where(t == 0, inner_edge, outer_edge)
    at_start = (hi == 0) & (t == 0)
    at_end = (hi == 1) & (t == 1)
    qi = lax.broadcasted_iota(jnp.int32, (WINDOW, 3 * WINDOW), 0)
    ki = lax.broadcasted_iota(jnp.int32, (WINDOW, 3 * WINDOW), 1) - WINDOW
    band = jnp.abs(ki - qi) <= WINDOW
    diag = lax.broadcasted_iota(jnp.int32, (WINDOW, WINDOW), 0) == lax.broadcasted_iota(
        jnp.int32, (WINDOW, WINDOW), 1
    )
    blocks = length // WINDOW
    per = tok // WINDOW
    for b in range(blocks):
        usable = band
        if b == 0:
            usable = usable & ((ki >= 0) | jnp.logical_not(at_start))
        if b == blocks - 1:
            usable = usable & ((ki < WINDOW) | jnp.logical_not(at_end))
        keys = kv[b * WINDOW : (b + 3) * WINDOW, :W_DIM]
        values = kv[b * WINDOW : (b + 3) * WINDOW, W_DIM:]
        mixed = []
        for h in range(2):
            lanes = slice(4 * LANES + h * W_DIM, 4 * LANES + (h + 1) * W_DIM)
            q = proj[b * WINDOW : (b + 1) * WINDOW, lanes]
            s = mm(q, keys, 1, 1) * W_DIM ** (-0.5)
            s = jnp.where(usable, s, EMPTY)
            sink_h = sink[sel, 2 * jl + h]
            peak = jnp.maximum(jnp.max(s, axis=1, keepdims=True), sink_h)
            e = jnp.exp(s - peak)
            total = jnp.exp(sink_h - peak) + jnp.sum(e, axis=1, keepdims=True)
            mixed.append(mm(e.astype(jnp.bfloat16), values) / total)
            log_col = peak + jnp.log(total)
            log_row = jnp.sum(jnp.where(diag, log_col, 0.0), axis=0, keepdims=True)
            at = h * per + b % per
            logs[b // per, at : at + 1, :] = log_row
        span = slice((b % per) * WINDOW, (b % per + 1) * WINDOW)
        store(False, b // per, span, jnp.concatenate(mixed, axis=1).astype(jnp.bfloat16))
    for c in range(chunks):
        x = logs[c]
        high = x.astype(jnp.bfloat16).astype(jnp.float32)
        mid = (x - high).astype(jnp.bfloat16).astype(jnp.float32)
        low = x - high - mid
        n = x.shape[0]
        pad = jnp.zeros((16 - 3 * n, LANES), jnp.float32)
        tail = jnp.concatenate([high, mid, low, pad], axis=0).astype(jnp.bfloat16)
        store(False, c, slice(tok, tok + 16), tail)


def output_kernel(meta, own, partner, *refs):
    mixed, log_total, left, weight, sems = refs[-5:]
    blocks = refs[:-5]
    t, p, z = meta[0], meta[1], meta[6]
    plane = len(blocks)
    heads, tok = own.shape[0], mixed.shape[0]
    planes = sems.shape[0] // plane
    rows = blocks[0].shape[0] // planes
    half = rows // 2
    total = weight.shape[0] // 2
    copies = []
    for r in range(plane):
        for zr in range(planes):
            source = (z ^ zr) * plane + (p ^ r)
            for i in range(2):
                to = pl.multiple_of(i * total + source * half, half)
                copies.append(
                    pltpu.make_async_copy(
                        blocks[r].at[pl.ds(zr * rows + i * half, half)],
                        weight.at[pl.ds(to, half)],
                        sems.at[r * planes + zr, i],
                    )
                )
    for copy in copies:
        copy.start()
    for j in range(heads):
        left[t * heads + j] = own[j, :tok, :]
        left[(1 - t) * heads + j] = partner[j, :tok, :]
    lhs = jnp.concatenate([left[i] for i in range(2 * heads)], axis=1)
    for copy in copies:
        copy.wait()
    mixed[...] = mm(lhs, weight[...]).astype(jnp.bfloat16)
    per = tok // LANES
    n = 2 * per
    for i in range(heads // 2):
        j = t * (heads // 2) + i
        rows = jnp.where(t == 1, own[j, tok:, :], partner[j, tok:, :]).astype(jnp.float32)
        x = rows[:n] + rows[n : 2 * n] + rows[2 * n : 3 * n]
        for h in range(2):
            log_total[2 * i + h : 2 * i + h + 1, :] = jnp.concatenate(
                [x[h * per + p : h * per + p + 1] for p in range(per)], axis=1
            )


def bf16_parts(x):
    high = lax.reduce_precision(x, 8, 7)
    mid = lax.reduce_precision(x - high, 8, 7)
    return jnp.stack([high, mid, x - high - mid]).astype(jnp.bfloat16)


def on_device_split(
    plan,
    tokens,
    input_norm_gain,
    mq_weight,
    mk_weight,
    mv_weight,
    mo_weight,
    gate_weight,
    gate_bias,
    decay_extra,
    m_gain,
    aq_weight,
    ak_weight,
    av_weight,
    sink_logit,
    out_m_weight,
    out_a_weight,
):
    sp, group, plane, lh, tok = (plan[n] for n in ("sp", "group", "plane", "lh", "tok"))
    width, rows = plan["width"], plan["rows"]
    half = rows // 2
    f32, bf16 = jnp.float32, jnp.bfloat16
    s = lax.axis_index("sp").astype(jnp.int32)
    t = lax.axis_index("tp").astype(jnp.int32)
    hi, j = s // group, s % group
    near_plane = (s // plane) % 2
    meta = jnp.stack(
        [t, s % plane, jnp.where(j // lh == t, 0, 1), j % lh, hi, near_plane, s // plane]
    ).astype(jnp.int32)
    swap = [(0, 1), (1, 0)]

    def flip(x):
        return lax.ppermute(x, "tp", swap)

    normed = rms_rows(tokens.astype(f32), input_norm_gain).astype(bf16)

    def core(a, same):
        return 2 * a + ((a // plane) % 2 if same else 1 - (a // plane) % 2)

    both_axes = ("sp", "tp")
    other = lax.ppermute(
        normed, both_axes, [(core(a, True), core(a ^ plane, False)) for a in range(sp)]
    )
    same_xs, other_xs = [normed], [other]
    for r in range(1, plane):
        same_xs.append(
            lax.ppermute(normed, both_axes, [(core(a, True), core(a ^ r, True)) for a in range(sp)])
        )

    gate_rows = jnp.transpose(gate_weight.reshape(2, half, 4, lh), (0, 3, 2, 1)).reshape(
        2, lh, 4 * half // LANES, LANES
    )
    decay_rows = jnp.transpose(bf16_parts(decay_extra), (1, 2, 0, 3)).reshape(
        2, lh, 3 * tok // LANES, LANES
    )
    small = jnp.concatenate([gate_rows, decay_rows], axis=2)
    n_gate, n_small = gate_rows.shape[2], small.shape[2]
    n_rows = 6 * half + n_small
    spread, send = vmem_call(
        pack_kernel,
        (
            jax.ShapeDtypeStruct((2, 2, lh, n_rows, LANES), bf16),
            jax.ShapeDtypeStruct((lh, n_rows, LANES), bf16),
        ),
        smem=1,
        n_in=8,
    )(meta, mq_weight, mk_weight, mv_weight, mo_weight, aq_weight, ak_weight, av_weight, small)
    got = flip(send)
    got = jnp.broadcast_to(got[None, None], (2, 1) + got.shape)
    spread = lax.dynamic_update_slice_in_dim(spread, got, 1 - t, 1)
    own_w = lax.all_to_all(spread.reshape(sp * n_rows, LANES), "sp", 0, 0, tiled=True)
    for r in range(1, plane):
        other_xs.append(
            lax.ppermute(
                other, both_axes, [(core(a, False), core(a ^ r, False)) for a in range(sp)]
            )
        )
    out_block = jnp.concatenate([out_m_weight, out_a_weight], axis=0)
    column = [out_block]
    for r in range(1, sp // plane):
        column.append(lax.ppermute(out_block, "sp", [(a, a ^ (r * plane)) for a in range(sp)]))
    partner_w = flip(own_w)
    own_w = own_w.reshape(sp, n_rows, LANES)
    partner_w = partner_w.reshape(sp, n_rows, LANES)
    small_both = jnp.stack([own_w[:, 6 * half :], partner_w[:, 6 * half :]])
    small_both = jnp.where(t == 0, small_both, small_both[::-1])
    gate_t = jnp.transpose(small_both[:, :, :n_gate].reshape(2, sp, 4, half), (2, 1, 0, 3))
    gate_t = jnp.pad(gate_t.reshape(4, width), ((0, LANES - 4), (0, 0)))
    first = (2 * hi + t) * plane
    decay = lax.dynamic_slice_in_dim(small_both[:, :, n_gate:], first, plane, 1)
    decay = jnp.sum(decay.reshape(2, plane, 3, tok).astype(f32), axis=2)
    decay = jnp.transpose(decay, (1, 0, 2))
    params = jnp.concatenate(
        [m_gain, gate_bias.reshape(-1), sink_logit, jnp.zeros((LANES - 6 * lh,), f32)]
    ).reshape(-1, LANES)
    params = jnp.stack([params, flip(params)])
    gain = params[:, :lh]
    bias = params[:, lh, : 4 * lh]
    sink = params[:, lh, 4 * lh : 6 * lh]

    quarter = plane * tok
    cols = 6 * LANES
    sum_rows = M_DIM + 8 + WINDOW
    proj, gates, summary = vmem_call(
        project_kernel,
        (
            jax.ShapeDtypeStruct((quarter, cols), bf16),
            jax.ShapeDtypeStruct((plane, 8, tok), f32),
            jax.ShapeDtypeStruct((2, sum_rows, LANES), f32),
        ),
        scratch=[
            pltpu.VMEM((width, cols), bf16),
            pltpu.VMEM((plane, tok, width), bf16),
            pltpu.VMEM((2, sp, n_rows, LANES), bf16),
            pltpu.SemaphoreType.DMA((plane + 2,)),
        ],
        smem=2,
        n_any=2 * plane + 2,
        n_tail=2,
        flops=2 * quarter * width * cols,
    )(meta, bias, *same_xs, *other_xs, own_w, partner_w, gate_t, decay)
    column = jnp.concatenate(column, axis=0)
    out_blocks = [column]
    for r in range(1, plane):
        out_blocks.append(lax.ppermute(column, "sp", [(a, a ^ r) for a in range(sp)]))
    partner_sum = flip(summary)
    sent = vmem_call(
        combine_kernel, jax.ShapeDtypeStruct((sum_rows, LANES), f32), smem=1, n_in=2
    )(meta, summary, partner_sum)
    across = lax.ppermute(sent, "sp", [(a, (a + group) % sp) for a in range(sp)])
    spread, send = vmem_call(
        mixer_kernel,
        (
            jax.ShapeDtypeStruct((2, plane, tok + 16, LANES), bf16),
            jax.ShapeDtypeStruct((plane, tok + 16, LANES), bf16),
        ),
        scratch=[
            pltpu.VMEM((quarter + 2 * WINDOW, LANES), bf16),
            pltpu.VMEM((plane, 2 * tok // WINDOW, LANES), f32),
        ],
        smem=2,
        n_in=5,
        flops=2 * quarter * width * cols,
    )(meta, sink, proj, gates, partner_sum, across, gain)
    got = flip(send)
    spread = lax.dynamic_update_slice_in_dim(spread, got[None], 1 - t, 0)
    groups = [list(range(g * group, (g + 1) * group)) for g in range(sp // group)]
    mine = lax.all_to_all(
        spread.reshape(group * (tok + 16), LANES),
        "sp",
        0,
        0,
        axis_index_groups=groups,
        tiled=True,
    )
    theirs = flip(mine)
    shape = (group, tok + 16, LANES)
    inner = 2 * group * LANES
    return vmem_call(
        output_kernel,
        (
            jax.ShapeDtypeStruct((tok, out_m_weight.shape[1]), bf16),
            jax.ShapeDtypeStruct((2 * lh, tok), f32),
        ),
        scratch=[
            pltpu.VMEM((2 * group, tok, LANES), bf16),
            pltpu.VMEM((inner, out_m_weight.shape[1]), bf16),
            pltpu.SemaphoreType.DMA((sp, 2)),
        ],
        smem=1,
        n_in=2,
        n_any=plane,
        flops=2 * tok * inner * out_m_weight.shape[1],
    )(meta, mine.reshape(shape), theirs.reshape(shape), *out_blocks)


def solution(mesh):
    in_specs = (
        P("sp", None),
        P(),
        P("sp", "tp"),
        P("sp", "tp"),
        P("sp", "tp"),
        P("sp", "tp"),
        P("sp", None, "tp"),
        P(None, "tp"),
        P(None, "tp", "sp"),
        P("tp"),
        P("sp", "tp"),
        P("sp", "tp"),
        P("sp", "tp"),
        P("tp"),
        P("sp", "tp"),
        P("sp", "tp"),
    )
    out_specs = (P("sp", "tp"), P("tp", "sp"))

    def per_device(*args):
        plan = split_plan(mesh, args)
        if plan is None:
            return on_device(*args)
        return on_device_split(plan, *args)

    return jax.shard_map(
        per_device, mesh=mesh, in_specs=in_specs, out_specs=out_specs, check_vma=False
    )
```

```python
import jax
import jax.numpy as jnp
from jax import lax
import math

from jax.experimental import pallas as pl
from jax.experimental.pallas import tpu as pltpu
from jax.sharding import PartitionSpec as P

M_DIM = 128
W_DIM = 64
WINDOW = 128
M_BLOCK = 64


EPS = 1e-06
FLOOR_LOG = -1e30
HIGHEST = lax.Precision.HIGHEST


def with_halo(x, sides, width):
    for axis, dim in sides:
        peers, length = (lax.axis_size(axis), x.shape[dim])
        up = [(i, (i + 1) % peers) for i in range(peers - 1)]
        down = [(j, i) for i, j in up]
        last = lax.slice_in_dim(x, length - width, length, axis=dim)
        first = lax.slice_in_dim(x, 0, width, axis=dim)
        before = lax.ppermute(last, axis, up)
        after = lax.ppermute(first, axis, down)
        x = jnp.concatenate([before, x, after], axis=dim)
    return x


def rms_rows(inputs, gain_vec):
    return inputs * lax.rsqrt(jnp.mean(inputs * inputs, axis=-1, keepdims=True) + EPS) * gain_vec


def stored(result):
    return lax.optimization_barrier(result.astype(jnp.bfloat16))


def flip_tokens(array_in):
    return jnp.flip(array_in, axis=1)


def block_pass(queries, key_vecs, value_vecs, in_gate, log_forget, start_state):
    head_count, length, head_width = queries.shape
    block_count = length // M_BLOCK

    def blocks(array_in):
        return jnp.moveaxis(
            array_in.reshape((head_count, block_count, M_BLOCK) + array_in.shape[2:]), 1, 0
        )

    lower_mask = jnp.tril(jnp.ones((M_BLOCK, M_BLOCK), dtype=bool))

    def advance(state_in, block_in):
        cell_mat, norm_vec, stab_max = state_in
        q_blk, k_blk, v_blk, i_blk, f_blk = block_in
        cum_log = jnp.cumsum(f_blk, axis=-1)
        seg_total = cum_log[:, -1]
        log_end = seg_total[:, None] - cum_log + i_blk
        max_next = jnp.maximum(seg_total + stab_max, jnp.max(log_end, axis=-1))
        w_end = jnp.exp(log_end - max_next[:, None])
        fade_old = jnp.exp(seg_total + stab_max - max_next)
        cell_next = fade_old[:, None, None] * cell_mat + jnp.einsum(
            "hsv,hsk->hvk", w_end[:, :, None] * v_blk, k_blk, precision=HIGHEST
        )
        norm_next = fade_old[:, None] * norm_vec + jnp.einsum(
            "hs,hsk->hk", w_end, k_blk, precision=HIGHEST
        )
        log_w = jnp.where(
            lower_mask, cum_log[:, :, None] - cum_log[:, None, :] + i_blk[:, None, :], -jnp.inf
        )
        log_inter = cum_log + stab_max[:, None]
        row_max = jnp.maximum(log_inter, jnp.max(log_w, axis=-1))
        w_intra = jnp.exp(log_w - row_max[:, :, None])
        w_inter = jnp.exp(log_inter - row_max)
        scores = jnp.einsum("htk,hsk->hts", q_blk, k_blk, precision=HIGHEST) * w_intra
        numerator = jnp.einsum("hts,hsv->htv", scores, v_blk, precision=HIGHEST) + w_inter[
            ..., None
        ] * jnp.einsum("hvk,htk->htv", cell_mat, q_blk, precision=HIGHEST)
        denominator = jnp.sum(scores, axis=-1) + w_inter * jnp.einsum(
            "hk,htk->ht", norm_vec, q_blk, precision=HIGHEST
        )
        result_rows = numerator / jnp.maximum(jnp.abs(denominator), jnp.exp(-row_max))[..., None]
        return ((cell_next, norm_next, max_next), result_rows)

    final_state, outputs = lax.scan(
        advance,
        start_state,
        tuple(
            (blocks(array_in) for array_in in (queries, key_vecs, value_vecs, in_gate, log_forget))
        ),
    )
    return (jnp.moveaxis(outputs, 0, 1).reshape(head_count, length, head_width), final_state)


def summarize(key_vecs, value_vecs, in_gate, log_forget):
    cum_log = jnp.cumsum(log_forget, axis=-1)
    seg_total = cum_log[:, -1]
    log_end = seg_total[:, None] - cum_log + in_gate
    peak_log = jnp.max(log_end, axis=-1)
    weights_end = jnp.exp(log_end - peak_log[:, None])
    cell_mat = jnp.einsum(
        "hsv,hsk->hvk", weights_end[:, :, None] * value_vecs, key_vecs, precision=HIGHEST
    )
    norm_vec = jnp.einsum("hs,hsk->hk", weights_end, key_vecs, precision=HIGHEST)
    return (seg_total, cell_mat, norm_vec, peak_log)


def merge_side(state_in, cell_mats, norm_vecs, logs, usable):
    cell_mat, norm_vec, peak_log = state_in
    masked = jnp.where(usable, logs, FLOOR_LOG)
    new_peak = jnp.maximum(peak_log, jnp.max(masked, axis=0))
    scales = jnp.where(usable, jnp.exp(masked - new_peak[None]), 0.0)
    cell_mat = jnp.einsum("jh,jhvk->hvk", scales, cell_mats, precision=HIGHEST)
    norm_vec = jnp.einsum("jh,jhk->hk", scales, norm_vecs, precision=HIGHEST)
    return (cell_mat, norm_vec, new_peak)


def gather_states(forward_sum, backward_sum):
    decay_all = (
        lax.all_gather(forward_sum[0][None], "sp", axis=0, tiled=True),
        lax.all_gather(backward_sum[0][None], "sp", axis=0, tiled=True),
    )
    own_index = lax.axis_index("sp")
    acc_fwd = jnp.cumsum(decay_all[0], axis=0)
    acc_bwd = jnp.cumsum(decay_all[1], axis=0)
    before_own = lax.dynamic_index_in_dim(acc_fwd - decay_all[0], own_index, 0, keepdims=False)
    after_own = lax.dynamic_index_in_dim(acc_bwd, own_index, 0, keepdims=False)
    lead_bwd = acc_bwd - decay_all[1]
    empty_side = (
        jnp.zeros_like(forward_sum[1]),
        jnp.zeros_like(forward_sum[2]),
        jnp.full_like(forward_sum[3], FLOOR_LOG),
    )
    state_in = empty_side + empty_side
    pieces = (
        lax.all_gather(forward_sum[1][None], "sp", axis=0, tiled=True),
        lax.all_gather(forward_sum[2][None], "sp", axis=0, tiled=True),
        lax.all_gather(forward_sum[3][None], "sp", axis=0, tiled=True),
        lax.all_gather(backward_sum[1][None], "sp", axis=0, tiled=True),
        lax.all_gather(backward_sum[2][None], "sp", axis=0, tiled=True),
        lax.all_gather(backward_sum[3][None], "sp", axis=0, tiled=True),
    )
    piece_count = pieces[0].shape[0]
    device_ids = jnp.arange(piece_count, dtype=jnp.int32)
    log_fwd = before_own[None] - acc_fwd + pieces[2]
    log_bwd = lead_bwd - after_own[None] + pieces[5]
    left_side = merge_side(
        state_in[:3], pieces[0], pieces[1], log_fwd, (device_ids < own_index)[:, None]
    )
    right_side = merge_side(
        state_in[3:], pieces[3], pieces[4], log_bwd, (device_ids > own_index)[:, None]
    )
    states = left_side + right_side
    return (states[:3], states[3:])


def window_attend(a_query, kv_pairs, sink_logit, first_row, total_rows):
    tok_rows = a_query.shape[0]
    block_len = WINDOW
    block_count = tok_rows // block_len
    kv_width = kv_pairs.shape[1] // 2
    kv_heads = kv_width // W_DIM
    q_heads = a_query.shape[1] // W_DIM
    groups = q_heads // kv_heads
    filled_margin = with_halo(kv_pairs, (("sp", 0),), WINDOW)
    windows = jnp.concatenate(
        [
            filled_margin[place_idx * block_len : place_idx * block_len + tok_rows].reshape(
                block_count, block_len, 2 * kv_width
            )
            for place_idx in range(3)
        ],
        axis=1,
    )
    key_block = windows[:, :, :kv_width].reshape(block_count, 3 * block_len, kv_heads, W_DIM)
    content_tile = windows[:, :, kv_width:].reshape(block_count, 3 * block_len, kv_heads, W_DIM)
    query_block = a_query.reshape(block_count, block_len, kv_heads, groups, W_DIM)
    scores = jnp.einsum(
        "nqgrd,nkgd->ngrqk", query_block, key_block, preferred_element_type=jnp.float32
    ) * W_DIM ** (-0.5)
    query_off = jnp.arange(block_len, dtype=jnp.int32)
    key_off = jnp.arange(3 * block_len, dtype=jnp.int32) - block_len
    in_window = jnp.abs(query_off[:, None] - key_off[None, :]) <= WINDOW
    key_place = (
        first_row + jnp.arange(block_count, dtype=jnp.int32)[:, None] * block_len + key_off[None, :]
    )
    inside = (key_place >= 0) & (key_place < total_rows)
    usable = in_window[None] & inside[:, None, :]
    scores = jnp.where(usable[:, None, None], scores, -jnp.inf)
    sink_col = sink_logit.reshape(kv_heads, groups)[None, :, :, None]
    peak_log = jnp.maximum(sink_col, jnp.max(scores, axis=-1))
    weights_exp = jnp.exp(scores - peak_log[..., None])
    weight_total_sum = jnp.exp(sink_col - peak_log) + jnp.sum(weights_exp, axis=-1)
    weighted = jnp.einsum(
        "ngrqk,nkgd->nqgrd",
        weights_exp.astype(jnp.bfloat16),
        content_tile,
        preferred_element_type=jnp.float32,
    )
    scale_back = jnp.transpose(weight_total_sum, (0, 3, 1, 2))[..., None]
    mixed_rows = (weighted / scale_back).astype(jnp.bfloat16).reshape(tok_rows, q_heads * W_DIM)
    log_total = jnp.transpose(peak_log + jnp.log(weight_total_sum), (1, 2, 0, 3)).reshape(
        q_heads, tok_rows
    )
    return (mixed_rows, log_total)


def on_device(
    tokens,
    input_norm_gain,
    mq_weight,
    mk_weight,
    mv_weight,
    mo_weight,
    gate_weight,
    gate_bias,
    decay_extra,
    m_gain,
    aq_weight,
    ak_weight,
    av_weight,
    sink_logit,
    out_m_weight,
    out_a_weight,
):
    tok_rows = tokens.shape[0]
    normed = rms_rows(tokens.astype(jnp.float32), input_norm_gain).astype(jnp.bfloat16)
    local_heads = gate_weight.shape[2]
    gate_cols = 4 * local_heads
    pieces = (
        lax.all_gather(mq_weight, "sp", axis=0, tiled=True),
        lax.all_gather(mk_weight, "sp", axis=0, tiled=True),
        lax.all_gather(mv_weight, "sp", axis=0, tiled=True),
        lax.all_gather(mo_weight, "sp", axis=0, tiled=True),
        lax.all_gather(gate_weight, "sp", axis=0, tiled=True),
        lax.all_gather(aq_weight, "sp", axis=0, tiled=True),
        lax.all_gather(ak_weight, "sp", axis=0, tiled=True),
        lax.all_gather(av_weight, "sp", axis=0, tiled=True),
    )
    piece_rows = pieces[0].shape[0]
    flat_gate = pieces[4].reshape(piece_rows, gate_cols)
    segments = (
        pieces[0],
        pieces[1],
        pieces[2],
        pieces[3],
        flat_gate,
        pieces[5],
        pieces[6],
        pieces[7],
    )
    projected = tuple(
        (jnp.dot(normed, segment, preferred_element_type=jnp.float32) for segment in segments)
    )
    m_query = stored(projected[0])
    m_key = stored(projected[1])
    m_value = stored(projected[2])
    m_out = stored(projected[3])
    gates = projected[4].reshape(tok_rows, 4, local_heads) + gate_bias[None]

    def heads_first(matrix):
        return jnp.transpose(
            matrix.astype(jnp.float32).reshape(tok_rows, local_heads, M_DIM), (1, 0, 2)
        )

    queries = heads_first(m_query)
    key_vecs = heads_first(m_key) * M_DIM ** (-0.5)
    value_vecs = heads_first(m_value)
    in_fwd = gates[:, 0, :].T
    forget_fwd = jax.nn.log_sigmoid(gates[:, 1, :].T) + decay_extra[0]
    in_bwd = flip_tokens(gates[:, 2, :].T)
    forget_bwd = flip_tokens(jax.nn.log_sigmoid(gates[:, 3, :].T) + decay_extra[1])
    queries_bwd = flip_tokens(queries)
    keys_bwd = flip_tokens(key_vecs)
    values_bwd = flip_tokens(value_vecs)
    forward_sum = summarize(key_vecs, value_vecs, in_fwd, forget_fwd)
    backward_sum = summarize(keys_bwd, values_bwd, in_bwd, forget_bwd)
    state_fwd, state_bwd = gather_states(forward_sum, backward_sum)
    hidden_fwd, _ = block_pass(queries, key_vecs, value_vecs, in_fwd, forget_fwd, state_fwd)
    hidden_bwd, _ = block_pass(queries_bwd, keys_bwd, values_bwd, in_bwd, forget_bwd, state_bwd)
    cell_out = hidden_fwd + flip_tokens(hidden_bwd)
    gate_open = jax.nn.sigmoid(m_out.astype(jnp.float32)).reshape(tok_rows, local_heads, M_DIM)
    cell_rows = jnp.transpose(cell_out, (1, 0, 2)) * gate_open
    mixed_m = (
        rms_rows(cell_rows, m_gain.reshape(local_heads, M_DIM))
        .astype(jnp.bfloat16)
        .reshape(tok_rows, local_heads * M_DIM)
    )
    a_query = stored(projected[5])
    kv_pairs = jnp.concatenate([stored(projected[6]), stored(projected[7])], axis=1)
    first_row = lax.axis_index("sp") * tok_rows
    total_rows = tok_rows * lax.axis_size("sp")
    mixed_a, log_total = window_attend(a_query, kv_pairs, sink_logit, first_row, total_rows)
    full_m, full_a = (
        lax.all_gather(mixed_m, "tp", axis=1, tiled=True),
        lax.all_gather(mixed_a, "tp", axis=1, tiled=True),
    )
    pieces = (
        lax.all_gather(out_m_weight, "sp", axis=0, tiled=True),
        lax.all_gather(out_a_weight, "sp", axis=0, tiled=True),
    )
    running = jnp.dot(full_m, pieces[0], preferred_element_type=jnp.float32)
    mixed = running + jnp.dot(full_a, pieces[1], preferred_element_type=jnp.float32)
    return (mixed.astype(jnp.bfloat16), log_total)


CHUNK = 256
LANES = 128
EMPTY = -1e30


def split_plan(mesh, args):
    sp, tp = mesh.shape["sp"], mesh.shape["tp"]
    tok_rows, width = args[0].shape
    rows = args[2].shape[0]
    local_heads = args[6].shape[2]
    group = local_heads * tp
    if tp != 2 or sp != 2 * group or group != 8:
        return None
    plane = group // 2
    ok = (
        args[2].shape[1] == local_heads * M_DIM
        and args[10].shape[1] == local_heads * LANES
        and args[11].shape[1] == local_heads * W_DIM
        and args[12].shape[1] == local_heads * W_DIM
        and 2 * W_DIM == LANES
        and M_DIM == LANES
        and WINDOW == LANES
        and tok_rows == CHUNK
        and rows == LANES
        and args[14].shape[0] * sp == group * M_DIM
        and args[15].shape[0] * sp == group * LANES
    )
    if not ok:
        return None
    return dict(
        sp=sp, tp=tp, tok=tok_rows, width=width, rows=rows, lh=local_heads, group=group, plane=plane
    )


def mm(a, b, ca=1, cb=0, precision=None):
    return lax.dot_general(
        a, b, (((ca,), (cb,)), ((), ())), precision=precision, preferred_element_type=jnp.float32
    )


def vmem_call(kernel, outs, scratch=(), smem=0, n_in=0, flops=0, n_any=0, n_tail=0):
    return pl.pallas_call(
        kernel,
        out_shape=outs,
        in_specs=[pl.BlockSpec(memory_space=pltpu.SMEM)] * smem
        + [pl.BlockSpec(memory_space=pltpu.VMEM)] * n_in
        + [pl.BlockSpec(memory_space=pl.ANY)] * n_any
        + [pl.BlockSpec(memory_space=pltpu.VMEM)] * n_tail,
        out_specs=jax.tree.map(lambda _: pl.BlockSpec(memory_space=pltpu.VMEM), outs),
        scratch_shapes=scratch,
        cost_estimate=pl.CostEstimate(flops=flops, bytes_accessed=0, transcendentals=0),
        compiler_params=pltpu.CompilerParams(vmem_limit_bytes=56 * 1024 * 1024),
    )


def pack_kernel(meta, mq, mk, mv, mo, aq, ak, av, small, keep, send):
    t = meta[0]
    copies, heads = keep.shape[0], keep.shape[2]
    rows = mq.shape[0] // 2
    at = pl.multiple_of(t * rows, rows)
    away = pl.multiple_of((1 - t) * rows, rows)
    for h in range(heads):
        lanes = slice(h * LANES, (h + 1) * LANES)
        narrow = slice(h * W_DIM, (h + 1) * W_DIM)
        for start, mine in ((at, True), (away, False)):
            parts = [ref[pl.ds(start, rows), lanes] for ref in (mq, mk, mv, mo, aq)]
            parts.append(
                jnp.concatenate([ref[pl.ds(start, rows), narrow] for ref in (ak, av)], axis=1)
            )
            parts.append(small[t if mine else 1 - t, h])
            row = 0
            for part in parts:
                span = slice(row, row + part.shape[0])
                row += part.shape[0]
                if mine:
                    for i in range(copies):
                        keep[i, t, h, span, :] = part
                else:
                    send[h, span, :] = part


def running_max(x, backward):
    n = x.shape[1]
    lane = lax.broadcasted_iota(jnp.int32, x.shape, 1)
    step = 1
    while step < n:
        if backward:
            moved = jnp.where(lane < n - step, pltpu.roll(x, n - step, 1), EMPTY)
        else:
            moved = jnp.where(lane >= step, pltpu.roll(x, step, 1), EMPTY)
        x = jnp.maximum(x, moved)
        step *= 2
    return x


def with_ones(value):
    lane = lax.broadcasted_iota(jnp.int32, value.shape, 1)
    ones = jnp.where(lane == 0, 1.0, 0.0).astype(value.dtype)
    return jnp.concatenate([value, ones], axis=1)


def merge(earlier, later, later_total):
    peak = jnp.maximum(later_total + earlier[1], later[1])
    old = jnp.exp(later_total + earlier[1] - peak)
    new = jnp.exp(later[1] - peak)
    return old * earlier[0] + new * later[0], peak


def project_kernel(meta, bias, *refs):
    plane = (len(refs) - 14) // 2
    same, other = refs[:plane], refs[plane : 2 * plane]
    own, partner, gate_t, decay = refs[2 * plane : 2 * plane + 4]
    proj, vrows, vcols, local, summary, weight, xs, raw, gates, sems = refs[2 * plane + 4 :]
    t, k, sel, jl, near = meta[0], meta[1], meta[2], meta[3], meta[5]
    copies = [
        pltpu.make_async_copy(own, raw.at[0], sems.at[plane]),
        pltpu.make_async_copy(partner, raw.at[1], sems.at[plane + 1]),
    ]
    for copy in copies:
        copy.start()

    @pl.when(t == near)
    def _():
        for r in range(plane):
            pltpu.make_async_copy(same[r], xs.at[r], sems.at[r]).start()

    @pl.when(t != near)
    def _():
        for r in range(plane):
            pltpu.make_async_copy(other[r], xs.at[r], sems.at[r]).start()

    for copy in copies:
        copy.wait()
    sources = own.shape[0]
    rows = weight.shape[0] // sources // 2
    cols = weight.shape[1] // LANES
    for i in range(sources):
        for c in range(cols):
            lanes = slice(c * LANES, (c + 1) * LANES)
            span = slice(c * rows, (c + 1) * rows)
            first = pl.multiple_of((2 * i + t) * rows, rows)
            second = pl.multiple_of((2 * i + 1 - t) * rows, rows)
            weight[pl.ds(first, rows), lanes] = raw[0, i, span, :]
            weight[pl.ds(second, rows), lanes] = raw[1, i, span, :]
    tok = xs.shape[1]
    for r in range(plane):
        pltpu.make_async_copy(same[r], xs.at[r], sems.at[r]).wait()
        at = pl.ds(pl.multiple_of((k ^ r) * tok, tok), tok)
        proj[at, :] = mm(xs[r], weight[...]).astype(jnp.bfloat16)
        gates[k ^ r] = jnp.transpose(mm(xs[r], gate_t[...], 1, 1))[:8]
    heads = bias.shape[1] // 4
    b = [bias[sel, g * heads + jl] for g in range(4)]
    g = [
        jnp.concatenate([gates[c, i : i + 1] for c in range(plane)], axis=0) + b[i]
        for i in range(4)
    ]

    def forget(i, direction):
        x = g[i]
        return jnp.minimum(x, 0.0) - jnp.log1p(jnp.exp(-jnp.abs(x))) + decay[direction]

    lf_f, lf_b = forget(1, 0), forget(3, 1)
    r = lax.broadcasted_iota(jnp.int32, (tok, tok), 0)
    c = lax.broadcasted_iota(jnp.int32, (tok, tok), 1)
    lower = jnp.where(r >= c, 1.0, 0.0).astype(jnp.float32)
    cum = mm(jnp.concatenate([lf_f, lf_b], axis=0), lower, 1, 1, HIGHEST)
    lead_f, lead_b = cum[:plane], lf_b - cum[plane:]
    src_f, src_b = g[0] - lead_f, g[2] - lead_b
    top_f, top_b = running_max(src_f, False), running_max(src_b, True)
    total_f, total_b = lead_f[:, tok - 1 :], cum[plane:, tok - 1 :]
    best_f, best_b = top_f[:, tok - 1 :], top_b[:, :1]
    end_f, end_b = jnp.exp(src_f - best_f), jnp.exp(src_b - best_b)
    peak_f, peak_b = best_f + total_f, best_b

    def wide(x):
        return jnp.broadcast_to(x, (plane, tok))

    vrows[...] = jnp.concatenate(
        [src_f, src_b, wide(total_f), wide(total_b), wide(peak_f), wide(peak_b)], axis=0
    )
    stack = [top_f, top_b, lead_f, lead_b, end_f, end_b]
    stack.append(jnp.zeros((LANES - 6 * plane, tok), jnp.float32))
    cols_all = jnp.transpose(jnp.concatenate(stack, axis=0))
    vcols[...] = cols_all
    for ch in range(plane):
        span = slice(ch * tok, (ch + 1) * tok)
        key = proj[span, LANES : 2 * LANES].astype(jnp.float32)
        value = with_ones(proj[span, 2 * LANES : 3 * LANES])
        for i in range(2):
            at = (4 + i) * plane + ch
            weighted = (key * cols_all[:, at : at + 1]).astype(jnp.bfloat16)
            local[i, ch] = mm(weighted, value, 0, 0)
    for i in range(2):
        state = (jnp.zeros((M_DIM, 2 * LANES), jnp.float32), jnp.full((1, 1), EMPTY, jnp.float32))
        total = jnp.zeros((1, 1), jnp.float32)
        for ch in range(plane) if i == 0 else range(plane - 1, -1, -1):
            chunk_total, chunk_peak = chunk_scalars(vrows, i, ch, plane)
            state = merge(state, (local[i, ch], chunk_peak), chunk_total)
            total = total + chunk_total
        summary[i, :M_DIM, :] = state[0][:, :LANES]
        summary[i, M_DIM : M_DIM + 8, :] = jnp.concatenate(
            [
                jnp.transpose(state[0][:, LANES:])[:1],
                jnp.broadcast_to(state[1], (1, LANES)),
                jnp.broadcast_to(total, (1, LANES)),
                jnp.zeros((5, LANES), jnp.float32),
            ],
            axis=0,
        )
    last = proj.shape[0]
    summary[0, M_DIM + 8 :, :] = proj[:WINDOW, 5 * LANES :].astype(jnp.float32)
    summary[1, M_DIM + 8 :, :] = proj[last - WINDOW :, 5 * LANES :].astype(jnp.float32)


def chunk_scalars(vrows, i, ch, plane):
    total, peak = (2 + i) * plane + ch, (4 + i) * plane + ch
    return vrows[total : total + 1, :1], vrows[peak : peak + 1, :1]


def packed_state(ref, i):
    rows = ref[i, : M_DIM + 8, :]
    return (rows, rows[M_DIM + 1 : M_DIM + 2, :1]), rows[M_DIM + 2 : M_DIM + 3, :1]


def open_state(packed):
    rows, peak = packed
    first = lax.broadcasted_iota(jnp.int32, (LANES, LANES), 0) == 0
    norm = jnp.transpose(jnp.where(first, rows[M_DIM : M_DIM + 1], 0.0))
    return jnp.concatenate([rows[:M_DIM], norm], axis=1), peak


def combine_kernel(meta, own, partner, out):
    t, hi = meta[0], meta[4]
    forward = hi == 0
    i = jnp.where(forward, 0, 1)
    (mine, mine_peak), mine_total = packed_state(own, i)
    (other, other_peak), other_total = packed_state(partner, i)
    mine_later = (t == 1) == forward

    def pick(x, y):
        return jnp.where(mine_later, x, y)

    rows, peak = merge(
        (pick(other, mine), pick(other_peak, mine_peak)),
        (pick(mine, other), pick(mine_peak, other_peak)),
        pick(mine_total, other_total),
    )
    out[: M_DIM + 8, :] = rows
    out[M_DIM + 1 : M_DIM + 2, :] = jnp.broadcast_to(peak, (1, LANES))
    out[M_DIM + 8 :, :] = partner[jnp.where(forward, 1, 0), M_DIM + 8 :, :]


def attend(q, kv, sinks, drop_first, drop_last):
    n = q.shape[0]
    q = q * jnp.bfloat16(W_DIM ** (-0.5))
    q = jnp.concatenate([q[:, :W_DIM], q[:, W_DIM:]], axis=0)
    r = lax.broadcasted_iota(jnp.int32, (2 * n, n), 0)
    c = lax.broadcasted_iota(jnp.int32, (2 * n, n), 1)
    row = jnp.where(r >= n, r - n, r)
    sink = jnp.where(
        lax.broadcasted_iota(jnp.int32, (2 * n, 1), 0) < n, sinks[0], sinks[1]
    )
    s = [mm(q, kv[i * n : (i + 1) * n, :W_DIM], 1, 1) for i in range(3)]
    before, after = c >= row, c <= row
    if drop_first is not None:
        before = before & jnp.logical_not(drop_first)
        after = after & jnp.logical_not(drop_last)
    s[0] = jnp.where(before, s[0], EMPTY)
    s[2] = jnp.where(after, s[2], EMPTY)
    peak = jnp.max(jnp.maximum(jnp.maximum(s[0], s[1]), s[2]), axis=1, keepdims=True)
    peak = jnp.maximum(peak, sink)
    e = [jnp.exp(x - peak) for x in s]
    total = jnp.exp(sink - peak) + jnp.sum(e[0] + e[1] + e[2], axis=1, keepdims=True)
    weights = jnp.concatenate([x.astype(jnp.bfloat16) for x in e], axis=1)
    mixed = mm(weights, kv[:, W_DIM:]) / total
    mixed = jnp.concatenate([mixed[:n], mixed[n:]], axis=1).astype(jnp.bfloat16)
    log_col = peak + jnp.log(total)
    diag = (c == row)
    logs = [
        jnp.sum(jnp.where(diag[:n], log_col[h * n : (h + 1) * n], 0.0), axis=0, keepdims=True)
        for h in range(2)
    ]
    return mixed, jnp.concatenate(logs + [jnp.zeros((6, n), jnp.float32)], axis=0)


def attend_kernel(meta, sink, proj, partner, mixed, logs, kv):
    t, sel, jl = meta[0], meta[2], meta[3]
    length = proj.shape[0]
    edge = partner[jnp.where(t == 0, 0, 1), M_DIM + 8 :, :].astype(jnp.bfloat16)
    kv[:WINDOW, :] = edge
    kv[WINDOW : WINDOW + length, :] = proj[:, 5 * LANES :]
    kv[WINDOW + length :, :] = edge
    sinks = (sink[sel, 2 * jl], sink[sel, 2 * jl + 1])
    for i in range(length // WINDOW - 1):
        b = i + 1 - t
        at = pl.multiple_of(b * WINDOW, WINDOW)
        q = proj[pl.ds(at, WINDOW), 4 * LANES : 5 * LANES]
        mixed[b], logs[b] = attend(q, kv[pl.ds(at, 3 * WINDOW), :], sinks, None, None)


def mixer_kernel(
    meta, sink, proj, vrows, vcols, local, partner, across, gain, att, att_logs, keep, send, am, al
):
    t, sel, jl, hi = meta[0], meta[2], meta[3], meta[4]
    tok = vrows.shape[1]
    chunks = vrows.shape[0] // 6

    def store(is_cell, c, span, value):
        @pl.when((t == 0) == is_cell)
        def _():
            keep[t, c, span, :] = value

        @pl.when((t == 0) != is_cell)
        def _():
            send[c, span, :] = value

    length = proj.shape[0]
    blocks = length // WINDOW
    am[...] = att[...]
    al[...] = att_logs[...]
    outer = across[M_DIM + 8 :, :].astype(jnp.bfloat16)
    inside = proj[pl.ds(pl.multiple_of(t * (length - 2 * WINDOW), WINDOW), 2 * WINDOW), 5 * LANES :]
    kv = jnp.where(
        t == 0,
        jnp.concatenate([outer, inside], axis=0),
        jnp.concatenate([inside, outer], axis=0),
    )
    sinks = (sink[sel, 2 * jl], sink[sel, 2 * jl + 1])
    at = pl.multiple_of(t * (length - WINDOW), WINDOW)
    q = proj[pl.ds(at, WINDOW), 4 * LANES : 5 * LANES]
    edge = t * (blocks - 1)
    am[edge], al[edge] = attend(q, kv, sinks, (t == 0) & (hi == 0), (t == 1) & (hi == 1))

    far = across[: M_DIM + 8, :]
    far_peak = across[M_DIM + 1 : M_DIM + 2, :1]

    def incoming(i, use_far, use_near):
        (near, near_peak), near_total = packed_state(partner, i)
        return open_state(
            merge(
                (far, jnp.where(use_far, far_peak, EMPTY)),
                (near, jnp.where(use_near, near_peak, EMPTY)),
                jnp.where(use_near, near_total, 0.0),
            )
        )

    fwd = incoming(0, hi == 1, t == 1)
    bwd = incoming(1, hi == 0, t == 0)
    entering = [[None, None] for _ in range(chunks)]
    for c in range(chunks):
        entering[c][0] = fwd
        total, peak = chunk_scalars(vrows, 0, c, chunks)
        if c + 1 < chunks:
            fwd = merge(fwd, (local[0, c], peak), total)
    for c in range(chunks - 1, -1, -1):
        total, peak = chunk_scalars(vrows, 1, c, chunks)
        entering[c][1] = (bwd[0], bwd[1] + total)
        if c:
            bwd = merge(bwd, (local[1, c], peak), total)
    r = lax.broadcasted_iota(jnp.int32, (tok, tok), 0)
    col = lax.broadcasted_iota(jnp.int32, (tok, tok), 1)
    gain_row = gain[sel, pl.ds(jl, 1), :]
    floor_lift = 0.5 * math.log(M_DIM)
    for c in range(chunks):
        span = slice(c * tok, (c + 1) * tok)
        q = proj[span, :LANES]
        value = with_ones(proj[span, 2 * LANES : 3 * LANES])
        scores = mm(q, proj[span, LANES : 2 * LANES], 1, 1)
        cell_out = None
        for i, mask in enumerate((r >= col, r <= col)):
            cell, reach = entering[c][i]
            at = i * chunks + c
            src = vrows[at : at + 1, :]
            top = jnp.maximum(vcols[:, at : at + 1], reach)
            lead = vcols[:, at + 2 * chunks : at + 2 * chunks + 1]
            w = jnp.where(mask, jnp.exp(src - top), 0.0)
            both = mm((scores * w).astype(jnp.bfloat16), value) + jnp.exp(reach - top) * mm(
                q, cell.astype(jnp.bfloat16)
            )
            denom = jnp.abs(both[:, LANES : LANES + 1])
            inv = 1.0 / jnp.maximum(denom, jnp.exp(floor_lift - (lead + top)))
            part = both[:, :LANES] * inv
            cell_out = part if cell_out is None else cell_out + part
        gate = proj[span, 3 * LANES : 4 * LANES].astype(jnp.float32)
        u = cell_out / (1.0 + jnp.exp(-gate))
        u = u * lax.rsqrt(jnp.mean(u * u, axis=1, keepdims=True) + EPS) * gain_row
        tail = jnp.zeros((16, LANES), jnp.bfloat16)
        store(True, c, slice(0, tok + 16), jnp.concatenate([u.astype(jnp.bfloat16), tail], axis=0))

    per = tok // WINDOW
    for c in range(chunks):
        x = jnp.concatenate(
            [al[c * per + p][h : h + 1] for h in range(2) for p in range(per)], axis=0
        )
        high = x.astype(jnp.bfloat16).astype(jnp.float32)
        mid = (x - high).astype(jnp.bfloat16).astype(jnp.float32)
        low = x - high - mid
        pad = jnp.zeros((16 - 3 * 2 * per, LANES), jnp.float32)
        tail = jnp.concatenate([high, mid, low, pad], axis=0).astype(jnp.bfloat16)
        rows = [am[c * per + p] for p in range(per)] + [tail]
        store(False, c, slice(0, tok + 16), jnp.concatenate(rows, axis=0))


def output_kernel(meta, own, partner, *refs):
    mixed, log_total, left, weight, sems = refs[-5:]
    blocks = refs[:-5]
    t, p, z = meta[0], meta[1], meta[6]
    plane = len(blocks) // 2
    heads, tok = own.shape[0], mixed.shape[0]
    planes = sems.shape[0] // plane
    rows = 2 * blocks[0].shape[0] // planes
    half = rows // 2
    total = weight.shape[0] // 2
    copies = []
    for r in range(plane):
        for zr in range(planes):
            source = (z ^ zr) * plane + (p ^ r)
            for i in range(2):
                to = pl.multiple_of(i * total + source * half, half)
                copies.append(
                    pltpu.make_async_copy(
                        blocks[2 * r + 2 * zr // planes].at[
                            pl.ds(zr % (planes // 2) * rows + i * half, half)
                        ],
                        weight.at[pl.ds(to, half)],
                        sems.at[r * planes + zr, i],
                    )
                )
    for copy in copies:
        copy.start()
    for j in range(heads):
        left[t * heads + j] = own[j, :tok, :]
        left[(1 - t) * heads + j] = partner[j, :tok, :]
    lhs = jnp.concatenate([left[i] for i in range(2 * heads)], axis=1)
    for copy in copies:
        copy.wait()
    mixed[...] = mm(lhs, weight[...]).astype(jnp.bfloat16)
    per = tok // LANES
    n = 2 * per
    for i in range(heads // 2):
        j = t * (heads // 2) + i
        rows = jnp.where(t == 1, own[j, tok:, :], partner[j, tok:, :]).astype(jnp.float32)
        x = rows[:n] + rows[n : 2 * n] + rows[2 * n : 3 * n]
        for h in range(2):
            log_total[2 * i + h : 2 * i + h + 1, :] = jnp.concatenate(
                [x[h * per + p : h * per + p + 1] for p in range(per)], axis=1
            )


def bf16_parts(x):
    high = lax.reduce_precision(x, 8, 7)
    mid = lax.reduce_precision(x - high, 8, 7)
    return jnp.stack([high, mid, x - high - mid]).astype(jnp.bfloat16)


def on_device_split(
    plan,
    tokens,
    input_norm_gain,
    mq_weight,
    mk_weight,
    mv_weight,
    mo_weight,
    gate_weight,
    gate_bias,
    decay_extra,
    m_gain,
    aq_weight,
    ak_weight,
    av_weight,
    sink_logit,
    out_m_weight,
    out_a_weight,
):
    sp, group, plane, lh, tok = (plan[n] for n in ("sp", "group", "plane", "lh", "tok"))
    width, rows = plan["width"], plan["rows"]
    half = rows // 2
    f32, bf16 = jnp.float32, jnp.bfloat16
    s = lax.axis_index("sp").astype(jnp.int32)
    t = lax.axis_index("tp").astype(jnp.int32)
    hi, j = s // group, s % group
    near_plane = (s // plane) % 2
    meta = jnp.stack(
        [t, s % plane, jnp.where(j // lh == t, 0, 1), j % lh, hi, near_plane, s // plane]
    ).astype(jnp.int32)
    swap = [(0, 1), (1, 0)]

    def flip(x):
        return lax.ppermute(x, "tp", swap)

    normed = rms_rows(tokens.astype(f32), input_norm_gain).astype(bf16)

    def core(a, same):
        return 2 * a + ((a // plane) % 2 if same else 1 - (a // plane) % 2)

    both_axes = ("sp", "tp")
    other = lax.ppermute(
        normed, both_axes, [(core(a, True), core(a ^ plane, False)) for a in range(sp)]
    )
    same_xs, other_xs = [normed], [other]
    for r in range(1, plane):
        same_xs.append(
            lax.ppermute(normed, both_axes, [(core(a, True), core(a ^ r, True)) for a in range(sp)])
        )

    gate_rows = jnp.transpose(gate_weight.reshape(2, half, 4, lh), (0, 3, 2, 1)).reshape(
        2, lh, 4 * half // LANES, LANES
    )
    decay_rows = jnp.transpose(bf16_parts(decay_extra), (1, 2, 0, 3)).reshape(
        2, lh, 3 * tok // LANES, LANES
    )
    small = jnp.concatenate([gate_rows, decay_rows], axis=2)
    n_gate, n_small = gate_rows.shape[2], small.shape[2]
    n_rows = 6 * half + n_small
    spread, send = vmem_call(
        pack_kernel,
        (
            jax.ShapeDtypeStruct((2, 2, lh, n_rows, LANES), bf16),
            jax.ShapeDtypeStruct((lh, n_rows, LANES), bf16),
        ),
        smem=1,
        n_in=8,
    )(meta, mq_weight, mk_weight, mv_weight, mo_weight, aq_weight, ak_weight, av_weight, small)
    got = flip(send)
    got = jnp.broadcast_to(got[None, None], (2, 1) + got.shape)
    spread = lax.dynamic_update_slice_in_dim(spread, got, 1 - t, 1)
    own_w = lax.all_to_all(spread.reshape(sp * n_rows, LANES), "sp", 0, 0, tiled=True)
    for r in range(1, plane):
        other_xs.append(
            lax.ppermute(
                other, both_axes, [(core(a, False), core(a ^ r, False)) for a in range(sp)]
            )
        )
    out_block = jnp.concatenate([out_m_weight, out_a_weight], axis=0)
    column = [out_block]
    for r in range(1, sp // plane):
        column.append(lax.ppermute(out_block, "sp", [(a, a ^ (r * plane)) for a in range(sp)]))
    partner_w = flip(own_w)
    own_w = own_w.reshape(sp, n_rows, LANES)
    partner_w = partner_w.reshape(sp, n_rows, LANES)
    small_both = jnp.stack([own_w[:, 6 * half :], partner_w[:, 6 * half :]])
    small_both = jnp.where(t == 0, small_both, small_both[::-1])
    gate_t = jnp.transpose(small_both[:, :, :n_gate].reshape(2, sp, 4, half), (2, 1, 0, 3))
    gate_t = jnp.pad(gate_t.reshape(4, width), ((0, LANES - 4), (0, 0)))
    first = (2 * hi + t) * plane
    decay = lax.dynamic_slice_in_dim(small_both[:, :, n_gate:], first, plane, 1)
    decay = jnp.sum(decay.reshape(2, plane, 3, tok).astype(f32), axis=2)
    params = jnp.concatenate(
        [m_gain, gate_bias.reshape(-1), sink_logit, jnp.zeros((LANES - 6 * lh,), f32)]
    ).reshape(-1, LANES)
    params = jnp.stack([params, flip(params)])
    gain = params[:, :lh]
    bias = params[:, lh, : 4 * lh]
    sink = params[:, lh, 4 * lh : 6 * lh]

    quarter = plane * tok
    cols = 6 * LANES
    sum_rows = M_DIM + 8 + WINDOW
    proj, vrows, vcols, local, summary = vmem_call(
        project_kernel,
        (
            jax.ShapeDtypeStruct((quarter, cols), bf16),
            jax.ShapeDtypeStruct((6 * plane, tok), f32),
            jax.ShapeDtypeStruct((tok, LANES), f32),
            jax.ShapeDtypeStruct((2, plane, M_DIM, 2 * LANES), f32),
            jax.ShapeDtypeStruct((2, sum_rows, LANES), f32),
        ),
        scratch=[
            pltpu.VMEM((width, cols), bf16),
            pltpu.VMEM((plane, tok, width), bf16),
            pltpu.VMEM((2, sp, n_rows, LANES), bf16),
            pltpu.VMEM((plane, 8, tok), f32),
            pltpu.SemaphoreType.DMA((plane + 2,)),
        ],
        smem=2,
        n_any=2 * plane + 2,
        n_tail=2,
        flops=2 * quarter * width * cols,
    )(meta, bias, *same_xs, *other_xs, own_w, partner_w, gate_t, decay)
    column = jnp.concatenate(column, axis=0)
    cut = column.shape[0] // 2
    upper, lower = column[:cut], column[cut:]

    def hop(x, r):
        return lax.ppermute(x, "sp", [(a, a ^ r) for a in range(sp)])

    upper_1, lower_2 = hop(upper, 1), hop(lower, 2)
    upper_2, lower_1 = hop(upper, 2), hop(lower, 1)
    upper_3, lower_3 = hop(upper_1, 2), hop(lower_2, 1)
    out_blocks = [upper, lower, upper_1, lower_1, upper_2, lower_2, upper_3, lower_3]
    partner_sum = flip(summary)
    sent = vmem_call(
        combine_kernel, jax.ShapeDtypeStruct((sum_rows, LANES), f32), smem=1, n_in=2
    )(meta, summary, partner_sum)
    across = lax.ppermute(sent, "sp", [(a, (a + group) % sp) for a in range(sp)])
    blocks = quarter // WINDOW
    att, att_logs = vmem_call(
        attend_kernel,
        (
            jax.ShapeDtypeStruct((blocks, WINDOW, LANES), bf16),
            jax.ShapeDtypeStruct((blocks, 8, WINDOW), f32),
        ),
        scratch=[pltpu.VMEM((quarter + 2 * WINDOW, LANES), bf16)],
        smem=2,
        n_in=2,
        flops=quarter * width * cols,
    )(meta, sink, proj, partner_sum)
    spread, send = vmem_call(
        mixer_kernel,
        (
            jax.ShapeDtypeStruct((2, plane, tok + 16, LANES), bf16),
            jax.ShapeDtypeStruct((plane, tok + 16, LANES), bf16),
        ),
        scratch=[pltpu.VMEM((blocks, WINDOW, LANES), bf16), pltpu.VMEM((blocks, 8, WINDOW), f32)],
        smem=2,
        n_in=9,
        flops=quarter * width * cols,
    )(meta, sink, proj, vrows, vcols, local, partner_sum, across, gain, att, att_logs)
    got = flip(send)
    spread = lax.dynamic_update_slice_in_dim(spread, got[None], 1 - t, 0)
    groups = [list(range(g * group, (g + 1) * group)) for g in range(sp // group)]
    mine = lax.all_to_all(
        spread.reshape(group * (tok + 16), LANES),
        "sp",
        0,
        0,
        axis_index_groups=groups,
        tiled=True,
    )
    theirs = flip(mine)
    shape = (group, tok + 16, LANES)
    inner = 2 * group * LANES
    return vmem_call(
        output_kernel,
        (
            jax.ShapeDtypeStruct((tok, out_m_weight.shape[1]), bf16),
            jax.ShapeDtypeStruct((2 * lh, tok), f32),
        ),
        scratch=[
            pltpu.VMEM((2 * group, tok, LANES), bf16),
            pltpu.VMEM((inner, out_m_weight.shape[1]), bf16),
            pltpu.SemaphoreType.DMA((sp, 2)),
        ],
        smem=1,
        n_in=2,
        n_any=2 * plane,
        flops=2 * tok * inner * out_m_weight.shape[1],
    )(meta, mine.reshape(shape), theirs.reshape(shape), *out_blocks)


def solution(mesh):
    in_specs = (
        P("sp", None),
        P(),
        P("sp", "tp"),
        P("sp", "tp"),
        P("sp", "tp"),
        P("sp", "tp"),
        P("sp", None, "tp"),
        P(None, "tp"),
        P(None, "tp", "sp"),
        P("tp"),
        P("sp", "tp"),
        P("sp", "tp"),
        P("sp", "tp"),
        P("tp"),
        P("sp", "tp"),
        P("sp", "tp"),
    )
    out_specs = (P("sp", "tp"), P("tp", "sp"))

    def per_device(*args):
        plan = split_plan(mesh, args)
        if plan is None:
            return on_device(*args)
        return on_device_split(plan, *args)

    return jax.shard_map(
        per_device, mesh=mesh, in_specs=in_specs, out_specs=out_specs, check_vma=False
    )
```

```python
import jax
import jax.numpy as jnp
from jax import lax
import math

from jax.experimental import pallas as pl
from jax.experimental.pallas import tpu as pltpu
from jax.sharding import PartitionSpec as P

M_DIM = 128
W_DIM = 64
WINDOW = 128
M_BLOCK = 64


EPS = 1e-06
FLOOR_LOG = -1e30
HIGHEST = lax.Precision.HIGHEST


def with_halo(x, sides, width):
    for axis, dim in sides:
        peers, length = (lax.axis_size(axis), x.shape[dim])
        up = [(i, (i + 1) % peers) for i in range(peers - 1)]
        down = [(j, i) for i, j in up]
        last = lax.slice_in_dim(x, length - width, length, axis=dim)
        first = lax.slice_in_dim(x, 0, width, axis=dim)
        before = lax.ppermute(last, axis, up)
        after = lax.ppermute(first, axis, down)
        x = jnp.concatenate([before, x, after], axis=dim)
    return x


def rms_rows(inputs, gain_vec):
    return inputs * lax.rsqrt(jnp.mean(inputs * inputs, axis=-1, keepdims=True) + EPS) * gain_vec


def stored(result):
    return lax.optimization_barrier(result.astype(jnp.bfloat16))


def flip_tokens(array_in):
    return jnp.flip(array_in, axis=1)


def block_pass(queries, key_vecs, value_vecs, in_gate, log_forget, start_state):
    head_count, length, head_width = queries.shape
    block_count = length // M_BLOCK

    def blocks(array_in):
        return jnp.moveaxis(
            array_in.reshape((head_count, block_count, M_BLOCK) + array_in.shape[2:]), 1, 0
        )

    lower_mask = jnp.tril(jnp.ones((M_BLOCK, M_BLOCK), dtype=bool))

    def advance(state_in, block_in):
        cell_mat, norm_vec, stab_max = state_in
        q_blk, k_blk, v_blk, i_blk, f_blk = block_in
        cum_log = jnp.cumsum(f_blk, axis=-1)
        seg_total = cum_log[:, -1]
        log_end = seg_total[:, None] - cum_log + i_blk
        max_next = jnp.maximum(seg_total + stab_max, jnp.max(log_end, axis=-1))
        w_end = jnp.exp(log_end - max_next[:, None])
        fade_old = jnp.exp(seg_total + stab_max - max_next)
        cell_next = fade_old[:, None, None] * cell_mat + jnp.einsum(
            "hsv,hsk->hvk", w_end[:, :, None] * v_blk, k_blk, precision=HIGHEST
        )
        norm_next = fade_old[:, None] * norm_vec + jnp.einsum(
            "hs,hsk->hk", w_end, k_blk, precision=HIGHEST
        )
        log_w = jnp.where(
            lower_mask, cum_log[:, :, None] - cum_log[:, None, :] + i_blk[:, None, :], -jnp.inf
        )
        log_inter = cum_log + stab_max[:, None]
        row_max = jnp.maximum(log_inter, jnp.max(log_w, axis=-1))
        w_intra = jnp.exp(log_w - row_max[:, :, None])
        w_inter = jnp.exp(log_inter - row_max)
        scores = jnp.einsum("htk,hsk->hts", q_blk, k_blk, precision=HIGHEST) * w_intra
        numerator = jnp.einsum("hts,hsv->htv", scores, v_blk, precision=HIGHEST) + w_inter[
            ..., None
        ] * jnp.einsum("hvk,htk->htv", cell_mat, q_blk, precision=HIGHEST)
        denominator = jnp.sum(scores, axis=-1) + w_inter * jnp.einsum(
            "hk,htk->ht", norm_vec, q_blk, precision=HIGHEST
        )
        result_rows = numerator / jnp.maximum(jnp.abs(denominator), jnp.exp(-row_max))[..., None]
        return ((cell_next, norm_next, max_next), result_rows)

    final_state, outputs = lax.scan(
        advance,
        start_state,
        tuple(
            (blocks(array_in) for array_in in (queries, key_vecs, value_vecs, in_gate, log_forget))
        ),
    )
    return (jnp.moveaxis(outputs, 0, 1).reshape(head_count, length, head_width), final_state)


def summarize(key_vecs, value_vecs, in_gate, log_forget):
    cum_log = jnp.cumsum(log_forget, axis=-1)
    seg_total = cum_log[:, -1]
    log_end = seg_total[:, None] - cum_log + in_gate
    peak_log = jnp.max(log_end, axis=-1)
    weights_end = jnp.exp(log_end - peak_log[:, None])
    cell_mat = jnp.einsum(
        "hsv,hsk->hvk", weights_end[:, :, None] * value_vecs, key_vecs, precision=HIGHEST
    )
    norm_vec = jnp.einsum("hs,hsk->hk", weights_end, key_vecs, precision=HIGHEST)
    return (seg_total, cell_mat, norm_vec, peak_log)


def merge_side(state_in, cell_mats, norm_vecs, logs, usable):
    cell_mat, norm_vec, peak_log = state_in
    masked = jnp.where(usable, logs, FLOOR_LOG)
    new_peak = jnp.maximum(peak_log, jnp.max(masked, axis=0))
    scales = jnp.where(usable, jnp.exp(masked - new_peak[None]), 0.0)
    cell_mat = jnp.einsum("jh,jhvk->hvk", scales, cell_mats, precision=HIGHEST)
    norm_vec = jnp.einsum("jh,jhk->hk", scales, norm_vecs, precision=HIGHEST)
    return (cell_mat, norm_vec, new_peak)


def gather_states(forward_sum, backward_sum):
    decay_all = (
        lax.all_gather(forward_sum[0][None], "sp", axis=0, tiled=True),
        lax.all_gather(backward_sum[0][None], "sp", axis=0, tiled=True),
    )
    own_index = lax.axis_index("sp")
    acc_fwd = jnp.cumsum(decay_all[0], axis=0)
    acc_bwd = jnp.cumsum(decay_all[1], axis=0)
    before_own = lax.dynamic_index_in_dim(acc_fwd - decay_all[0], own_index, 0, keepdims=False)
    after_own = lax.dynamic_index_in_dim(acc_bwd, own_index, 0, keepdims=False)
    lead_bwd = acc_bwd - decay_all[1]
    empty_side = (
        jnp.zeros_like(forward_sum[1]),
        jnp.zeros_like(forward_sum[2]),
        jnp.full_like(forward_sum[3], FLOOR_LOG),
    )
    state_in = empty_side + empty_side
    pieces = (
        lax.all_gather(forward_sum[1][None], "sp", axis=0, tiled=True),
        lax.all_gather(forward_sum[2][None], "sp", axis=0, tiled=True),
        lax.all_gather(forward_sum[3][None], "sp", axis=0, tiled=True),
        lax.all_gather(backward_sum[1][None], "sp", axis=0, tiled=True),
        lax.all_gather(backward_sum[2][None], "sp", axis=0, tiled=True),
        lax.all_gather(backward_sum[3][None], "sp", axis=0, tiled=True),
    )
    piece_count = pieces[0].shape[0]
    device_ids = jnp.arange(piece_count, dtype=jnp.int32)
    log_fwd = before_own[None] - acc_fwd + pieces[2]
    log_bwd = lead_bwd - after_own[None] + pieces[5]
    left_side = merge_side(
        state_in[:3], pieces[0], pieces[1], log_fwd, (device_ids < own_index)[:, None]
    )
    right_side = merge_side(
        state_in[3:], pieces[3], pieces[4], log_bwd, (device_ids > own_index)[:, None]
    )
    states = left_side + right_side
    return (states[:3], states[3:])


def window_attend(a_query, kv_pairs, sink_logit, first_row, total_rows):
    tok_rows = a_query.shape[0]
    block_len = WINDOW
    block_count = tok_rows // block_len
    kv_width = kv_pairs.shape[1] // 2
    kv_heads = kv_width // W_DIM
    q_heads = a_query.shape[1] // W_DIM
    groups = q_heads // kv_heads
    filled_margin = with_halo(kv_pairs, (("sp", 0),), WINDOW)
    windows = jnp.concatenate(
        [
            filled_margin[place_idx * block_len : place_idx * block_len + tok_rows].reshape(
                block_count, block_len, 2 * kv_width
            )
            for place_idx in range(3)
        ],
        axis=1,
    )
    key_block = windows[:, :, :kv_width].reshape(block_count, 3 * block_len, kv_heads, W_DIM)
    content_tile = windows[:, :, kv_width:].reshape(block_count, 3 * block_len, kv_heads, W_DIM)
    query_block = a_query.reshape(block_count, block_len, kv_heads, groups, W_DIM)
    scores = jnp.einsum(
        "nqgrd,nkgd->ngrqk", query_block, key_block, preferred_element_type=jnp.float32
    ) * W_DIM ** (-0.5)
    query_off = jnp.arange(block_len, dtype=jnp.int32)
    key_off = jnp.arange(3 * block_len, dtype=jnp.int32) - block_len
    in_window = jnp.abs(query_off[:, None] - key_off[None, :]) <= WINDOW
    key_place = (
        first_row + jnp.arange(block_count, dtype=jnp.int32)[:, None] * block_len + key_off[None, :]
    )
    inside = (key_place >= 0) & (key_place < total_rows)
    usable = in_window[None] & inside[:, None, :]
    scores = jnp.where(usable[:, None, None], scores, -jnp.inf)
    sink_col = sink_logit.reshape(kv_heads, groups)[None, :, :, None]
    peak_log = jnp.maximum(sink_col, jnp.max(scores, axis=-1))
    weights_exp = jnp.exp(scores - peak_log[..., None])
    weight_total_sum = jnp.exp(sink_col - peak_log) + jnp.sum(weights_exp, axis=-1)
    weighted = jnp.einsum(
        "ngrqk,nkgd->nqgrd",
        weights_exp.astype(jnp.bfloat16),
        content_tile,
        preferred_element_type=jnp.float32,
    )
    scale_back = jnp.transpose(weight_total_sum, (0, 3, 1, 2))[..., None]
    mixed_rows = (weighted / scale_back).astype(jnp.bfloat16).reshape(tok_rows, q_heads * W_DIM)
    log_total = jnp.transpose(peak_log + jnp.log(weight_total_sum), (1, 2, 0, 3)).reshape(
        q_heads, tok_rows
    )
    return (mixed_rows, log_total)


def on_device(
    tokens,
    input_norm_gain,
    mq_weight,
    mk_weight,
    mv_weight,
    mo_weight,
    gate_weight,
    gate_bias,
    decay_extra,
    m_gain,
    aq_weight,
    ak_weight,
    av_weight,
    sink_logit,
    out_m_weight,
    out_a_weight,
):
    tok_rows = tokens.shape[0]
    normed = rms_rows(tokens.astype(jnp.float32), input_norm_gain).astype(jnp.bfloat16)
    local_heads = gate_weight.shape[2]
    gate_cols = 4 * local_heads
    pieces = (
        lax.all_gather(mq_weight, "sp", axis=0, tiled=True),
        lax.all_gather(mk_weight, "sp", axis=0, tiled=True),
        lax.all_gather(mv_weight, "sp", axis=0, tiled=True),
        lax.all_gather(mo_weight, "sp", axis=0, tiled=True),
        lax.all_gather(gate_weight, "sp", axis=0, tiled=True),
        lax.all_gather(aq_weight, "sp", axis=0, tiled=True),
        lax.all_gather(ak_weight, "sp", axis=0, tiled=True),
        lax.all_gather(av_weight, "sp", axis=0, tiled=True),
    )
    piece_rows = pieces[0].shape[0]
    flat_gate = pieces[4].reshape(piece_rows, gate_cols)
    segments = (
        pieces[0],
        pieces[1],
        pieces[2],
        pieces[3],
        flat_gate,
        pieces[5],
        pieces[6],
        pieces[7],
    )
    projected = tuple(
        (jnp.dot(normed, segment, preferred_element_type=jnp.float32) for segment in segments)
    )
    m_query = stored(projected[0])
    m_key = stored(projected[1])
    m_value = stored(projected[2])
    m_out = stored(projected[3])
    gates = projected[4].reshape(tok_rows, 4, local_heads) + gate_bias[None]

    def heads_first(matrix):
        return jnp.transpose(
            matrix.astype(jnp.float32).reshape(tok_rows, local_heads, M_DIM), (1, 0, 2)
        )

    queries = heads_first(m_query)
    key_vecs = heads_first(m_key) * M_DIM ** (-0.5)
    value_vecs = heads_first(m_value)
    in_fwd = gates[:, 0, :].T
    forget_fwd = jax.nn.log_sigmoid(gates[:, 1, :].T) + decay_extra[0]
    in_bwd = flip_tokens(gates[:, 2, :].T)
    forget_bwd = flip_tokens(jax.nn.log_sigmoid(gates[:, 3, :].T) + decay_extra[1])
    queries_bwd = flip_tokens(queries)
    keys_bwd = flip_tokens(key_vecs)
    values_bwd = flip_tokens(value_vecs)
    forward_sum = summarize(key_vecs, value_vecs, in_fwd, forget_fwd)
    backward_sum = summarize(keys_bwd, values_bwd, in_bwd, forget_bwd)
    state_fwd, state_bwd = gather_states(forward_sum, backward_sum)
    hidden_fwd, _ = block_pass(queries, key_vecs, value_vecs, in_fwd, forget_fwd, state_fwd)
    hidden_bwd, _ = block_pass(queries_bwd, keys_bwd, values_bwd, in_bwd, forget_bwd, state_bwd)
    cell_out = hidden_fwd + flip_tokens(hidden_bwd)
    gate_open = jax.nn.sigmoid(m_out.astype(jnp.float32)).reshape(tok_rows, local_heads, M_DIM)
    cell_rows = jnp.transpose(cell_out, (1, 0, 2)) * gate_open
    mixed_m = (
        rms_rows(cell_rows, m_gain.reshape(local_heads, M_DIM))
        .astype(jnp.bfloat16)
        .reshape(tok_rows, local_heads * M_DIM)
    )
    a_query = stored(projected[5])
    kv_pairs = jnp.concatenate([stored(projected[6]), stored(projected[7])], axis=1)
    first_row = lax.axis_index("sp") * tok_rows
    total_rows = tok_rows * lax.axis_size("sp")
    mixed_a, log_total = window_attend(a_query, kv_pairs, sink_logit, first_row, total_rows)
    full_m, full_a = (
        lax.all_gather(mixed_m, "tp", axis=1, tiled=True),
        lax.all_gather(mixed_a, "tp", axis=1, tiled=True),
    )
    pieces = (
        lax.all_gather(out_m_weight, "sp", axis=0, tiled=True),
        lax.all_gather(out_a_weight, "sp", axis=0, tiled=True),
    )
    running = jnp.dot(full_m, pieces[0], preferred_element_type=jnp.float32)
    mixed = running + jnp.dot(full_a, pieces[1], preferred_element_type=jnp.float32)
    return (mixed.astype(jnp.bfloat16), log_total)


CHUNK = 256
LANES = 128
EMPTY = -1e30


def split_plan(mesh, args):
    sp, tp = mesh.shape["sp"], mesh.shape["tp"]
    tok_rows, width = args[0].shape
    rows = args[2].shape[0]
    local_heads = args[6].shape[2]
    group = local_heads * tp
    if tp != 2 or sp != 2 * group or group != 8:
        return None
    plane = group // 2
    ok = (
        args[2].shape[1] == local_heads * M_DIM
        and args[10].shape[1] == local_heads * LANES
        and args[11].shape[1] == local_heads * W_DIM
        and args[12].shape[1] == local_heads * W_DIM
        and 2 * W_DIM == LANES
        and M_DIM == LANES
        and WINDOW == LANES
        and tok_rows == CHUNK
        and rows == LANES
        and args[14].shape[0] * sp == group * M_DIM
        and args[15].shape[0] * sp == group * LANES
    )
    if not ok:
        return None
    return dict(
        sp=sp, tp=tp, tok=tok_rows, width=width, rows=rows, lh=local_heads, group=group, plane=plane
    )


def mm(a, b, ca=1, cb=0, precision=None):
    return lax.dot_general(
        a, b, (((ca,), (cb,)), ((), ())), precision=precision, preferred_element_type=jnp.float32
    )


def vmem_call(kernel, outs, scratch=(), smem=0, n_in=0, flops=0, n_any=0, n_tail=0, keep=False):
    return pl.pallas_call(
        kernel,
        out_shape=jax.tree.map(lambda x: pltpu.VMEM(x.shape, x.dtype), outs) if keep else outs,
        in_specs=[pl.BlockSpec(memory_space=pltpu.SMEM)] * smem
        + [pl.BlockSpec(memory_space=pltpu.VMEM)] * n_in
        + [pl.BlockSpec(memory_space=pl.ANY)] * n_any
        + [pl.BlockSpec(memory_space=pltpu.VMEM)] * n_tail,
        out_specs=jax.tree.map(lambda _: pl.BlockSpec(memory_space=pltpu.VMEM), outs),
        scratch_shapes=scratch,
        cost_estimate=pl.CostEstimate(flops=flops, bytes_accessed=0, transcendentals=0),
        compiler_params=pltpu.CompilerParams(vmem_limit_bytes=24 * 1024 * 1024),
    )


def near(*arrays):
    return [pltpu.with_memory_space_constraint(x, pltpu.VMEM) for x in arrays]


def pack_kernel(meta, mq, mk, mv, mo, aq, ak, av, small, keep, send):
    t = meta[0]
    copies, heads = keep.shape[0], keep.shape[2]
    rows = mq.shape[0] // 2
    at = pl.multiple_of(t * rows, rows)
    away = pl.multiple_of((1 - t) * rows, rows)
    for h in range(heads):
        lanes = slice(h * LANES, (h + 1) * LANES)
        narrow = slice(h * W_DIM, (h + 1) * W_DIM)
        for start, mine in ((at, True), (away, False)):
            parts = [ref[pl.ds(start, rows), lanes] for ref in (mq, mk, mv, mo, aq)]
            parts.append(
                jnp.concatenate([ref[pl.ds(start, rows), narrow] for ref in (ak, av)], axis=1)
            )
            parts.append(small[t if mine else 1 - t, h])
            row = 0
            for part in parts:
                span = slice(row, row + part.shape[0])
                row += part.shape[0]
                if mine:
                    for i in range(copies):
                        keep[i, t, h, span, :] = part
                else:
                    send[h, span, :] = part


def running_max(x, backward):
    n = x.shape[1]
    lane = lax.broadcasted_iota(jnp.int32, x.shape, 1)
    step = 1
    while step < n:
        if backward:
            moved = jnp.where(lane < n - step, pltpu.roll(x, n - step, 1), EMPTY)
        else:
            moved = jnp.where(lane >= step, pltpu.roll(x, step, 1), EMPTY)
        x = jnp.maximum(x, moved)
        step *= 2
    return x


def with_ones(value):
    lane = lax.broadcasted_iota(jnp.int32, value.shape, 1)
    ones = jnp.where(lane == 0, 1.0, 0.0).astype(value.dtype)
    return jnp.concatenate([value, ones], axis=1)


def merge(earlier, later, later_total):
    peak = jnp.maximum(later_total + earlier[1], later[1])
    old = jnp.exp(later_total + earlier[1] - peak)
    new = jnp.exp(later[1] - peak)
    return old * earlier[0] + new * later[0], peak


def weave_kernel(meta, own, partner, weight, gate_t, decay):
    t, hi = meta[0], meta[4]
    sources = own.shape[0]
    rows = weight.shape[0] // sources // 2
    cols = weight.shape[1] // LANES
    plane = decay.shape[1]
    for i in range(sources):
        first = pl.multiple_of((2 * i + t) * rows, rows)
        second = pl.multiple_of((2 * i + 1 - t) * rows, rows)
        for c in range(cols):
            lanes = slice(c * LANES, (c + 1) * LANES)
            span = slice(c * rows, (c + 1) * rows)
            weight[pl.ds(first, rows), lanes] = own[i, span, :]
            weight[pl.ds(second, rows), lanes] = partner[i, span, :]

    def small(ref, i):
        return ref[i, cols * rows :, :].astype(jnp.float32)

    gate_t[...] = jnp.zeros(gate_t.shape, jnp.bfloat16)
    for i in range(sources):
        pair = [
            jnp.concatenate(
                [x[0:1, :rows], x[0:1, rows:], x[1:2, :rows], x[1:2, rows:]], axis=0
            )
            for x in (small(own, i), small(partner, i))
        ]
        piece = jnp.where(
            t == 0,
            jnp.concatenate(pair, axis=1),
            jnp.concatenate(pair[::-1], axis=1),
        )
        piece = jnp.concatenate([piece, jnp.zeros((12, LANES), jnp.float32)], axis=0)
        gate_t[:16, i * LANES : (i + 1) * LANES] = piece.astype(jnp.bfloat16)
    for b in range(plane):
        for ref, at in ((own, t), (partner, 1 - t)):
            x = small(ref, (2 * hi + t) * plane + b)
            x = x[2:4] + x[4:6] + x[6:8]
            decay[at, b : b + 1, :] = jnp.concatenate([x[:1], x[1:]], axis=1)


def project_kernel(meta, bias, *refs):
    plane = (len(refs) - 11) // 2
    same, other = refs[:plane], refs[plane : 2 * plane]
    weight, gate_t, decay = refs[2 * plane : 2 * plane + 3]
    proj, vrows, vcols, local, summary, xs, gates, sems = refs[2 * plane + 3 :]
    t, k, sel, jl, near = meta[0], meta[1], meta[2], meta[3], meta[5]

    @pl.when(t == near)
    def _():
        for r in range(plane):
            pltpu.make_async_copy(same[r], xs.at[r], sems.at[r]).start()

    @pl.when(t != near)
    def _():
        for r in range(plane):
            pltpu.make_async_copy(other[r], xs.at[r], sems.at[r]).start()

    tok = xs.shape[1]
    for r in range(plane):
        pltpu.make_async_copy(same[r], xs.at[r], sems.at[r]).wait()
        at = pl.ds(pl.multiple_of((k ^ r) * tok, tok), tok)
        proj[at, :] = mm(xs[r], weight[...]).astype(jnp.bfloat16)
        gates[k ^ r] = jnp.transpose(mm(xs[r], gate_t[...], 1, 1))[:8]
    heads = bias.shape[1] // 4
    b = [bias[sel, g * heads + jl] for g in range(4)]
    g = [
        jnp.concatenate([gates[c, i : i + 1] for c in range(plane)], axis=0) + b[i]
        for i in range(4)
    ]

    def forget(i, direction):
        x = g[i]
        return jnp.minimum(x, 0.0) - jnp.log1p(jnp.exp(-jnp.abs(x))) + decay[direction]

    lf_f, lf_b = forget(1, 0), forget(3, 1)
    r = lax.broadcasted_iota(jnp.int32, (tok, tok), 0)
    c = lax.broadcasted_iota(jnp.int32, (tok, tok), 1)
    lower = jnp.where(r >= c, 1.0, 0.0).astype(jnp.float32)
    cum = mm(jnp.concatenate([lf_f, lf_b], axis=0), lower, 1, 1, HIGHEST)
    lead_f, lead_b = cum[:plane], lf_b - cum[plane:]
    src_f, src_b = g[0] - lead_f, g[2] - lead_b
    top_f, top_b = running_max(src_f, False), running_max(src_b, True)
    total_f, total_b = lead_f[:, tok - 1 :], cum[plane:, tok - 1 :]
    best_f, best_b = top_f[:, tok - 1 :], top_b[:, :1]
    end_f, end_b = jnp.exp(src_f - best_f), jnp.exp(src_b - best_b)
    peak_f, peak_b = best_f + total_f, best_b

    def wide(x):
        return jnp.broadcast_to(x, (plane, tok))

    vrows[...] = jnp.concatenate(
        [src_f, src_b, wide(total_f), wide(total_b), wide(peak_f), wide(peak_b)], axis=0
    )
    stack = [top_f, top_b, lead_f, lead_b, end_f, end_b]
    stack.append(jnp.zeros((LANES - 6 * plane, tok), jnp.float32))
    cols_all = jnp.transpose(jnp.concatenate(stack, axis=0))
    vcols[...] = cols_all
    for ch in range(plane):
        span = slice(ch * tok, (ch + 1) * tok)
        key = proj[span, LANES : 2 * LANES].astype(jnp.float32)
        value = with_ones(proj[span, 2 * LANES : 3 * LANES])
        for i in range(2):
            at = (4 + i) * plane + ch
            weighted = (key * cols_all[:, at : at + 1]).astype(jnp.bfloat16)
            local[i, ch] = mm(weighted, value, 0, 0)
    for i in range(2):
        state = (jnp.zeros((M_DIM, 2 * LANES), jnp.float32), jnp.full((1, 1), EMPTY, jnp.float32))
        total = jnp.zeros((1, 1), jnp.float32)
        for ch in range(plane) if i == 0 else range(plane - 1, -1, -1):
            chunk_total, chunk_peak = chunk_scalars(vrows, i, ch, plane)
            state = merge(state, (local[i, ch], chunk_peak), chunk_total)
            total = total + chunk_total
        summary[i, :M_DIM, :] = state[0][:, :LANES]
        summary[i, M_DIM : M_DIM + 8, :] = jnp.concatenate(
            [
                jnp.transpose(state[0][:, LANES:])[:1],
                jnp.broadcast_to(state[1], (1, LANES)),
                jnp.broadcast_to(total, (1, LANES)),
                jnp.zeros((5, LANES), jnp.float32),
            ],
            axis=0,
        )
    last = proj.shape[0]
    summary[0, M_DIM + 8 :, :] = proj[:WINDOW, 5 * LANES :].astype(jnp.float32)
    summary[1, M_DIM + 8 :, :] = proj[last - WINDOW :, 5 * LANES :].astype(jnp.float32)


def chunk_scalars(vrows, i, ch, plane):
    total, peak = (2 + i) * plane + ch, (4 + i) * plane + ch
    return vrows[total : total + 1, :1], vrows[peak : peak + 1, :1]


def packed_state(ref, i):
    rows = ref[i, : M_DIM + 8, :]
    return (rows, rows[M_DIM + 1 : M_DIM + 2, :1]), rows[M_DIM + 2 : M_DIM + 3, :1]


def open_state(packed):
    rows, peak = packed
    first = lax.broadcasted_iota(jnp.int32, (LANES, LANES), 0) == 0
    norm = jnp.transpose(jnp.where(first, rows[M_DIM : M_DIM + 1], 0.0))
    return jnp.concatenate([rows[:M_DIM], norm], axis=1), peak


def combine_kernel(meta, own, partner, out):
    t, hi = meta[0], meta[4]
    forward = hi == 0
    i = jnp.where(forward, 0, 1)
    (mine, mine_peak), mine_total = packed_state(own, i)
    (other, other_peak), other_total = packed_state(partner, i)
    mine_later = (t == 1) == forward

    def pick(x, y):
        return jnp.where(mine_later, x, y)

    rows, peak = merge(
        (pick(other, mine), pick(other_peak, mine_peak)),
        (pick(mine, other), pick(mine_peak, other_peak)),
        pick(mine_total, other_total),
    )
    out[: M_DIM + 8, :] = rows
    out[M_DIM + 1 : M_DIM + 2, :] = jnp.broadcast_to(peak, (1, LANES))
    out[M_DIM + 8 :, :] = partner[jnp.where(forward, 1, 0), M_DIM + 8 :, :]


def attend(q, kv, sinks, drop_first, drop_last):
    n = q.shape[0]
    q = q * jnp.bfloat16(W_DIM ** (-0.5))
    q = jnp.concatenate([q[:, :W_DIM], q[:, W_DIM:]], axis=0)
    r = lax.broadcasted_iota(jnp.int32, (2 * n, n), 0)
    c = lax.broadcasted_iota(jnp.int32, (2 * n, n), 1)
    row = jnp.where(r >= n, r - n, r)
    sink = jnp.where(
        lax.broadcasted_iota(jnp.int32, (2 * n, 1), 0) < n, sinks[0], sinks[1]
    )
    s = [mm(q, kv[i * n : (i + 1) * n, :W_DIM], 1, 1) for i in range(3)]
    before, after = c >= row, c <= row
    if drop_first is not None:
        before = before & jnp.logical_not(drop_first)
        after = after & jnp.logical_not(drop_last)
    s[0] = jnp.where(before, s[0], EMPTY)
    s[2] = jnp.where(after, s[2], EMPTY)
    peak = jnp.max(jnp.maximum(jnp.maximum(s[0], s[1]), s[2]), axis=1, keepdims=True)
    peak = jnp.maximum(peak, sink)
    e = [jnp.exp(x - peak) for x in s]
    total = jnp.exp(sink - peak) + jnp.sum(e[0] + e[1] + e[2], axis=1, keepdims=True)
    weights = jnp.concatenate([x.astype(jnp.bfloat16) for x in e], axis=1)
    mixed = mm(weights, kv[:, W_DIM:]) / total
    mixed = jnp.concatenate([mixed[:n], mixed[n:]], axis=1).astype(jnp.bfloat16)
    log_col = peak + jnp.log(total)
    diag = (c == row)
    logs = [
        jnp.sum(jnp.where(diag[:n], log_col[h * n : (h + 1) * n], 0.0), axis=0, keepdims=True)
        for h in range(2)
    ]
    return mixed, jnp.concatenate(logs + [jnp.zeros((6, n), jnp.float32)], axis=0)


def attend_kernel(meta, sink, proj, partner, mixed, logs, kv):
    t, sel, jl = meta[0], meta[2], meta[3]
    length = proj.shape[0]
    edge = partner[jnp.where(t == 0, 0, 1), M_DIM + 8 :, :].astype(jnp.bfloat16)
    kv[:WINDOW, :] = edge
    kv[WINDOW : WINDOW + length, :] = proj[:, 5 * LANES :]
    kv[WINDOW + length :, :] = edge
    sinks = (sink[sel, 2 * jl], sink[sel, 2 * jl + 1])
    for i in range(length // WINDOW - 1):
        b = i + 1 - t
        at = pl.multiple_of(b * WINDOW, WINDOW)
        q = proj[pl.ds(at, WINDOW), 4 * LANES : 5 * LANES]
        mixed[b], logs[b] = attend(q, kv[pl.ds(at, 3 * WINDOW), :], sinks, None, None)


def mixer_kernel(
    meta, sink, proj, vrows, vcols, local, partner, across, gain, att, att_logs, keep, send, am, al
):
    t, sel, jl, hi = meta[0], meta[2], meta[3], meta[4]
    tok = vrows.shape[1]
    chunks = vrows.shape[0] // 6

    def store(is_cell, c, span, value):
        @pl.when((t == 0) == is_cell)
        def _():
            keep[t, c, span, :] = value

        @pl.when((t == 0) != is_cell)
        def _():
            send[c, span, :] = value

    length = proj.shape[0]
    blocks = length // WINDOW
    am[...] = att[...]
    al[...] = att_logs[...]
    outer = across[M_DIM + 8 :, :].astype(jnp.bfloat16)
    inside = proj[pl.ds(pl.multiple_of(t * (length - 2 * WINDOW), WINDOW), 2 * WINDOW), 5 * LANES :]
    kv = jnp.where(
        t == 0,
        jnp.concatenate([outer, inside], axis=0),
        jnp.concatenate([inside, outer], axis=0),
    )
    sinks = (sink[sel, 2 * jl], sink[sel, 2 * jl + 1])
    at = pl.multiple_of(t * (length - WINDOW), WINDOW)
    q = proj[pl.ds(at, WINDOW), 4 * LANES : 5 * LANES]
    edge = t * (blocks - 1)
    am[edge], al[edge] = attend(q, kv, sinks, (t == 0) & (hi == 0), (t == 1) & (hi == 1))

    far = across[: M_DIM + 8, :]
    far_peak = across[M_DIM + 1 : M_DIM + 2, :1]

    def incoming(i, use_far, use_near):
        (near, near_peak), near_total = packed_state(partner, i)
        return open_state(
            merge(
                (far, jnp.where(use_far, far_peak, EMPTY)),
                (near, jnp.where(use_near, near_peak, EMPTY)),
                jnp.where(use_near, near_total, 0.0),
            )
        )

    fwd = incoming(0, hi == 1, t == 1)
    bwd = incoming(1, hi == 0, t == 0)
    entering = [[None, None] for _ in range(chunks)]
    for c in range(chunks):
        entering[c][0] = fwd
        total, peak = chunk_scalars(vrows, 0, c, chunks)
        if c + 1 < chunks:
            fwd = merge(fwd, (local[0, c], peak), total)
    for c in range(chunks - 1, -1, -1):
        total, peak = chunk_scalars(vrows, 1, c, chunks)
        entering[c][1] = (bwd[0], bwd[1] + total)
        if c:
            bwd = merge(bwd, (local[1, c], peak), total)
    r = lax.broadcasted_iota(jnp.int32, (tok, tok), 0)
    col = lax.broadcasted_iota(jnp.int32, (tok, tok), 1)
    gain_row = gain[sel, pl.ds(jl, 1), :]
    floor_lift = 0.5 * math.log(M_DIM)
    for c in range(chunks):
        span = slice(c * tok, (c + 1) * tok)
        q = proj[span, :LANES]
        value = with_ones(proj[span, 2 * LANES : 3 * LANES])
        scores = mm(q, proj[span, LANES : 2 * LANES], 1, 1)
        cell_out = None
        for i, mask in enumerate((r >= col, r <= col)):
            cell, reach = entering[c][i]
            at = i * chunks + c
            src = vrows[at : at + 1, :]
            top = jnp.maximum(vcols[:, at : at + 1], reach)
            lead = vcols[:, at + 2 * chunks : at + 2 * chunks + 1]
            w = jnp.where(mask, jnp.exp(src - top), 0.0)
            both = mm((scores * w).astype(jnp.bfloat16), value) + jnp.exp(reach - top) * mm(
                q, cell.astype(jnp.bfloat16)
            )
            denom = jnp.abs(both[:, LANES : LANES + 1])
            inv = 1.0 / jnp.maximum(denom, jnp.exp(floor_lift - (lead + top)))
            part = both[:, :LANES] * inv
            cell_out = part if cell_out is None else cell_out + part
        gate = proj[span, 3 * LANES : 4 * LANES].astype(jnp.float32)
        u = cell_out / (1.0 + jnp.exp(-gate))
        u = u * lax.rsqrt(jnp.mean(u * u, axis=1, keepdims=True) + EPS) * gain_row
        tail = jnp.zeros((16, LANES), jnp.bfloat16)
        store(True, c, slice(0, tok + 16), jnp.concatenate([u.astype(jnp.bfloat16), tail], axis=0))

    per = tok // WINDOW
    for c in range(chunks):
        x = jnp.concatenate(
            [al[c * per + p][h : h + 1] for h in range(2) for p in range(per)], axis=0
        )
        high = x.astype(jnp.bfloat16).astype(jnp.float32)
        mid = (x - high).astype(jnp.bfloat16).astype(jnp.float32)
        low = x - high - mid
        pad = jnp.zeros((16 - 3 * 2 * per, LANES), jnp.float32)
        tail = jnp.concatenate([high, mid, low, pad], axis=0).astype(jnp.bfloat16)
        rows = [am[c * per + p] for p in range(per)] + [tail]
        store(False, c, slice(0, tok + 16), jnp.concatenate(rows, axis=0))


def output_kernel(meta, own, partner, *refs):
    mixed, log_total, left, weight, sems = refs[-5:]
    blocks = refs[:-5]
    t, p, z = meta[0], meta[1], meta[6]
    plane = len(blocks) // 2
    heads, tok = own.shape[0], mixed.shape[0]
    planes = sems.shape[0] // plane
    rows = 2 * blocks[0].shape[0] // planes
    half = rows // 2
    total = weight.shape[0] // 2
    copies = []
    for r in range(plane):
        for zr in range(planes):
            source = (z ^ zr) * plane + (p ^ r)
            for i in range(2):
                to = pl.multiple_of(i * total + source * half, half)
                copies.append(
                    pltpu.make_async_copy(
                        blocks[2 * r + 2 * zr // planes].at[
                            pl.ds(zr % (planes // 2) * rows + i * half, half)
                        ],
                        weight.at[pl.ds(to, half)],
                        sems.at[r * planes + zr, i],
                    )
                )
    for copy in copies:
        copy.start()
    for j in range(heads):
        left[t * heads + j] = own[j, :tok, :]
        left[(1 - t) * heads + j] = partner[j, :tok, :]
    lhs = jnp.concatenate([left[i] for i in range(2 * heads)], axis=1)
    for copy in copies:
        copy.wait()
    mixed[...] = mm(lhs, weight[...]).astype(jnp.bfloat16)
    per = tok // LANES
    n = 2 * per
    for i in range(heads // 2):
        j = t * (heads // 2) + i
        rows = jnp.where(t == 1, own[j, tok:, :], partner[j, tok:, :]).astype(jnp.float32)
        x = rows[:n] + rows[n : 2 * n] + rows[2 * n : 3 * n]
        for h in range(2):
            log_total[2 * i + h : 2 * i + h + 1, :] = jnp.concatenate(
                [x[h * per + p : h * per + p + 1] for p in range(per)], axis=1
            )


def bf16_parts(x):
    high = lax.reduce_precision(x, 8, 7)
    mid = lax.reduce_precision(x - high, 8, 7)
    return jnp.stack([high, mid, x - high - mid]).astype(jnp.bfloat16)


def on_device_split(
    plan,
    tokens,
    input_norm_gain,
    mq_weight,
    mk_weight,
    mv_weight,
    mo_weight,
    gate_weight,
    gate_bias,
    decay_extra,
    m_gain,
    aq_weight,
    ak_weight,
    av_weight,
    sink_logit,
    out_m_weight,
    out_a_weight,
):
    sp, group, plane, lh, tok = (plan[n] for n in ("sp", "group", "plane", "lh", "tok"))
    width, rows = plan["width"], plan["rows"]
    half = rows // 2
    f32, bf16 = jnp.float32, jnp.bfloat16
    s = lax.axis_index("sp").astype(jnp.int32)
    t = lax.axis_index("tp").astype(jnp.int32)
    hi, j = s // group, s % group
    near_plane = (s // plane) % 2
    meta = jnp.stack(
        [t, s % plane, jnp.where(j // lh == t, 0, 1), j % lh, hi, near_plane, s // plane]
    ).astype(jnp.int32)
    swap = [(0, 1), (1, 0)]

    def flip(x):
        return lax.ppermute(x, "tp", swap)

    normed = rms_rows(tokens.astype(f32), input_norm_gain).astype(bf16)

    def core(a, same):
        return 2 * a + ((a // plane) % 2 if same else 1 - (a // plane) % 2)

    both_axes = ("sp", "tp")
    other = lax.ppermute(
        normed, both_axes, [(core(a, True), core(a ^ plane, False)) for a in range(sp)]
    )
    same_xs, other_xs = [normed], [other]
    for r in range(1, plane):
        same_xs.append(
            lax.ppermute(normed, both_axes, [(core(a, True), core(a ^ r, True)) for a in range(sp)])
        )

    gate_rows = jnp.transpose(gate_weight.reshape(2, half, 4, lh), (0, 3, 2, 1)).reshape(
        2, lh, 4 * half // LANES, LANES
    )
    decay_rows = jnp.transpose(bf16_parts(decay_extra), (1, 2, 0, 3)).reshape(
        2, lh, 3 * tok // LANES, LANES
    )
    small = jnp.concatenate([gate_rows, decay_rows], axis=2)
    n_rows = 6 * half + small.shape[2]
    spread, send = vmem_call(
        pack_kernel,
        (
            jax.ShapeDtypeStruct((2, 2, lh, n_rows, LANES), bf16),
            jax.ShapeDtypeStruct((lh, n_rows, LANES), bf16),
        ),
        smem=1,
        n_in=8,
    )(meta, mq_weight, mk_weight, mv_weight, mo_weight, aq_weight, ak_weight, av_weight, small)
    got = flip(send)
    got = jnp.broadcast_to(got[None, None], (2, 1) + got.shape)
    spread = lax.dynamic_update_slice_in_dim(spread, got, 1 - t, 1)
    own_w = lax.all_to_all(spread.reshape(sp * n_rows, LANES), "sp", 0, 0, tiled=True)
    for r in range(1, plane):
        other_xs.append(
            lax.ppermute(
                other, both_axes, [(core(a, False), core(a ^ r, False)) for a in range(sp)]
            )
        )
    out_block = jnp.concatenate([out_m_weight, out_a_weight], axis=0)
    column = [out_block]
    for r in range(1, sp // plane):
        column.append(lax.ppermute(out_block, "sp", [(a, a ^ (r * plane)) for a in range(sp)]))
    partner_w = flip(own_w)
    params = jnp.concatenate(
        [m_gain, gate_bias.reshape(-1), sink_logit, jnp.zeros((LANES - 6 * lh,), f32)]
    ).reshape(-1, LANES)
    params = jnp.stack([params, flip(params)])
    gain = params[:, :lh]
    bias = params[:, lh, : 4 * lh]
    sink = params[:, lh, 4 * lh : 6 * lh]

    quarter = plane * tok
    cols = 6 * LANES
    sum_rows = M_DIM + 8 + WINDOW
    woven, gate_t, decay = vmem_call(
        weave_kernel,
        (
            jax.ShapeDtypeStruct((width, cols), bf16),
            jax.ShapeDtypeStruct((LANES, width), bf16),
            jax.ShapeDtypeStruct((2, plane, tok), f32),
        ),
        smem=1,
        n_in=2,
        keep=True,
        flops=quarter * width,
    )(meta, *near(*(x.reshape(sp, n_rows, LANES) for x in (own_w, partner_w))))
    proj, vrows, vcols, local, summary = vmem_call(
        project_kernel,
        (
            jax.ShapeDtypeStruct((quarter, cols), bf16),
            jax.ShapeDtypeStruct((6 * plane, tok), f32),
            jax.ShapeDtypeStruct((tok, LANES), f32),
            jax.ShapeDtypeStruct((2, plane, M_DIM, 2 * LANES), f32),
            jax.ShapeDtypeStruct((2, sum_rows, LANES), f32),
        ),
        scratch=[
            pltpu.VMEM((plane, tok, width), bf16),
            pltpu.VMEM((plane, 8, tok), f32),
            pltpu.SemaphoreType.DMA((plane,)),
        ],
        smem=2,
        n_any=2 * plane,
        n_tail=3,
        keep=True,
        flops=2 * quarter * width * cols,
    )(meta, bias, *same_xs, *other_xs, *near(woven, gate_t, decay))
    column = jnp.concatenate(column, axis=0)
    cut = column.shape[0] // 2
    upper, lower = column[:cut], column[cut:]

    def hop(x, r):
        return lax.ppermute(x, "sp", [(a, a ^ r) for a in range(sp)])

    upper_1, lower_2 = hop(upper, 1), hop(lower, 2)
    upper_2, lower_1 = hop(upper, 2), hop(lower, 1)
    upper_3, lower_3 = hop(upper_1, 2), hop(lower_2, 1)
    out_blocks = [upper, lower, upper_1, lower_1, upper_2, lower_2, upper_3, lower_3]
    partner_sum = flip(summary)
    sent = vmem_call(
        combine_kernel, jax.ShapeDtypeStruct((sum_rows, LANES), f32), smem=1, n_in=2
    )(meta, *near(summary, partner_sum))
    across = lax.ppermute(sent, "sp", [(a, (a + group) % sp) for a in range(sp)])
    blocks = quarter // WINDOW
    att, att_logs = vmem_call(
        attend_kernel,
        (
            jax.ShapeDtypeStruct((blocks, WINDOW, LANES), bf16),
            jax.ShapeDtypeStruct((blocks, 8, WINDOW), f32),
        ),
        scratch=[pltpu.VMEM((quarter + 2 * WINDOW, LANES), bf16)],
        smem=2,
        n_in=2,
        keep=True,
        flops=quarter * width * cols,
    )(meta, sink, *near(proj, partner_sum))
    spread, send = vmem_call(
        mixer_kernel,
        (
            jax.ShapeDtypeStruct((2, plane, tok + 16, LANES), bf16),
            jax.ShapeDtypeStruct((plane, tok + 16, LANES), bf16),
        ),
        scratch=[pltpu.VMEM((blocks, WINDOW, LANES), bf16), pltpu.VMEM((blocks, 8, WINDOW), f32)],
        smem=2,
        n_in=9,
        flops=quarter * width * cols,
    )(meta, sink, *near(proj, vrows, vcols, local, partner_sum, across), gain, *near(att, att_logs))
    got = flip(send)
    spread = lax.dynamic_update_slice_in_dim(spread, got[None], 1 - t, 0)
    groups = [list(range(g * group, (g + 1) * group)) for g in range(sp // group)]
    mine = lax.all_to_all(
        spread.reshape(group * (tok + 16), LANES),
        "sp",
        0,
        0,
        axis_index_groups=groups,
        tiled=True,
    )
    theirs = flip(mine)
    shape = (group, tok + 16, LANES)
    inner = 2 * group * LANES
    return vmem_call(
        output_kernel,
        (
            jax.ShapeDtypeStruct((tok, out_m_weight.shape[1]), bf16),
            jax.ShapeDtypeStruct((2 * lh, tok), f32),
        ),
        scratch=[
            pltpu.VMEM((2 * group, tok, LANES), bf16),
            pltpu.VMEM((inner, out_m_weight.shape[1]), bf16),
            pltpu.SemaphoreType.DMA((sp, 2)),
        ],
        smem=1,
        n_in=2,
        n_any=2 * plane,
        flops=2 * tok * inner * out_m_weight.shape[1],
    )(meta, *near(mine.reshape(shape), theirs.reshape(shape)), *out_blocks)


def solution(mesh):
    in_specs = (
        P("sp", None),
        P(),
        P("sp", "tp"),
        P("sp", "tp"),
        P("sp", "tp"),
        P("sp", "tp"),
        P("sp", None, "tp"),
        P(None, "tp"),
        P(None, "tp", "sp"),
        P("tp"),
        P("sp", "tp"),
        P("sp", "tp"),
        P("sp", "tp"),
        P("tp"),
        P("sp", "tp"),
        P("sp", "tp"),
    )
    out_specs = (P("sp", "tp"), P("tp", "sp"))

    def per_device(*args):
        plan = split_plan(mesh, args)
        if plan is None:
            return on_device(*args)
        return on_device_split(plan, *args)

    return jax.shard_map(
        per_device, mesh=mesh, in_specs=in_specs, out_specs=out_specs, check_vma=False
    )
```

```python
import jax
import jax.numpy as jnp
from jax import lax
import math

from jax.experimental import pallas as pl
from jax.experimental.pallas import tpu as pltpu
from jax.sharding import PartitionSpec as P

M_DIM = 128
W_DIM = 64
WINDOW = 128
M_BLOCK = 64


EPS = 1e-06
FLOOR_LOG = -1e30
HIGHEST = lax.Precision.HIGHEST


def with_halo(x, sides, width):
    for axis, dim in sides:
        peers, length = (lax.axis_size(axis), x.shape[dim])
        up = [(i, (i + 1) % peers) for i in range(peers - 1)]
        down = [(j, i) for i, j in up]
        last = lax.slice_in_dim(x, length - width, length, axis=dim)
        first = lax.slice_in_dim(x, 0, width, axis=dim)
        before = lax.ppermute(last, axis, up)
        after = lax.ppermute(first, axis, down)
        x = jnp.concatenate([before, x, after], axis=dim)
    return x


def rms_rows(inputs, gain_vec):
    return inputs * lax.rsqrt(jnp.mean(inputs * inputs, axis=-1, keepdims=True) + EPS) * gain_vec


def stored(result):
    return lax.optimization_barrier(result.astype(jnp.bfloat16))


def flip_tokens(array_in):
    return jnp.flip(array_in, axis=1)


def block_pass(queries, key_vecs, value_vecs, in_gate, log_forget, start_state):
    head_count, length, head_width = queries.shape
    block_count = length // M_BLOCK

    def blocks(array_in):
        return jnp.moveaxis(
            array_in.reshape((head_count, block_count, M_BLOCK) + array_in.shape[2:]), 1, 0
        )

    lower_mask = jnp.tril(jnp.ones((M_BLOCK, M_BLOCK), dtype=bool))

    def advance(state_in, block_in):
        cell_mat, norm_vec, stab_max = state_in
        q_blk, k_blk, v_blk, i_blk, f_blk = block_in
        cum_log = jnp.cumsum(f_blk, axis=-1)
        seg_total = cum_log[:, -1]
        log_end = seg_total[:, None] - cum_log + i_blk
        max_next = jnp.maximum(seg_total + stab_max, jnp.max(log_end, axis=-1))
        w_end = jnp.exp(log_end - max_next[:, None])
        fade_old = jnp.exp(seg_total + stab_max - max_next)
        cell_next = fade_old[:, None, None] * cell_mat + jnp.einsum(
            "hsv,hsk->hvk", w_end[:, :, None] * v_blk, k_blk, precision=HIGHEST
        )
        norm_next = fade_old[:, None] * norm_vec + jnp.einsum(
            "hs,hsk->hk", w_end, k_blk, precision=HIGHEST
        )
        log_w = jnp.where(
            lower_mask, cum_log[:, :, None] - cum_log[:, None, :] + i_blk[:, None, :], -jnp.inf
        )
        log_inter = cum_log + stab_max[:, None]
        row_max = jnp.maximum(log_inter, jnp.max(log_w, axis=-1))
        w_intra = jnp.exp(log_w - row_max[:, :, None])
        w_inter = jnp.exp(log_inter - row_max)
        scores = jnp.einsum("htk,hsk->hts", q_blk, k_blk, precision=HIGHEST) * w_intra
        numerator = jnp.einsum("hts,hsv->htv", scores, v_blk, precision=HIGHEST) + w_inter[
            ..., None
        ] * jnp.einsum("hvk,htk->htv", cell_mat, q_blk, precision=HIGHEST)
        denominator = jnp.sum(scores, axis=-1) + w_inter * jnp.einsum(
            "hk,htk->ht", norm_vec, q_blk, precision=HIGHEST
        )
        result_rows = numerator / jnp.maximum(jnp.abs(denominator), jnp.exp(-row_max))[..., None]
        return ((cell_next, norm_next, max_next), result_rows)

    final_state, outputs = lax.scan(
        advance,
        start_state,
        tuple(
            (blocks(array_in) for array_in in (queries, key_vecs, value_vecs, in_gate, log_forget))
        ),
    )
    return (jnp.moveaxis(outputs, 0, 1).reshape(head_count, length, head_width), final_state)


def summarize(key_vecs, value_vecs, in_gate, log_forget):
    cum_log = jnp.cumsum(log_forget, axis=-1)
    seg_total = cum_log[:, -1]
    log_end = seg_total[:, None] - cum_log + in_gate
    peak_log = jnp.max(log_end, axis=-1)
    weights_end = jnp.exp(log_end - peak_log[:, None])
    cell_mat = jnp.einsum(
        "hsv,hsk->hvk", weights_end[:, :, None] * value_vecs, key_vecs, precision=HIGHEST
    )
    norm_vec = jnp.einsum("hs,hsk->hk", weights_end, key_vecs, precision=HIGHEST)
    return (seg_total, cell_mat, norm_vec, peak_log)


def merge_side(state_in, cell_mats, norm_vecs, logs, usable):
    cell_mat, norm_vec, peak_log = state_in
    masked = jnp.where(usable, logs, FLOOR_LOG)
    new_peak = jnp.maximum(peak_log, jnp.max(masked, axis=0))
    scales = jnp.where(usable, jnp.exp(masked - new_peak[None]), 0.0)
    cell_mat = jnp.einsum("jh,jhvk->hvk", scales, cell_mats, precision=HIGHEST)
    norm_vec = jnp.einsum("jh,jhk->hk", scales, norm_vecs, precision=HIGHEST)
    return (cell_mat, norm_vec, new_peak)


def gather_states(forward_sum, backward_sum):
    decay_all = (
        lax.all_gather(forward_sum[0][None], "sp", axis=0, tiled=True),
        lax.all_gather(backward_sum[0][None], "sp", axis=0, tiled=True),
    )
    own_index = lax.axis_index("sp")
    acc_fwd = jnp.cumsum(decay_all[0], axis=0)
    acc_bwd = jnp.cumsum(decay_all[1], axis=0)
    before_own = lax.dynamic_index_in_dim(acc_fwd - decay_all[0], own_index, 0, keepdims=False)
    after_own = lax.dynamic_index_in_dim(acc_bwd, own_index, 0, keepdims=False)
    lead_bwd = acc_bwd - decay_all[1]
    empty_side = (
        jnp.zeros_like(forward_sum[1]),
        jnp.zeros_like(forward_sum[2]),
        jnp.full_like(forward_sum[3], FLOOR_LOG),
    )
    state_in = empty_side + empty_side
    pieces = (
        lax.all_gather(forward_sum[1][None], "sp", axis=0, tiled=True),
        lax.all_gather(forward_sum[2][None], "sp", axis=0, tiled=True),
        lax.all_gather(forward_sum[3][None], "sp", axis=0, tiled=True),
        lax.all_gather(backward_sum[1][None], "sp", axis=0, tiled=True),
        lax.all_gather(backward_sum[2][None], "sp", axis=0, tiled=True),
        lax.all_gather(backward_sum[3][None], "sp", axis=0, tiled=True),
    )
    piece_count = pieces[0].shape[0]
    device_ids = jnp.arange(piece_count, dtype=jnp.int32)
    log_fwd = before_own[None] - acc_fwd + pieces[2]
    log_bwd = lead_bwd - after_own[None] + pieces[5]
    left_side = merge_side(
        state_in[:3], pieces[0], pieces[1], log_fwd, (device_ids < own_index)[:, None]
    )
    right_side = merge_side(
        state_in[3:], pieces[3], pieces[4], log_bwd, (device_ids > own_index)[:, None]
    )
    states = left_side + right_side
    return (states[:3], states[3:])


def window_attend(a_query, kv_pairs, sink_logit, first_row, total_rows):
    tok_rows = a_query.shape[0]
    block_len = WINDOW
    block_count = tok_rows // block_len
    kv_width = kv_pairs.shape[1] // 2
    kv_heads = kv_width // W_DIM
    q_heads = a_query.shape[1] // W_DIM
    groups = q_heads // kv_heads
    filled_margin = with_halo(kv_pairs, (("sp", 0),), WINDOW)
    windows = jnp.concatenate(
        [
            filled_margin[place_idx * block_len : place_idx * block_len + tok_rows].reshape(
                block_count, block_len, 2 * kv_width
            )
            for place_idx in range(3)
        ],
        axis=1,
    )
    key_block = windows[:, :, :kv_width].reshape(block_count, 3 * block_len, kv_heads, W_DIM)
    content_tile = windows[:, :, kv_width:].reshape(block_count, 3 * block_len, kv_heads, W_DIM)
    query_block = a_query.reshape(block_count, block_len, kv_heads, groups, W_DIM)
    scores = jnp.einsum(
        "nqgrd,nkgd->ngrqk", query_block, key_block, preferred_element_type=jnp.float32
    ) * W_DIM ** (-0.5)
    query_off = jnp.arange(block_len, dtype=jnp.int32)
    key_off = jnp.arange(3 * block_len, dtype=jnp.int32) - block_len
    in_window = jnp.abs(query_off[:, None] - key_off[None, :]) <= WINDOW
    key_place = (
        first_row + jnp.arange(block_count, dtype=jnp.int32)[:, None] * block_len + key_off[None, :]
    )
    inside = (key_place >= 0) & (key_place < total_rows)
    usable = in_window[None] & inside[:, None, :]
    scores = jnp.where(usable[:, None, None], scores, -jnp.inf)
    sink_col = sink_logit.reshape(kv_heads, groups)[None, :, :, None]
    peak_log = jnp.maximum(sink_col, jnp.max(scores, axis=-1))
    weights_exp = jnp.exp(scores - peak_log[..., None])
    weight_total_sum = jnp.exp(sink_col - peak_log) + jnp.sum(weights_exp, axis=-1)
    weighted = jnp.einsum(
        "ngrqk,nkgd->nqgrd",
        weights_exp.astype(jnp.bfloat16),
        content_tile,
        preferred_element_type=jnp.float32,
    )
    scale_back = jnp.transpose(weight_total_sum, (0, 3, 1, 2))[..., None]
    mixed_rows = (weighted / scale_back).astype(jnp.bfloat16).reshape(tok_rows, q_heads * W_DIM)
    log_total = jnp.transpose(peak_log + jnp.log(weight_total_sum), (1, 2, 0, 3)).reshape(
        q_heads, tok_rows
    )
    return (mixed_rows, log_total)


def on_device(
    tokens,
    input_norm_gain,
    mq_weight,
    mk_weight,
    mv_weight,
    mo_weight,
    gate_weight,
    gate_bias,
    decay_extra,
    m_gain,
    aq_weight,
    ak_weight,
    av_weight,
    sink_logit,
    out_m_weight,
    out_a_weight,
):
    tok_rows = tokens.shape[0]
    normed = rms_rows(tokens.astype(jnp.float32), input_norm_gain).astype(jnp.bfloat16)
    local_heads = gate_weight.shape[2]
    gate_cols = 4 * local_heads
    pieces = (
        lax.all_gather(mq_weight, "sp", axis=0, tiled=True),
        lax.all_gather(mk_weight, "sp", axis=0, tiled=True),
        lax.all_gather(mv_weight, "sp", axis=0, tiled=True),
        lax.all_gather(mo_weight, "sp", axis=0, tiled=True),
        lax.all_gather(gate_weight, "sp", axis=0, tiled=True),
        lax.all_gather(aq_weight, "sp", axis=0, tiled=True),
        lax.all_gather(ak_weight, "sp", axis=0, tiled=True),
        lax.all_gather(av_weight, "sp", axis=0, tiled=True),
    )
    piece_rows = pieces[0].shape[0]
    flat_gate = pieces[4].reshape(piece_rows, gate_cols)
    segments = (
        pieces[0],
        pieces[1],
        pieces[2],
        pieces[3],
        flat_gate,
        pieces[5],
        pieces[6],
        pieces[7],
    )
    projected = tuple(
        (jnp.dot(normed, segment, preferred_element_type=jnp.float32) for segment in segments)
    )
    m_query = stored(projected[0])
    m_key = stored(projected[1])
    m_value = stored(projected[2])
    m_out = stored(projected[3])
    gates = projected[4].reshape(tok_rows, 4, local_heads) + gate_bias[None]

    def heads_first(matrix):
        return jnp.transpose(
            matrix.astype(jnp.float32).reshape(tok_rows, local_heads, M_DIM), (1, 0, 2)
        )

    queries = heads_first(m_query)
    key_vecs = heads_first(m_key) * M_DIM ** (-0.5)
    value_vecs = heads_first(m_value)
    in_fwd = gates[:, 0, :].T
    forget_fwd = jax.nn.log_sigmoid(gates[:, 1, :].T) + decay_extra[0]
    in_bwd = flip_tokens(gates[:, 2, :].T)
    forget_bwd = flip_tokens(jax.nn.log_sigmoid(gates[:, 3, :].T) + decay_extra[1])
    queries_bwd = flip_tokens(queries)
    keys_bwd = flip_tokens(key_vecs)
    values_bwd = flip_tokens(value_vecs)
    forward_sum = summarize(key_vecs, value_vecs, in_fwd, forget_fwd)
    backward_sum = summarize(keys_bwd, values_bwd, in_bwd, forget_bwd)
    state_fwd, state_bwd = gather_states(forward_sum, backward_sum)
    hidden_fwd, _ = block_pass(queries, key_vecs, value_vecs, in_fwd, forget_fwd, state_fwd)
    hidden_bwd, _ = block_pass(queries_bwd, keys_bwd, values_bwd, in_bwd, forget_bwd, state_bwd)
    cell_out = hidden_fwd + flip_tokens(hidden_bwd)
    gate_open = jax.nn.sigmoid(m_out.astype(jnp.float32)).reshape(tok_rows, local_heads, M_DIM)
    cell_rows = jnp.transpose(cell_out, (1, 0, 2)) * gate_open
    mixed_m = (
        rms_rows(cell_rows, m_gain.reshape(local_heads, M_DIM))
        .astype(jnp.bfloat16)
        .reshape(tok_rows, local_heads * M_DIM)
    )
    a_query = stored(projected[5])
    kv_pairs = jnp.concatenate([stored(projected[6]), stored(projected[7])], axis=1)
    first_row = lax.axis_index("sp") * tok_rows
    total_rows = tok_rows * lax.axis_size("sp")
    mixed_a, log_total = window_attend(a_query, kv_pairs, sink_logit, first_row, total_rows)
    full_m, full_a = (
        lax.all_gather(mixed_m, "tp", axis=1, tiled=True),
        lax.all_gather(mixed_a, "tp", axis=1, tiled=True),
    )
    pieces = (
        lax.all_gather(out_m_weight, "sp", axis=0, tiled=True),
        lax.all_gather(out_a_weight, "sp", axis=0, tiled=True),
    )
    running = jnp.dot(full_m, pieces[0], preferred_element_type=jnp.float32)
    mixed = running + jnp.dot(full_a, pieces[1], preferred_element_type=jnp.float32)
    return (mixed.astype(jnp.bfloat16), log_total)


CHUNK = 256
LANES = 128
EMPTY = -1e30


def split_plan(mesh, args):
    sp, tp = mesh.shape["sp"], mesh.shape["tp"]
    tok_rows, width = args[0].shape
    rows = args[2].shape[0]
    local_heads = args[6].shape[2]
    group = local_heads * tp
    if tp != 2 or sp != 2 * group or group != 8:
        return None
    plane = group // 2
    ok = (
        args[2].shape[1] == local_heads * M_DIM
        and args[10].shape[1] == local_heads * LANES
        and args[11].shape[1] == local_heads * W_DIM
        and args[12].shape[1] == local_heads * W_DIM
        and 2 * W_DIM == LANES
        and M_DIM == LANES
        and WINDOW == LANES
        and tok_rows == CHUNK
        and rows == LANES
        and args[14].shape[0] * sp == group * M_DIM
        and args[15].shape[0] * sp == group * LANES
    )
    if not ok:
        return None
    return dict(
        sp=sp, tp=tp, tok=tok_rows, width=width, rows=rows, lh=local_heads, group=group, plane=plane
    )


def mm(a, b, ca=1, cb=0, precision=None):
    return lax.dot_general(
        a, b, (((ca,), (cb,)), ((), ())), precision=precision, preferred_element_type=jnp.float32
    )


def vmem_call(kernel, outs, scratch=(), smem=0, n_in=0, flops=0, n_any=0, n_tail=0, keep=False):
    return pl.pallas_call(
        kernel,
        out_shape=jax.tree.map(lambda x: pltpu.VMEM(x.shape, x.dtype), outs) if keep else outs,
        in_specs=[pl.BlockSpec(memory_space=pltpu.SMEM)] * smem
        + [pl.BlockSpec(memory_space=pltpu.VMEM)] * n_in
        + [pl.BlockSpec(memory_space=pl.ANY)] * n_any
        + [pl.BlockSpec(memory_space=pltpu.VMEM)] * n_tail,
        out_specs=jax.tree.map(lambda _: pl.BlockSpec(memory_space=pltpu.VMEM), outs),
        scratch_shapes=scratch,
        cost_estimate=pl.CostEstimate(flops=flops, bytes_accessed=0, transcendentals=0),
        compiler_params=pltpu.CompilerParams(vmem_limit_bytes=24 * 1024 * 1024),
    )


def near(*arrays):
    return [pltpu.with_memory_space_constraint(x, pltpu.VMEM) for x in arrays]


def pack_kernel(meta, *refs):
    sources, small, keep, send = refs[:7], refs[7], refs[8], refs[9]
    held, sems = refs[10:17], refs[17]
    t = meta[0]
    fetches = [
        pltpu.make_async_copy(a, b, sems.at[i]) for i, (a, b) in enumerate(zip(sources, held))
    ]
    for fetch in fetches:
        fetch.start()
    for fetch in fetches:
        fetch.wait()
    mq, mk, mv, mo, aq, ak, av = held
    copies, heads = keep.shape[0], keep.shape[2]
    rows = mq.shape[0] // 2
    at = pl.multiple_of(t * rows, rows)
    away = pl.multiple_of((1 - t) * rows, rows)
    for h in range(heads):
        lanes = slice(h * LANES, (h + 1) * LANES)
        narrow = slice(h * W_DIM, (h + 1) * W_DIM)
        for start, mine in ((at, True), (away, False)):
            parts = [ref[pl.ds(start, rows), lanes] for ref in (mq, mk, mv, mo, aq)]
            parts.append(
                jnp.concatenate([ref[pl.ds(start, rows), narrow] for ref in (ak, av)], axis=1)
            )
            parts.append(small[t if mine else 1 - t, h])
            row = 0
            for part in parts:
                span = slice(row, row + part.shape[0])
                row += part.shape[0]
                if mine:
                    for i in range(copies):
                        keep[i, t, h, span, :] = part
                else:
                    send[h, span, :] = part


def running_max(x, backward):
    n = x.shape[1]
    lane = lax.broadcasted_iota(jnp.int32, x.shape, 1)
    step = 1
    while step < n:
        if backward:
            moved = jnp.where(lane < n - step, pltpu.roll(x, n - step, 1), EMPTY)
        else:
            moved = jnp.where(lane >= step, pltpu.roll(x, step, 1), EMPTY)
        x = jnp.maximum(x, moved)
        step *= 2
    return x


def with_ones(value):
    lane = lax.broadcasted_iota(jnp.int32, value.shape, 1)
    ones = jnp.where(lane == 0, 1.0, 0.0).astype(value.dtype)
    return jnp.concatenate([value, ones], axis=1)


def merge(earlier, later, later_total):
    peak = jnp.maximum(later_total + earlier[1], later[1])
    old = jnp.exp(later_total + earlier[1] - peak)
    new = jnp.exp(later[1] - peak)
    return old * earlier[0] + new * later[0], peak


def weave_kernel(meta, own, partner, weight, gate_t, decay):
    t, hi = meta[0], meta[4]
    sources = own.shape[0]
    rows = weight.shape[0] // sources // 2
    cols = weight.shape[1] // LANES
    plane = decay.shape[1]
    for i in range(sources):
        first = pl.multiple_of((2 * i + t) * rows, rows)
        second = pl.multiple_of((2 * i + 1 - t) * rows, rows)
        for c in range(cols):
            lanes = slice(c * LANES, (c + 1) * LANES)
            span = slice(c * rows, (c + 1) * rows)
            weight[pl.ds(first, rows), lanes] = own[i, span, :]
            weight[pl.ds(second, rows), lanes] = partner[i, span, :]

    def small(ref, i):
        return ref[i, cols * rows :, :].astype(jnp.float32)

    gate_t[...] = jnp.zeros(gate_t.shape, jnp.bfloat16)
    for i in range(sources):
        pair = [
            jnp.concatenate(
                [x[0:1, :rows], x[0:1, rows:], x[1:2, :rows], x[1:2, rows:]], axis=0
            )
            for x in (small(own, i), small(partner, i))
        ]
        piece = jnp.where(
            t == 0,
            jnp.concatenate(pair, axis=1),
            jnp.concatenate(pair[::-1], axis=1),
        )
        piece = jnp.concatenate([piece, jnp.zeros((12, LANES), jnp.float32)], axis=0)
        gate_t[:16, i * LANES : (i + 1) * LANES] = piece.astype(jnp.bfloat16)
    for b in range(plane):
        for ref, at in ((own, t), (partner, 1 - t)):
            x = small(ref, (2 * hi + t) * plane + b)
            x = x[2:4] + x[4:6] + x[6:8]
            decay[at, b : b + 1, :] = jnp.concatenate([x[:1], x[1:]], axis=1)


def project_kernel(meta, bias, *refs):
    plane = (len(refs) - 11) // 2
    same, other = refs[:plane], refs[plane : 2 * plane]
    weight, gate_t, decay = refs[2 * plane : 2 * plane + 3]
    proj, vrows, vcols, local, summary, xs, gates, sems = refs[2 * plane + 3 :]
    t, k, sel, jl, near = meta[0], meta[1], meta[2], meta[3], meta[5]

    @pl.when(t == near)
    def _():
        for r in range(plane):
            pltpu.make_async_copy(same[r], xs.at[r], sems.at[r]).start()

    @pl.when(t != near)
    def _():
        for r in range(plane):
            pltpu.make_async_copy(other[r], xs.at[r], sems.at[r]).start()

    tok = xs.shape[1]
    for r in range(plane):
        pltpu.make_async_copy(same[r], xs.at[r], sems.at[r]).wait()
        at = pl.ds(pl.multiple_of((k ^ r) * tok, tok), tok)
        proj[at, :] = mm(xs[r], weight[...]).astype(jnp.bfloat16)
        gates[k ^ r] = jnp.transpose(mm(xs[r], gate_t[...], 1, 1))[:8]
    heads = bias.shape[1] // 4
    b = [bias[sel, g * heads + jl] for g in range(4)]
    g = [
        jnp.concatenate([gates[c, i : i + 1] for c in range(plane)], axis=0) + b[i]
        for i in range(4)
    ]

    def forget(i, direction):
        x = g[i]
        return jnp.minimum(x, 0.0) - jnp.log1p(jnp.exp(-jnp.abs(x))) + decay[direction]

    lf_f, lf_b = forget(1, 0), forget(3, 1)
    r = lax.broadcasted_iota(jnp.int32, (tok, tok), 0)
    c = lax.broadcasted_iota(jnp.int32, (tok, tok), 1)
    lower = jnp.where(r >= c, 1.0, 0.0).astype(jnp.float32)
    cum = mm(jnp.concatenate([lf_f, lf_b], axis=0), lower, 1, 1, HIGHEST)
    lead_f, lead_b = cum[:plane], lf_b - cum[plane:]
    src_f, src_b = g[0] - lead_f, g[2] - lead_b
    top_f, top_b = running_max(src_f, False), running_max(src_b, True)
    total_f, total_b = lead_f[:, tok - 1 :], cum[plane:, tok - 1 :]
    best_f, best_b = top_f[:, tok - 1 :], top_b[:, :1]
    end_f, end_b = jnp.exp(src_f - best_f), jnp.exp(src_b - best_b)
    peak_f, peak_b = best_f + total_f, best_b

    def wide(x):
        return jnp.broadcast_to(x, (plane, tok))

    vrows[...] = jnp.concatenate(
        [src_f, src_b, wide(total_f), wide(total_b), wide(peak_f), wide(peak_b)], axis=0
    )
    stack = [top_f, top_b, lead_f, lead_b, end_f, end_b]
    stack.append(jnp.zeros((LANES - 6 * plane, tok), jnp.float32))
    cols_all = jnp.transpose(jnp.concatenate(stack, axis=0))
    vcols[...] = cols_all
    for ch in range(plane):
        span = slice(ch * tok, (ch + 1) * tok)
        key = proj[span, LANES : 2 * LANES].astype(jnp.float32)
        value = with_ones(proj[span, 2 * LANES : 3 * LANES])
        for i in range(2):
            at = (4 + i) * plane + ch
            weighted = (key * cols_all[:, at : at + 1]).astype(jnp.bfloat16)
            local[i, ch] = mm(weighted, value, 0, 0)
    for i in range(2):
        state = (jnp.zeros((M_DIM, 2 * LANES), jnp.float32), jnp.full((1, 1), EMPTY, jnp.float32))
        total = jnp.zeros((1, 1), jnp.float32)
        for ch in range(plane) if i == 0 else range(plane - 1, -1, -1):
            chunk_total, chunk_peak = chunk_scalars(vrows, i, ch, plane)
            state = merge(state, (local[i, ch], chunk_peak), chunk_total)
            total = total + chunk_total
        summary[i, :M_DIM, :] = state[0][:, :LANES]
        summary[i, M_DIM : M_DIM + 8, :] = jnp.concatenate(
            [
                jnp.transpose(state[0][:, LANES:])[:1],
                jnp.broadcast_to(state[1], (1, LANES)),
                jnp.broadcast_to(total, (1, LANES)),
                jnp.zeros((5, LANES), jnp.float32),
            ],
            axis=0,
        )
    last = proj.shape[0]
    summary[0, M_DIM + 8 :, :] = proj[:WINDOW, 5 * LANES :].astype(jnp.float32)
    summary[1, M_DIM + 8 :, :] = proj[last - WINDOW :, 5 * LANES :].astype(jnp.float32)


def chunk_scalars(vrows, i, ch, plane):
    total, peak = (2 + i) * plane + ch, (4 + i) * plane + ch
    return vrows[total : total + 1, :1], vrows[peak : peak + 1, :1]


def packed_state(ref, i):
    rows = ref[i, : M_DIM + 8, :]
    return (rows, rows[M_DIM + 1 : M_DIM + 2, :1]), rows[M_DIM + 2 : M_DIM + 3, :1]


def open_state(packed):
    rows, peak = packed
    first = lax.broadcasted_iota(jnp.int32, (LANES, LANES), 0) == 0
    norm = jnp.transpose(jnp.where(first, rows[M_DIM : M_DIM + 1], 0.0))
    return jnp.concatenate([rows[:M_DIM], norm], axis=1), peak


def combine_kernel(meta, own, partner, out):
    t, hi = meta[0], meta[4]
    forward = hi == 0
    i = jnp.where(forward, 0, 1)
    (mine, mine_peak), mine_total = packed_state(own, i)
    (other, other_peak), other_total = packed_state(partner, i)
    mine_later = (t == 1) == forward

    def pick(x, y):
        return jnp.where(mine_later, x, y)

    rows, peak = merge(
        (pick(other, mine), pick(other_peak, mine_peak)),
        (pick(mine, other), pick(mine_peak, other_peak)),
        pick(mine_total, other_total),
    )
    out[: M_DIM + 8, :] = rows
    out[M_DIM + 1 : M_DIM + 2, :] = jnp.broadcast_to(peak, (1, LANES))
    out[M_DIM + 8 :, :] = partner[jnp.where(forward, 1, 0), M_DIM + 8 :, :]


def attend(q, kv, sinks, drop_first, drop_last):
    n = q.shape[0]
    q = q * jnp.bfloat16(W_DIM ** (-0.5))
    q = jnp.concatenate([q[:, :W_DIM], q[:, W_DIM:]], axis=0)
    r = lax.broadcasted_iota(jnp.int32, (2 * n, n), 0)
    c = lax.broadcasted_iota(jnp.int32, (2 * n, n), 1)
    row = jnp.where(r >= n, r - n, r)
    sink = jnp.where(
        lax.broadcasted_iota(jnp.int32, (2 * n, 1), 0) < n, sinks[0], sinks[1]
    )
    s = [mm(q, kv[i * n : (i + 1) * n, :W_DIM], 1, 1) for i in range(3)]
    before, after = c >= row, c <= row
    if drop_first is not None:
        before = before & jnp.logical_not(drop_first)
        after = after & jnp.logical_not(drop_last)
    s[0] = jnp.where(before, s[0], EMPTY)
    s[2] = jnp.where(after, s[2], EMPTY)
    peak = jnp.max(jnp.maximum(jnp.maximum(s[0], s[1]), s[2]), axis=1, keepdims=True)
    peak = jnp.maximum(peak, sink)
    e = [jnp.exp(x - peak) for x in s]
    total = jnp.exp(sink - peak) + jnp.sum(e[0] + e[1] + e[2], axis=1, keepdims=True)
    weights = jnp.concatenate([x.astype(jnp.bfloat16) for x in e], axis=1)
    mixed = mm(weights, kv[:, W_DIM:]) / total
    mixed = jnp.concatenate([mixed[:n], mixed[n:]], axis=1).astype(jnp.bfloat16)
    log_col = peak + jnp.log(total)
    diag = (c == row)
    logs = [
        jnp.sum(jnp.where(diag[:n], log_col[h * n : (h + 1) * n], 0.0), axis=0, keepdims=True)
        for h in range(2)
    ]
    return mixed, jnp.concatenate(logs + [jnp.zeros((6, n), jnp.float32)], axis=0)


def attend_kernel(meta, sink, proj, partner, mixed, logs, kv):
    t, sel, jl = meta[0], meta[2], meta[3]
    length = proj.shape[0]
    edge = partner[jnp.where(t == 0, 0, 1), M_DIM + 8 :, :].astype(jnp.bfloat16)
    kv[:WINDOW, :] = edge
    kv[WINDOW : WINDOW + length, :] = proj[:, 5 * LANES :]
    kv[WINDOW + length :, :] = edge
    sinks = (sink[sel, 2 * jl], sink[sel, 2 * jl + 1])
    for i in range(length // WINDOW - 1):
        b = i + 1 - t
        at = pl.multiple_of(b * WINDOW, WINDOW)
        q = proj[pl.ds(at, WINDOW), 4 * LANES : 5 * LANES]
        mixed[b], logs[b] = attend(q, kv[pl.ds(at, 3 * WINDOW), :], sinks, None, None)


def mixer_kernel(
    meta, sink, proj, vrows, vcols, local, partner, across, gain, att, att_logs, keep, send, am, al
):
    t, sel, jl, hi = meta[0], meta[2], meta[3], meta[4]
    tok = vrows.shape[1]
    chunks = vrows.shape[0] // 6

    def store(is_cell, c, span, value):
        @pl.when((t == 0) == is_cell)
        def _():
            keep[t, c, span, :] = value

        @pl.when((t == 0) != is_cell)
        def _():
            send[c, span, :] = value

    length = proj.shape[0]
    blocks = length // WINDOW
    am[...] = att[...]
    al[...] = att_logs[...]
    outer = across[M_DIM + 8 :, :].astype(jnp.bfloat16)
    inside = proj[pl.ds(pl.multiple_of(t * (length - 2 * WINDOW), WINDOW), 2 * WINDOW), 5 * LANES :]
    kv = jnp.where(
        t == 0,
        jnp.concatenate([outer, inside], axis=0),
        jnp.concatenate([inside, outer], axis=0),
    )
    sinks = (sink[sel, 2 * jl], sink[sel, 2 * jl + 1])
    at = pl.multiple_of(t * (length - WINDOW), WINDOW)
    q = proj[pl.ds(at, WINDOW), 4 * LANES : 5 * LANES]
    edge = t * (blocks - 1)
    am[edge], al[edge] = attend(q, kv, sinks, (t == 0) & (hi == 0), (t == 1) & (hi == 1))

    far = across[: M_DIM + 8, :]
    far_peak = across[M_DIM + 1 : M_DIM + 2, :1]

    def incoming(i, use_far, use_near):
        (near, near_peak), near_total = packed_state(partner, i)
        return open_state(
            merge(
                (far, jnp.where(use_far, far_peak, EMPTY)),
                (near, jnp.where(use_near, near_peak, EMPTY)),
                jnp.where(use_near, near_total, 0.0),
            )
        )

    fwd = incoming(0, hi == 1, t == 1)
    bwd = incoming(1, hi == 0, t == 0)
    entering = [[None, None] for _ in range(chunks)]
    for c in range(chunks):
        entering[c][0] = fwd
        total, peak = chunk_scalars(vrows, 0, c, chunks)
        if c + 1 < chunks:
            fwd = merge(fwd, (local[0, c], peak), total)
    for c in range(chunks - 1, -1, -1):
        total, peak = chunk_scalars(vrows, 1, c, chunks)
        entering[c][1] = (bwd[0], bwd[1] + total)
        if c:
            bwd = merge(bwd, (local[1, c], peak), total)
    r = lax.broadcasted_iota(jnp.int32, (tok, tok), 0)
    col = lax.broadcasted_iota(jnp.int32, (tok, tok), 1)
    gain_row = gain[sel, pl.ds(jl, 1), :]
    floor_lift = 0.5 * math.log(M_DIM)
    for c in range(chunks):
        span = slice(c * tok, (c + 1) * tok)
        q = proj[span, :LANES]
        value = with_ones(proj[span, 2 * LANES : 3 * LANES])
        scores = mm(q, proj[span, LANES : 2 * LANES], 1, 1)
        cell_out = None
        for i, mask in enumerate((r >= col, r <= col)):
            cell, reach = entering[c][i]
            at = i * chunks + c
            src = vrows[at : at + 1, :]
            top = jnp.maximum(vcols[:, at : at + 1], reach)
            lead = vcols[:, at + 2 * chunks : at + 2 * chunks + 1]
            w = jnp.where(mask, jnp.exp(src - top), 0.0)
            both = mm((scores * w).astype(jnp.bfloat16), value) + jnp.exp(reach - top) * mm(
                q, cell.astype(jnp.bfloat16)
            )
            denom = jnp.abs(both[:, LANES : LANES + 1])
            inv = 1.0 / jnp.maximum(denom, jnp.exp(floor_lift - (lead + top)))
            part = both[:, :LANES] * inv
            cell_out = part if cell_out is None else cell_out + part
        gate = proj[span, 3 * LANES : 4 * LANES].astype(jnp.float32)
        u = cell_out / (1.0 + jnp.exp(-gate))
        u = u * lax.rsqrt(jnp.mean(u * u, axis=1, keepdims=True) + EPS) * gain_row
        tail = jnp.zeros((16, LANES), jnp.bfloat16)
        store(True, c, slice(0, tok + 16), jnp.concatenate([u.astype(jnp.bfloat16), tail], axis=0))

    per = tok // WINDOW
    for c in range(chunks):
        x = jnp.concatenate(
            [al[c * per + p][h : h + 1] for h in range(2) for p in range(per)], axis=0
        )
        high = x.astype(jnp.bfloat16).astype(jnp.float32)
        mid = (x - high).astype(jnp.bfloat16).astype(jnp.float32)
        low = x - high - mid
        pad = jnp.zeros((16 - 3 * 2 * per, LANES), jnp.float32)
        tail = jnp.concatenate([high, mid, low, pad], axis=0).astype(jnp.bfloat16)
        rows = [am[c * per + p] for p in range(per)] + [tail]
        store(False, c, slice(0, tok + 16), jnp.concatenate(rows, axis=0))


def output_kernel(meta, own, partner, *refs):
    mixed, log_total, left, weight = refs[-4:]
    blocks = refs[:-4]
    t, p, z = meta[0], meta[1], meta[6]
    plane = len(blocks) // 2
    heads, tok = own.shape[0], mixed.shape[0]
    total = weight.shape[0] // 2
    rows = 2 * total // (2 * heads)
    half = rows // 2
    for r in range(plane):
        for zr in range(2 * heads // plane):
            source = (z ^ zr) * plane + (p ^ r)
            for i in range(2):
                to = pl.multiple_of(i * total + source * half, half)
                at = zr // 2 * rows + i * half
                weight[pl.ds(to, half), :] = blocks[2 * r + zr % 2][at : at + half, :]
    for j in range(heads):
        left[t * heads + j] = own[j, :tok, :]
        left[(1 - t) * heads + j] = partner[j, :tok, :]
    lhs = jnp.concatenate([left[i] for i in range(2 * heads)], axis=1)
    mixed[...] = mm(lhs, weight[...]).astype(jnp.bfloat16)
    per = tok // LANES
    n = 2 * per
    for i in range(heads // 2):
        j = t * (heads // 2) + i
        rows = jnp.where(t == 1, own[j, tok:, :], partner[j, tok:, :]).astype(jnp.float32)
        x = rows[:n] + rows[n : 2 * n] + rows[2 * n : 3 * n]
        for h in range(2):
            log_total[2 * i + h : 2 * i + h + 1, :] = jnp.concatenate(
                [x[h * per + p : h * per + p + 1] for p in range(per)], axis=1
            )


def bf16_parts(x):
    high = lax.reduce_precision(x, 8, 7)
    mid = lax.reduce_precision(x - high, 8, 7)
    return jnp.stack([high, mid, x - high - mid]).astype(jnp.bfloat16)


def on_device_split(
    plan,
    tokens,
    input_norm_gain,
    mq_weight,
    mk_weight,
    mv_weight,
    mo_weight,
    gate_weight,
    gate_bias,
    decay_extra,
    m_gain,
    aq_weight,
    ak_weight,
    av_weight,
    sink_logit,
    out_m_weight,
    out_a_weight,
):
    sp, group, plane, lh, tok = (plan[n] for n in ("sp", "group", "plane", "lh", "tok"))
    width, rows = plan["width"], plan["rows"]
    half = rows // 2
    f32, bf16 = jnp.float32, jnp.bfloat16
    s = lax.axis_index("sp").astype(jnp.int32)
    t = lax.axis_index("tp").astype(jnp.int32)
    hi, j = s // group, s % group
    near_plane = (s // plane) % 2
    meta = jnp.stack(
        [t, s % plane, jnp.where(j // lh == t, 0, 1), j % lh, hi, near_plane, s // plane]
    ).astype(jnp.int32)
    swap = [(0, 1), (1, 0)]

    def flip(x):
        return lax.ppermute(x, "tp", swap)

    normed = rms_rows(tokens.astype(f32), input_norm_gain).astype(bf16)

    def core(a, same):
        return 2 * a + ((a // plane) % 2 if same else 1 - (a // plane) % 2)

    both_axes = ("sp", "tp")
    other = lax.ppermute(
        normed, both_axes, [(core(a, True), core(a ^ plane, False)) for a in range(sp)]
    )
    same_xs, other_xs = [normed], [other]
    for r in range(1, plane):
        same_xs.append(
            lax.ppermute(normed, both_axes, [(core(a, True), core(a ^ r, True)) for a in range(sp)])
        )

    gate_rows = jnp.transpose(gate_weight.reshape(2, half, 4, lh), (0, 3, 2, 1)).reshape(
        2, lh, 4 * half // LANES, LANES
    )
    decay_rows = jnp.transpose(bf16_parts(decay_extra), (1, 2, 0, 3)).reshape(
        2, lh, 3 * tok // LANES, LANES
    )
    small = jnp.concatenate([gate_rows, decay_rows], axis=2)
    n_rows = 6 * half + small.shape[2]
    projections = (mq_weight, mk_weight, mv_weight, mo_weight, aq_weight, ak_weight, av_weight)
    spread, send = vmem_call(
        pack_kernel,
        (
            jax.ShapeDtypeStruct((2, 2, lh, n_rows, LANES), bf16),
            jax.ShapeDtypeStruct((lh, n_rows, LANES), bf16),
        ),
        scratch=[pltpu.VMEM(w.shape, bf16) for w in projections]
        + [pltpu.SemaphoreType.DMA((len(projections),))],
        smem=1,
        n_any=7,
        n_tail=1,
    )(meta, *projections, small)
    got = flip(send)
    got = jnp.broadcast_to(got[None, None], (2, 1) + got.shape)
    spread = lax.dynamic_update_slice_in_dim(spread, got, 1 - t, 1)
    own_w = lax.all_to_all(spread.reshape(sp * n_rows, LANES), "sp", 0, 0, tiled=True)
    for r in range(1, plane):
        other_xs.append(
            lax.ppermute(
                other, both_axes, [(core(a, False), core(a ^ r, False)) for a in range(sp)]
            )
        )
    out_block = jnp.concatenate([out_m_weight, out_a_weight], axis=0)
    out_next = lax.ppermute(out_block, "sp", [(a, (a + group) % sp) for a in range(sp)])
    upper = jnp.concatenate([out_block, out_next], axis=0)
    lower = lax.ppermute(upper, "sp", [(a, a ^ plane) for a in range(sp)])
    partner_w = flip(own_w)
    params = jnp.concatenate(
        [m_gain, gate_bias.reshape(-1), sink_logit, jnp.zeros((LANES - 6 * lh,), f32)]
    ).reshape(-1, LANES)
    params = jnp.stack([params, flip(params)])
    gain = params[:, :lh]
    bias = params[:, lh, : 4 * lh]
    sink = params[:, lh, 4 * lh : 6 * lh]

    quarter = plane * tok
    cols = 6 * LANES
    sum_rows = M_DIM + 8 + WINDOW
    woven, gate_t, decay = vmem_call(
        weave_kernel,
        (
            jax.ShapeDtypeStruct((width, cols), bf16),
            jax.ShapeDtypeStruct((LANES, width), bf16),
            jax.ShapeDtypeStruct((2, plane, tok), f32),
        ),
        smem=1,
        n_in=2,
        keep=True,
        flops=quarter * width,
    )(meta, *near(*(x.reshape(sp, n_rows, LANES) for x in (own_w, partner_w))))
    proj, vrows, vcols, local, summary = vmem_call(
        project_kernel,
        (
            jax.ShapeDtypeStruct((quarter, cols), bf16),
            jax.ShapeDtypeStruct((6 * plane, tok), f32),
            jax.ShapeDtypeStruct((tok, LANES), f32),
            jax.ShapeDtypeStruct((2, plane, M_DIM, 2 * LANES), f32),
            jax.ShapeDtypeStruct((2, sum_rows, LANES), f32),
        ),
        scratch=[
            pltpu.VMEM((plane, tok, width), bf16),
            pltpu.VMEM((plane, 8, tok), f32),
            pltpu.SemaphoreType.DMA((plane,)),
        ],
        smem=2,
        n_any=2 * plane,
        n_tail=3,
        keep=True,
        flops=2 * quarter * width * cols,
    )(meta, bias, *same_xs, *other_xs, *near(woven, gate_t, decay))

    def hop(x, r):
        return lax.ppermute(x, "sp", [(a, a ^ r) for a in range(sp)])

    upper_1, lower_2 = hop(upper, 1), hop(lower, 2)
    upper_2, lower_1 = hop(upper, 2), hop(lower, 1)
    upper_3, lower_3 = hop(upper_1, 2), hop(lower_2, 1)
    out_blocks = [upper, lower, upper_1, lower_1, upper_2, lower_2, upper_3, lower_3]
    partner_sum = flip(summary)
    sent = vmem_call(
        combine_kernel, jax.ShapeDtypeStruct((sum_rows, LANES), f32), smem=1, n_in=2
    )(meta, *near(summary, partner_sum))
    across = lax.ppermute(sent, "sp", [(a, (a + group) % sp) for a in range(sp)])
    blocks = quarter // WINDOW
    att, att_logs = vmem_call(
        attend_kernel,
        (
            jax.ShapeDtypeStruct((blocks, WINDOW, LANES), bf16),
            jax.ShapeDtypeStruct((blocks, 8, WINDOW), f32),
        ),
        scratch=[pltpu.VMEM((quarter + 2 * WINDOW, LANES), bf16)],
        smem=2,
        n_in=2,
        keep=True,
        flops=quarter * width * cols,
    )(meta, sink, *near(proj, partner_sum))
    spread, send = vmem_call(
        mixer_kernel,
        (
            jax.ShapeDtypeStruct((2, plane, tok + 16, LANES), bf16),
            jax.ShapeDtypeStruct((plane, tok + 16, LANES), bf16),
        ),
        scratch=[pltpu.VMEM((blocks, WINDOW, LANES), bf16), pltpu.VMEM((blocks, 8, WINDOW), f32)],
        smem=2,
        n_in=9,
        flops=quarter * width * cols,
    )(meta, sink, *near(proj, vrows, vcols, local, partner_sum, across), gain, *near(att, att_logs))
    got = flip(send)
    spread = lax.dynamic_update_slice_in_dim(spread, got[None], 1 - t, 0)
    groups = [list(range(g * group, (g + 1) * group)) for g in range(sp // group)]
    mine = lax.all_to_all(
        spread.reshape(group * (tok + 16), LANES),
        "sp",
        0,
        0,
        axis_index_groups=groups,
        tiled=True,
    )
    theirs = flip(mine)
    shape = (group, tok + 16, LANES)
    inner = 2 * group * LANES
    return vmem_call(
        output_kernel,
        (
            jax.ShapeDtypeStruct((tok, out_m_weight.shape[1]), bf16),
            jax.ShapeDtypeStruct((2 * lh, tok), f32),
        ),
        scratch=[
            pltpu.VMEM((2 * group, tok, LANES), bf16),
            pltpu.VMEM((inner, out_m_weight.shape[1]), bf16),
        ],
        smem=1,
        n_in=2 + 2 * plane,
        flops=2 * tok * inner * out_m_weight.shape[1],
    )(meta, *near(mine.reshape(shape), theirs.reshape(shape), *out_blocks))


def solution(mesh):
    in_specs = (
        P("sp", None),
        P(),
        P("sp", "tp"),
        P("sp", "tp"),
        P("sp", "tp"),
        P("sp", "tp"),
        P("sp", None, "tp"),
        P(None, "tp"),
        P(None, "tp", "sp"),
        P("tp"),
        P("sp", "tp"),
        P("sp", "tp"),
        P("sp", "tp"),
        P("tp"),
        P("sp", "tp"),
        P("sp", "tp"),
    )
    out_specs = (P("sp", "tp"), P("tp", "sp"))

    def per_device(*args):
        plan = split_plan(mesh, args)
        if plan is None:
            return on_device(*args)
        return on_device_split(plan, *args)

    return jax.shard_map(
        per_device, mesh=mesh, in_specs=in_specs, out_specs=out_specs, check_vma=False
    )
```
